256 devices in a mesh: grp: 2 (over y), sp: 64 (over z, x), tp: 2 (over core).
Axes of the slice: x: 4, y: 2, z: 16, core: 2. Of those that a mesh axis runs over, the one named last changes fastest.
The devices are a block of a 4x16x16 slice.
Arguments:
- layer_input: bfloat16 [4, 8192, 2048], P('grp', ('sp', 'tp')), parts along dimension 0, may hold values from -6 to 6
- norm_gain: float32 [2048], replicated, may hold values from 0.1 to 1.9
- in_weight: bfloat16 [2048, 1024], P(None, 'tp'), may hold values from -0.125 to 0.125
- gate_weight: bfloat16 [2048, 1024], P(None, 'tp'), may hold values from -0.125 to 0.125
- rate_real: float32 [64, 64], P('tp'), may hold values from -1 to 0
- rate_imag: float32 [64, 64], P('tp'), may hold values from -3 to 3
- log_step: float32 [64], P('tp'), may hold values from -8 to -2.5
- input_real: bfloat16 [64, 64, 16], P('tp'), may hold values from -4 to 4
- input_imag: bfloat16 [64, 64, 16], P('tp'), may hold values from -4 to 4
- output_real: bfloat16 [64, 16, 64], P('tp'), may hold values from -10 to 10
- output_imag: bfloat16 [64, 16, 64], P('tp'), may hold values from -10 to 10
- skip_weight: float32 [1024], P('tp'), may hold values from -20 to 20
- decay_offset: float32 [4, 8192, 64], P('grp', 'sp', 'tp'), parts along dimension 0, may hold values from -1.5 to 0
- channel_gain: float32 [1024], replicated, may hold values from 0.1 to 1.9
- out_weight: bfloat16 [1024, 2048], P('tp'), may hold values from -0.1875 to 0.1875
Outputs:
- layer_output: bfloat16 [4, 8192, 2048], P('grp', ('sp', 'tp')), parts along dimension 0
The draws below stay inside these ranges and needn't reach their ends.
There are 2 independent parts, one for each index of `grp`. The reference program is written for one: setup_inputs(seed, part) draws one part's arguments, and reference() takes and returns one part's arrays. A program takes and returns all parts, laid end to end along the dimension named above; an argument that names none is the same for every part. Nothing has to cross between parts.
All inputs are finite; a program needn't handle non-finite values.
Results may differ from the reference program's by a relative error of at most 0.014.
Values may be sent and summed in bfloat16 or wider, within the bound.
A program may use at most 128 MiB of HBM per device.

```python
import math
import jax
import jax.numpy as jnp
from jax import lax

D = 2048
CHANNEL_GROUPS = 64
GROUP_CH = 16
STATE = 64
WIDTH = 1024
SEQUENCE_COUNT = 2
POS_DEV = 128
SEQUENCE_LENGTH = 8192


def group_speed(key):
    ranking = jax.random.permutation(jax.random.fold_in(key, 101), CHANNEL_GROUPS)
    fast_count = CHANNEL_GROUPS // 2
    return (ranking >= fast_count).astype(jnp.float32)


def group_scales():
    exponent = lax.iota(jnp.float32, CHANNEL_GROUPS) / (CHANNEL_GROUPS - 1)
    spread_base = 3.0
    return spread_base ** exponent


def draw_rate_real(key, part):
    slow_mask = group_speed(key)[:, None]
    slow_rate = -jnp.exp(jax.random.uniform(jax.random.fold_in(key, 3), (CHANNEL_GROUPS, STATE), jnp.float32, math.log(0.5), 0.0)) * math.sqrt(5.0 / SEQUENCE_LENGTH)
    fast_rate = -jax.random.uniform(jax.random.fold_in(key, 4), (CHANNEL_GROUPS, STATE), jnp.float32, 0.25, 1.0)
    return slow_mask * slow_rate + (1.0 - slow_mask) * fast_rate


def draw_log_step(key, part):
    slow_mask = group_speed(key)
    jitter = jax.random.uniform(jax.random.fold_in(key, 5), (CHANNEL_GROUPS,), jnp.float32, -0.2, 0.2)
    slow_value = math.log(0.07 * math.sqrt(5.0 / SEQUENCE_LENGTH))
    fast_value = math.log(0.05)
    return slow_mask * slow_value + (1.0 - slow_mask) * fast_value + jitter


def output_table(key, salt):
    values = jax.random.truncated_normal(jax.random.fold_in(key, salt), -4.0, 4.0, (CHANNEL_GROUPS, GROUP_CH, STATE), jnp.float32)
    return values * 0.25 * group_scales()[:, None, None]


def draw_output_real(key, part):
    return output_table(key, 31).astype(jnp.bfloat16)


def draw_output_imag(key, part):
    return output_table(key, 32).astype(jnp.bfloat16)


def draw_skip_weight(key, part):
    values = jax.random.truncated_normal(jax.random.fold_in(key, 41), -4.0, 4.0, (WIDTH,), jnp.float32)
    return values * 0.5 * jnp.repeat(group_scales(), GROUP_CH)


def draw_decay_offset(key, part):
    block_count = SEQUENCE_LENGTH // POS_DEV
    block_scale = jnp.exp(jax.random.uniform(jax.random.fold_in(key, 21), (SEQUENCE_COUNT, block_count, CHANNEL_GROUPS), jnp.float32, math.log(0.5), math.log(4.0)))
    block_scale = jnp.repeat(block_scale, POS_DEV, axis=1)
    roughness = jax.random.uniform(jax.random.fold_in(key, 22), (SEQUENCE_COUNT, SEQUENCE_LENGTH, CHANNEL_GROUPS), jnp.float32, 0.5, 1.5)
    steady = -(0.2 / SEQUENCE_LENGTH) * block_scale * roughness
    spike_location = jax.random.randint(jax.random.fold_in(key, 23), (SEQUENCE_COUNT, 2, CHANNEL_GROUPS), 0, SEQUENCE_LENGTH)
    spike_depth = jax.random.uniform(jax.random.fold_in(key, 24), (SEQUENCE_COUNT, 2, CHANNEL_GROUPS), jnp.float32, 0.22, 0.69)
    token_position = lax.iota(jnp.int32, SEQUENCE_LENGTH)[None, :, None]
    loss_values = jnp.where(token_position == spike_location[:, 0:1, :], spike_depth[:, 0:1, :], 0.0) + jnp.where(token_position == spike_location[:, 1:2, :], spike_depth[:, 1:2, :], 0.0)
    return steady - loss_values


def shard_levels(rng, dims, shards, least, largest):
    def one(axis_at, blocks):
        steps = jax.random.uniform(jax.random.fold_in(jax.random.fold_in(rng, 6), axis_at), (blocks,), jnp.float32, least / len(shards), largest / len(shards))
        return jnp.repeat(jnp.exp(steps), dims[axis_at] // blocks).reshape((-1,) + (1,) * (len(dims) - axis_at - 1))

    loudness = one(*shards[0])
    for cut in shards[1:]:
        loudness = loudness * one(*cut)
    return loudness


def gaussian(stream_key, dims, deviation, reach, shards=(), kind=jnp.bfloat16):
    result = deviation * jax.random.normal(stream_key, dims, jnp.float32)
    if shards:
        result = result * shard_levels(stream_key, dims, shards, -0.22, 0.18)
    return jnp.clip(result, -reach, reach).astype(kind)


def setup_inputs(seed: int = 0, part: int = 0) -> dict:
    seeds = jax.random.split(jax.random.key(seed), 16)
    own_keys = jax.random.split(jax.random.fold_in(seeds[15], part), 16)
    layer_input = gaussian(own_keys[0], (SEQUENCE_COUNT, SEQUENCE_LENGTH, D), 1.0, 6.0, ((1, 128),))
    norm_gain = jnp.clip(1.0 + 0.18 * jax.random.normal(seeds[1], (D,), jnp.float32), 0.1, 1.9)
    in_weight = gaussian(seeds[2], (D, WIDTH), D ** -0.5, 0.125, ((1, 2),))
    gate_weight = gaussian(seeds[3], (D, WIDTH), D ** -0.5, 0.125, ((1, 2),))
    rate_real = draw_rate_real(jax.random.fold_in(seeds[15], 71), part)
    rate_imag = jnp.clip(jax.random.uniform(seeds[5], (CHANNEL_GROUPS, STATE), jnp.float32, -3.0, 3.0) * shard_levels(seeds[5], (CHANNEL_GROUPS, STATE), ((0, 2),), -0.4, 0.0), -3.0, 3.0)
    log_step = draw_log_step(jax.random.fold_in(seeds[15], 71), part)
    input_real = gaussian(seeds[7], (CHANNEL_GROUPS, STATE, GROUP_CH), 0.25, 4.0, ((0, 2),))
    input_imag = gaussian(seeds[8], (CHANNEL_GROUPS, STATE, GROUP_CH), 0.25, 4.0, ((0, 2),))
    output_real = draw_output_real(jax.random.fold_in(seeds[15], 71), part)
    output_imag = draw_output_imag(jax.random.fold_in(seeds[15], 71), part)
    skip_weight = draw_skip_weight(jax.random.fold_in(seeds[15], 71), part)
    decay_offset = draw_decay_offset(jax.random.fold_in(jax.random.fold_in(seeds[15], part), 71), part)
    channel_gain = jnp.clip(1.0 + 0.18 * jax.random.normal(seeds[13], (WIDTH,), jnp.float32), 0.1, 1.9)
    out_weight = gaussian(seeds[14], (WIDTH, D), WIDTH ** -0.5, 0.1875, ((0, 2),))
    return dict(layer_input=layer_input, norm_gain=norm_gain, in_weight=in_weight, gate_weight=gate_weight, rate_real=rate_real, rate_imag=rate_imag, log_step=log_step, input_real=input_real, input_imag=input_imag, output_real=output_real, output_imag=output_imag, skip_weight=skip_weight, decay_offset=decay_offset, channel_gain=channel_gain, out_weight=out_weight)


epsilon = 1e-06
HIGHEST = lax.Precision.HIGHEST

def coefficients(rate_real, rate_imag, log_step, input_real, input_imag):
    step_size = jnp.exp(log_step)[:, None]
    real_step = rate_real * step_size
    angle_step = rate_imag * step_size
    top_re = jnp.expm1(real_step) * jnp.cos(angle_step) - 2.0 * jnp.sin(0.5 * angle_step) ** 2
    top_im = jnp.exp(real_step) * jnp.sin(angle_step)
    inverse = 1.0 / (rate_real * rate_real + rate_imag * rate_imag)
    coef_re = (top_re * rate_real + top_im * rate_imag) * inverse
    coef_im = (top_im * rate_real - top_re * rate_imag) * inverse
    table_re = input_real.astype(jnp.float32)
    table_im = input_imag.astype(jnp.float32)
    bbar_re = coef_re[..., None] * table_re - coef_im[..., None] * table_im
    bbar_im = coef_re[..., None] * table_im + coef_im[..., None] * table_re
    return (real_step, angle_step, bbar_re, bbar_im)

def compose(earlier, later):
    new_a_re = later[0] * earlier[0] - later[1] * earlier[1]
    new_a_im = later[0] * earlier[1] + later[1] * earlier[0]
    new_b_re = later[0] * earlier[2] - later[1] * earlier[3] + later[2]
    new_b_im = later[0] * earlier[3] + later[1] * earlier[2] + later[3]
    return (new_a_re, new_a_im, new_b_re, new_b_im)

def one_group(group_items):
    inputs_group, offset_group, real_row, rot_re, rot_im, bbar_re, bbar_im, read_re, read_im, skip_row = group_items
    magnitude = jnp.exp(real_row[None, None, :] + offset_group[..., None])
    trans_re = magnitude * rot_re[None, None, :]
    trans_im = magnitude * rot_im[None, None, :]
    drive_re = jnp.einsum('slc,pc->slp', inputs_group, bbar_re, precision=HIGHEST)
    drive_im = jnp.einsum('slc,pc->slp', inputs_group, bbar_im, precision=HIGHEST)
    scanned = lax.associative_scan(compose, (trans_re, trans_im, drive_re, drive_im), axis=1)
    mixed = jnp.einsum('slp,cp->slc', scanned[2], read_re, precision=HIGHEST) - jnp.einsum('slp,cp->slc', scanned[3], read_im, precision=HIGHEST)
    return mixed + skip_row[None, None, :] * inputs_group

def reference(layer_input, norm_gain, in_weight, gate_weight, rate_real, rate_imag, log_step, input_real, input_imag, output_real, output_imag, skip_weight, decay_offset, channel_gain, out_weight):
    wide_tokens = layer_input.astype(jnp.float32)
    normed = (wide_tokens * lax.rsqrt(lax.optimization_barrier(jnp.mean(wide_tokens * wide_tokens, axis=-1, keepdims=True)) + epsilon) * norm_gain).astype(jnp.bfloat16)
    flat_rows = normed.reshape(SEQUENCE_COUNT * SEQUENCE_LENGTH, D)
    inputs = jnp.dot(flat_rows, in_weight, preferred_element_type=jnp.float32).astype(jnp.bfloat16)
    gates = jnp.dot(flat_rows, gate_weight, preferred_element_type=jnp.float32).astype(jnp.bfloat16)
    inputs = inputs.reshape(SEQUENCE_COUNT, SEQUENCE_LENGTH, WIDTH)
    gates = gates.reshape(SEQUENCE_COUNT, SEQUENCE_LENGTH, WIDTH)
    real_step, angle_step, bbar_re, bbar_im = coefficients(rate_real, rate_imag, log_step, input_real, input_imag)
    inputs_wide = inputs.astype(jnp.float32)
    inputs_groups = jnp.moveaxis(inputs_wide.reshape(SEQUENCE_COUNT, SEQUENCE_LENGTH, CHANNEL_GROUPS, GROUP_CH), 2, 0)
    offset_groups = jnp.moveaxis(decay_offset, 2, 0)
    skip_groups = skip_weight.reshape(CHANNEL_GROUPS, GROUP_CH)
    mixed = lax.map(one_group, (inputs_groups, offset_groups, real_step, jnp.cos(angle_step), jnp.sin(angle_step), bbar_re, bbar_im, output_real.astype(jnp.float32), output_imag.astype(jnp.float32), skip_groups))
    mixed = jnp.moveaxis(mixed, 0, 2).reshape(SEQUENCE_COUNT, SEQUENCE_LENGTH, WIDTH)
    activated = jax.nn.gelu(mixed, approximate=False) * jax.nn.sigmoid(gates.astype(jnp.float32))
    normalized = (activated * lax.rsqrt(lax.optimization_barrier(jnp.mean(activated * activated, axis=-1, keepdims=True)) + epsilon) * channel_gain).astype(jnp.bfloat16)
    output = jnp.dot(normalized.reshape(SEQUENCE_COUNT * SEQUENCE_LENGTH, WIDTH), out_weight, preferred_element_type=jnp.float32)
    return output.astype(jnp.bfloat16).reshape(SEQUENCE_COUNT, SEQUENCE_LENGTH, D)
```

```python
import functools
import math

import jax
import jax.numpy as jnp
from jax import lax
from jax.experimental import pallas as pl
from jax.experimental.pallas import tpu as pltpu
from jax.sharding import Mesh
from jax.sharding import PartitionSpec as P

SP = ("sp_0", "sp_1")
SP_TP = ("sp_0", "sp_1", "tp")
MESH = pl.DeviceIdType.MESH
F32 = jnp.float32
BF16 = jnp.bfloat16
EPS = 1e-06
LANES = 128
CHUNKS = 8


def dot(a, b):
    return jnp.dot(a, b, preferred_element_type=F32)


def dot_t(a, b):
    return lax.dot_general(a, b, (((1,), (1,)), ((), ())), preferred_element_type=F32)


def iota(shape, dim):
    return lax.broadcasted_iota(jnp.int32, shape, dim)


def one_hot(cond):
    return jnp.where(cond, 1.0, 0.0).astype(BF16)


def split(value):
    high = value.astype(BF16)
    rest = value - high.astype(F32)
    middle = rest.astype(BF16)
    low = (rest - middle.astype(F32)).astype(BF16)
    return high, middle, low


def exact_dot(value, table):
    high, middle, low = split(value)
    return dot(high, table) + dot(middle, table) + dot(low, table)


def cmul(a, b):
    return a[0] * b[0] - a[1] * b[1], a[0] * b[1] + a[1] * b[0]


def small_expm1(x):
    series = x * (1.0 + x * (1 / 2 + x * (1 / 6 + x * (1 / 24 + x * (1 / 120 + x * (1 / 720 + x / 5040))))))
    return jnp.where(x > -0.3, series, jnp.exp(x) - 1.0)


def scan_order(rows):
    steps = rows // CHUNKS
    at = iota((rows, rows), 0)
    return one_hot(iota((rows, rows), 1) == (at & (CHUNKS - 1)) * steps + (at >> 3))


def natural_order(rows):
    steps = rows // CHUNKS
    at = iota((rows, rows), 1)
    return one_hot(iota((rows, rows), 0) == (at & (CHUNKS - 1)) * steps + (at >> 3))


def project_kernel(
    x_hbm,
    gain_ref,
    in_hbm,
    gate_hbm,
    inputs_ref,
    gates_ref,
    tokens,
    in_w,
    gate_w,
    normed,
    raw_in,
    raw_gate,
    local_sem,
    send_sem,
    recv_sem,
):
    tp = lax.axis_index("tp")
    sequences, own, depth = x_hbm.shape
    width = in_w.shape[1]
    barrier = pltpu.get_barrier_semaphore()
    pl.semaphore_signal(barrier, inc=1, device_id={"tp": 1 - tp}, device_id_type=MESH)
    mine = pl.ds(pl.multiple_of(tp * own, own), own)
    copies = [
        pltpu.make_async_copy(x_hbm, tokens.at[:, mine, :], local_sem.at[0]),
        pltpu.make_async_copy(in_hbm, in_w, local_sem.at[1]),
        pltpu.make_async_copy(gate_hbm, gate_w, local_sem.at[2]),
    ]
    for copy in copies:
        copy.start()
    pl.semaphore_wait(barrier, 1)
    remote = pltpu.make_async_remote_copy(
        src_ref=x_hbm,
        dst_ref=tokens.at[:, mine, :],
        send_sem=send_sem,
        recv_sem=recv_sem,
        device_id={"tp": 1 - tp},
        device_id_type=MESH,
    )
    remote.start()

    def norm(side):
        per = own // 16

        @pl.loop(0, sequences * per)
        def _(i):
            s = i // per
            row = pl.multiple_of(side * own + (i % per) * 16, 16)
            wide = tokens[s, pl.ds(row, 16), :].astype(F32)
            scale = lax.rsqrt(jnp.mean(wide * wide, axis=-1, keepdims=True) + EPS)
            normed[pl.ds(pl.multiple_of(i * 16, 16), 16), :] = (wide * scale * gain_ref[...]).astype(BF16)

    def project(side, weight, out):
        rows = pl.ds(pl.multiple_of(side * own, own), own)

        @pl.loop(0, width // 256)
        def _(c):
            lanes = pl.ds(pl.multiple_of(c * 256, 256), 256)
            part = dot(normed[...], weight[:, lanes])
            out[:, rows, lanes] = part.reshape(sequences, own, 256).astype(BF16)

    copies[0].wait()
    norm(tp)
    copies[1].wait()
    project(tp, in_w, raw_in)
    copies[2].wait()
    project(tp, gate_w, raw_gate)
    remote.wait()
    norm(1 - tp)
    project(1 - tp, in_w, raw_in)
    project(1 - tp, gate_w, raw_gate)
    rows = sequences * 2 * own
    order = scan_order(rows)
    inputs_ref[...] = dot(order, raw_in[...].reshape(rows, width)).astype(BF16)
    gates_ref[...] = dot(order, raw_gate[...].reshape(rows, width)).astype(BF16)


def mixer_kernel(
    inputs_ref,
    gates_ref,
    rate_re_ref,
    rate_im_ref,
    log_step_ref,
    table_re_ref,
    table_im_ref,
    read_re_ref,
    read_im_ref,
    skip_ref,
    offset_ref,
    gain_ref,
    out_w_hbm,
    out_ref,
    out_w,
    mags,
    drive_re,
    drive_im,
    states_re,
    states_im,
    lift_re,
    lift_im,
    vec,
    ends,
    before,
    init,
    log_pack,
    log_x,
    log_row,
    log_z,
    sum_stage,
    sum_pack,
    sum_x,
    sum_row,
    sum_z,
    carry_pack,
    carry_x,
    lam_pack,
    act,
    act_in,
    w_sem,
    w_send,
    w_recv,
    lx_send,
    lx_recv,
    lz_send,
    lz_recv,
    sx_send,
    sx_recv,
    sz_send,
    sz_recv,
    cx_send,
    cx_recv,
    a_send,
    a_recv,
):
    nz, nx = lax.axis_size("sp_0"), lax.axis_size("sp_1")
    mz, mx, tp = lax.axis_index("sp_0"), lax.axis_index("sp_1"), lax.axis_index("tp")
    rows, width = inputs_ref.shape
    groups, states = rate_re_ref.shape
    modes = groups * states
    steps = rows // CHUNKS
    sequences, own, depth = out_ref.shape
    quarters = CHUNKS // sequences
    part = modes // nx
    blocks = part // LANES
    tile = sequences * blocks
    half = modes // 2

    log_z[...] = jnp.zeros_like(log_z)
    sum_z[...] = jnp.zeros_like(sum_z)
    barrier = pltpu.get_barrier_semaphore()
    for d in range(1, nx):
        pl.semaphore_signal(barrier, inc=1, device_id={"sp_1": lax.rem(mx + d, nx)}, device_id_type=MESH)
    for d in range(1, nz):
        pl.semaphore_signal(barrier, inc=1, device_id={"sp_0": lax.rem(mz + d, nz)}, device_id_type=MESH)
    pl.semaphore_signal(barrier, inc=1, device_id={"tp": 1 - tp}, device_id_type=MESH)
    own_w = pltpu.make_async_copy(out_w_hbm, out_w.at[tp], w_sem)
    own_w.start()

    def to_x(source, target, send, recv):
        made = []
        for d in range(1, nx):
            k = lax.rem(mx + d, nx)
            made.append(
                pltpu.make_async_remote_copy(
                    src_ref=source.at[k],
                    dst_ref=target.at[mx],
                    send_sem=send.at[d - 1],
                    recv_sem=recv.at[d - 1],
                    device_id={"sp_1": k},
                    device_id_type=MESH,
                )
            )
        return made

    def to_z(source, target, send, recv):
        made = []
        for d in range(1, nz):
            made.append(
                pltpu.make_async_remote_copy(
                    src_ref=source,
                    dst_ref=target.at[d - 1],
                    send_sem=send.at[d - 1],
                    recv_sem=recv.at[d - 1],
                    device_id={"sp_0": lax.rem(mz + d, nz)},
                    device_id_type=MESH,
                )
            )
        return made

    def start_z(made):
        for d, copy in enumerate(made, 1):
            pl.when(mz + d < nz)(copy.start)

    def recv_z(made):
        for d, copy in enumerate(made, 1):
            pl.when(d <= mz)(copy.wait_recv)

    def sent_z(made):
        for d, copy in enumerate(made, 1):
            pl.when(mz + d < nz)(copy.wait_send)

    spread_g = one_hot((iota((groups, modes), 1) >> 6) == iota((groups, modes), 0))
    spread_p = one_hot((iota((states, modes), 1) & (states - 1)) == iota((states, modes), 0))

    offsets = offset_ref[...]
    chunk_logs = exact_dot(jnp.sum(offsets.reshape(CHUNKS, steps, groups), axis=1), spread_g)
    vec[pl.ds(16, CHUNKS), :] = chunk_logs
    for s in range(sequences):
        total = jnp.sum(chunk_logs[s * quarters : (s + 1) * quarters], axis=0, keepdims=True)
        for k in range(nx):
            for b in range(blocks):
                lo = k * part + b * LANES
                row = s * blocks + b
                log_pack[k, row : row + 1, :] = total[:, lo : lo + LANES]

    on_group = (iota((groups, modes), 1) >> 6) == iota((groups, modes), 0)

    def flat(ref):
        return jnp.sum(jnp.where(on_group, exact_dot(ref[...], spread_p), 0.0), axis=0, keepdims=True)

    step = exact_dot(jnp.broadcast_to(jnp.exp(log_step_ref[...]), (8, groups)), spread_g)[0:1]
    rate_re, rate_im = flat(rate_re_ref), flat(rate_im_ref)
    real_step, angle = rate_re * step, rate_im * step
    size = jnp.exp(real_step)
    cosine, sine = jnp.cos(angle), jnp.sin(angle)
    half_sine = jnp.sin(0.5 * angle)
    top_re = small_expm1(real_step) * cosine - 2.0 * half_sine * half_sine
    top_im = size * sine
    inverse = 1.0 / (rate_re * rate_re + rate_im * rate_im)
    coef_re = (top_re * rate_re + top_im * rate_im) * inverse
    coef_im = (top_im * rate_re - top_re * rate_im) * inverse
    lam = (size * cosine, size * sine)
    power = lam
    for _ in range(int(math.log2(steps))):
        power = cmul(power, power)
    lam_chunk = power
    for _ in range(int(math.log2(quarters))):
        power = cmul(power, power)
    for i, value in enumerate((*lam, *lam_chunk, *power, coef_re, coef_im)):
        vec[i : i + 1, :] = value

    order = scan_order(rows)
    pieces = [dot(order, piece) for piece in split(jnp.exp(offsets))]
    spread_3 = one_hot((iota((3 * groups, modes), 1) >> 6) == (iota((3 * groups, modes), 0) & (groups - 1)))
    mags[...] = dot(jnp.concatenate(pieces, axis=1).astype(BF16), spread_3)

    channels = table_re_ref.shape[1]
    eye = one_hot(iota((channels, channels), 0) == iota((channels, channels), 1))
    hw = width // 2
    same = (iota((hw, half), 0) >> 4) == (iota((hw, half), 1) >> 6)
    for h in range(2):
        for table, drive in ((table_re_ref, drive_re), (table_im_ref, drive_im)):
            turned = dot_t(eye, table[h * half : (h + 1) * half, :])
            wide = jnp.where(same, jnp.concatenate([turned] * (hw // channels), axis=0), 0.0).astype(BF16)
            drive[:, h * half : (h + 1) * half] = dot(inputs_ref[:, h * hw : (h + 1) * hw], wide)

    pl.semaphore_wait(barrier, nx + nz - 1)
    log_sends = to_x(log_pack, log_x, lx_send, lx_recv)
    for copy in log_sends:
        copy.start()
    w_copy = pltpu.make_async_remote_copy(
        src_ref=out_w_hbm,
        dst_ref=out_w.at[tp],
        send_sem=w_send,
        recv_sem=w_recv,
        device_id={"tp": 1 - tp},
        device_id_type=MESH,
    )
    w_copy.start()
    log_x[pl.ds(mx, 1)] = log_pack[pl.ds(mx, 1)]

    span = 512

    def scan(first, keep):
        @pl.loop(0, modes // span)
        def _(c):
            lanes = pl.ds(pl.multiple_of(c * span, span), span)
            lr = jnp.broadcast_to(vec[0:1, lanes], (CHUNKS, span))
            li = jnp.broadcast_to(vec[1:2, lanes], (CHUNKS, span))
            if first is None:
                start = (jnp.zeros((CHUNKS, span), F32), jnp.zeros((CHUNKS, span), F32))
            else:
                start = (first[0, :, lanes], first[1, :, lanes])

            def body(t, now):
                re, im = now
                at = pl.ds(pl.multiple_of(t * 16, 16), 16)
                m, dr, di = mags[at, lanes], drive_re[at, lanes], drive_im[at, lanes]
                kept = []
                for u in range(2):
                    use = slice(u * CHUNKS, (u + 1) * CHUNKS)
                    ar, ai = m[use] * lr, m[use] * li
                    re, im = ar * re - ai * im + dr[use], ar * im + ai * re + di[use]
                    kept.append((re, im))
                if keep:
                    states_re[at, lanes] = jnp.concatenate([k[0] for k in kept], axis=0).astype(BF16)
                    states_im[at, lanes] = jnp.concatenate([k[1] for k in kept], axis=0).astype(BF16)
                return re, im

            re, im = lax.fori_loop(0, steps // 2, body, start)
            if not keep:
                ends[0, :, lanes] = re
                ends[1, :, lanes] = im

    scan(None, False)

    place = iota((CHUNKS, modes), 0) & (quarters - 1)
    grown = jnp.exp(vec[pl.ds(16, CHUNKS), :])
    a = (grown * vec[2:3, :], grown * vec[3:4, :])
    b = (ends[0], ends[1])
    d = 1
    while d < quarters:
        ok = place >= d
        a_old = tuple(pltpu.roll(v, d, axis=0) for v in a)
        b_old = tuple(pltpu.roll(v, d, axis=0) for v in b)
        add = cmul(a, b_old)
        new_a = cmul(a, a_old)
        b = tuple(jnp.where(ok, v + w, v) for v, w in zip(b, add))
        a = tuple(jnp.where(ok, w, v) for v, w in zip(a, new_a))
        d *= 2
    for i, (value, empty) in enumerate(((a[0], 1.0), (a[1], 0.0), (b[0], 0.0), (b[1], 0.0))):
        before[i] = jnp.where(place == 0, empty, pltpu.roll(value, 1, axis=0))
    for c in range(2):
        for s in range(sequences):
            last = (s + 1) * quarters - 1
            for k in range(nx):
                for blk in range(blocks):
                    lo = k * part + blk * LANES
                    row = c * tile + s * blocks + blk
                    sum_stage[k, row : row + 1, :] = b[c][last : last + 1, lo : lo + LANES]
    sum_pack[...] = sum_stage[...].astype(BF16)
    sum_sends = to_x(sum_pack, sum_x, sx_send, sx_recv)
    for copy in sum_sends:
        copy.start()
    sum_x[pl.ds(mx, 1)] = sum_pack[pl.ds(mx, 1)]

    for copy in log_sends:
        copy.wait()
    log_row[...] = jnp.sum(log_x[...], axis=0)
    log_z_sends = to_z(log_row, log_z, lz_send, lz_recv)
    start_z(log_z_sends)
    for c in range(2):
        for blk in range(blocks):
            lanes = pl.ds(pl.multiple_of(mx * part + blk * LANES, LANES), LANES)
            value = vec[4 + c : 5 + c, lanes]
            for s in range(sequences):
                row = s * blocks + blk
                lam_pack[c, row : row + 1, :] = value
    lam_dev = (lam_pack[0], lam_pack[1])
    lam_row = lam_dev
    for _ in range(int(math.log2(nx))):
        lam_row = cmul(lam_row, lam_row)

    def grow(logs, base):
        size = jnp.exp(logs)
        return size * base[0], size * base[1]

    def halves(value):
        wide = value.astype(F32)
        return wide[:tile], wide[tile:]

    def step_over(carry, trans, add):
        moved = cmul(carry, trans)
        return moved[0] + add[0], moved[1] + add[1]

    for copy in sum_sends:
        copy.wait()
    nothing = (jnp.zeros((tile, LANES), F32), jnp.zeros((tile, LANES), F32))
    total = nothing
    for k in range(nx):
        total = step_over(total, grow(log_x[k], lam_dev), halves(sum_x[k]))
    sum_row[...] = jnp.concatenate(total, axis=0).astype(BF16)
    sum_z_sends = to_z(sum_row, sum_z, sz_send, sz_recv)
    start_z(sum_z_sends)

    reads = (iota((hw, half), 0) >> 4) == (iota((hw, half), 1) >> 6)
    for h in range(2):
        use = slice(h * hw, (h + 1) * hw)
        wide_re = dot(read_re_ref[use, :], spread_p[:, :half])
        wide_im = dot(read_im_ref[use, :], spread_p[:, :half])
        kr, ki = vec[6:7, h * half : (h + 1) * half], vec[7:8, h * half : (h + 1) * half]
        lift_re[use, :] = jnp.where(reads, wide_re * kr - wide_im * ki, 0.0).astype(BF16)
        lift_im[use, :] = jnp.where(reads, -(wide_re * ki + wide_im * kr), 0.0).astype(BF16)

    recv_z(log_z_sends)
    recv_z(sum_z_sends)
    carry = nothing
    for d in range(nz - 1, 0, -1):
        new = step_over(carry, grow(log_z[d - 1], lam_row), halves(sum_z[d - 1]))
        carry = tuple(jnp.where(d <= mz, n, o) for n, o in zip(new, carry))
    for k in range(nx):
        carry_pack[k] = jnp.concatenate(carry, axis=0).astype(BF16)
        carry = step_over(carry, grow(log_x[k], lam_dev), halves(sum_x[k]))
    carry_sends = to_x(carry_pack, carry_x, cx_send, cx_recv)
    for copy in carry_sends:
        copy.start()
    carry_x[pl.ds(mx, 1)] = carry_pack[pl.ds(mx, 1)]
    for copy in carry_sends:
        copy.wait()
    upper = iota((CHUNKS, LANES), 0) < quarters
    for k in range(nx):
        got = carry_x[k].astype(F32)
        for blk in range(blocks):
            lo = k * part + blk * LANES
            lanes = slice(lo, lo + LANES)
            came = tuple(
                jnp.where(upper, got[c * tile + blk][None], got[c * tile + blocks + blk][None]) for c in range(2)
            )
            moved = cmul((before[0, :, lanes], before[1, :, lanes]), came)
            init[0, :, lanes] = before[2, :, lanes] + moved[0]
            init[1, :, lanes] = before[3, :, lanes] + moved[1]

    scan(init, True)

    parts = []
    for h in range(2):
        use = slice(h * hw, (h + 1) * hw)
        lanes = slice(h * half, (h + 1) * half)
        mixed = dot_t(states_re[:, lanes], lift_re[use, :]) + dot_t(states_im[:, lanes], lift_im[use, :])
        mixed = mixed + skip_ref[:, use] * inputs_ref[:, use].astype(F32)
        gelu = 0.5 * mixed * (1.0 + lax.erf(mixed * math.sqrt(0.5)))
        gated = gelu / (1.0 + jnp.exp(-gates_ref[:, use].astype(F32)))
        parts.append(gated.astype(BF16))
    back = natural_order(rows)
    for h in range(2):
        act[:, :, h * hw : (h + 1) * hw] = dot(back, parts[h]).astype(BF16).reshape(sequences, 2 * own, hw)
    theirs = pl.ds(pl.multiple_of((1 - tp) * own, own), own)
    mine = pl.ds(pl.multiple_of(tp * own, own), own)
    a_copy = pltpu.make_async_remote_copy(
        src_ref=act.at[:, theirs, :],
        dst_ref=act_in,
        send_sem=a_send,
        recv_sem=a_recv,
        device_id={"tp": 1 - tp},
        device_id_type=MESH,
    )
    a_copy.start()
    near = act[:, mine, :].astype(F32).reshape(sequences * own, width)
    near_square = jnp.sum(near * near, axis=-1, keepdims=True)
    own_w.wait()
    w_copy.wait()
    a_copy.wait()
    far = act_in[...].astype(F32).reshape(sequences * own, width)
    scale = lax.rsqrt((near_square + jnp.sum(far * far, axis=-1, keepdims=True)) * (0.5 / width) + EPS)
    gain_near = gain_ref[:, pl.ds(pl.multiple_of(tp * width, width), width)]
    gain_far = gain_ref[:, pl.ds(pl.multiple_of((1 - tp) * width, width), width)]
    near = (near * scale * gain_near).astype(BF16)
    far = (far * scale * gain_far).astype(BF16)

    for c in range(depth // 256):
        lanes = slice(c * 256, (c + 1) * 256)
        result = dot(near, out_w[tp, :, lanes]) + dot(far, out_w[1 - tp, :, lanes])
        out_ref[:, :, lanes] = result.astype(BF16).reshape(sequences, own, 256)

    sent_z(log_z_sends)
    sent_z(sum_z_sends)


def vmem():
    return pl.BlockSpec(memory_space=pltpu.VMEM)


def hbm():
    return pl.BlockSpec(memory_space=pl.ANY)


def shards(
    layer_input,
    norm_gain,
    in_weight,
    gate_weight,
    rate_real,
    rate_imag,
    log_step,
    input_real,
    input_imag,
    output_real,
    output_imag,
    skip_weight,
    decay_offset,
    channel_gain,
    out_weight,
):
    nz, nx = lax.axis_size("sp_0"), lax.axis_size("sp_1")
    sequences, own, depth = layer_input.shape
    width = in_weight.shape[1]
    groups, states = rate_real.shape
    channels = input_real.shape[2]
    modes = groups * states
    rows = sequences * 2 * own
    dma = pltpu.SemaphoreType.DMA
    inputs, gates = pl.pallas_call(
        project_kernel,
        name="project",
        out_shape=[jax.ShapeDtypeStruct((rows, width), BF16)] * 2,
        in_specs=[hbm(), vmem(), hbm(), hbm()],
        out_specs=[vmem(), vmem()],
        scratch_shapes=[
            pltpu.VMEM((sequences, 2 * own, depth), BF16),
            pltpu.VMEM((depth, width), BF16),
            pltpu.VMEM((depth, width), BF16),
            pltpu.VMEM((sequences * own, depth), BF16),
            pltpu.VMEM((sequences, 2 * own, width), BF16),
            pltpu.VMEM((sequences, 2 * own, width), BF16),
            dma((3,)),
            dma,
            dma,
        ],
        compiler_params=pltpu.CompilerParams(collective_id=0, has_side_effects=True),
    )(layer_input, norm_gain[None], in_weight, gate_weight)

    tile = sequences * (modes // nx // LANES)
    f32 = functools.partial(pltpu.VMEM, dtype=F32)
    b16 = functools.partial(pltpu.VMEM, dtype=BF16)
    return pl.pallas_call(
        mixer_kernel,
        name="mixer",
        out_shape=jax.ShapeDtypeStruct((sequences, own, depth), BF16),
        in_specs=[vmem()] * 12 + [hbm()],
        out_specs=vmem(),
        scratch_shapes=[
            b16((2, width, depth)),
            f32((rows, modes)),
            f32((rows, modes)),
            f32((rows, modes)),
            b16((rows, modes)),
            b16((rows, modes)),
            b16((width, modes // 2)),
            b16((width, modes // 2)),
            f32((24, modes)),
            f32((2, CHUNKS, modes)),
            f32((4, CHUNKS, modes)),
            f32((2, CHUNKS, modes)),
            f32((nx, tile, LANES)),
            f32((nx, tile, LANES)),
            f32((tile, LANES)),
            f32((nz - 1, tile, LANES)),
            f32((nx, 2 * tile, LANES)),
            b16((nx, 2 * tile, LANES)),
            b16((nx, 2 * tile, LANES)),
            b16((2 * tile, LANES)),
            b16((nz - 1, 2 * tile, LANES)),
            b16((nx, 2 * tile, LANES)),
            b16((nx, 2 * tile, LANES)),
            f32((2, tile, LANES)),
            b16((sequences, 2 * own, width)),
            b16((sequences, own, width)),
            dma,
            dma,
            dma,
            dma((nx - 1,)),
            dma((nx - 1,)),
            dma((nz - 1,)),
            dma((nz - 1,)),
            dma((nx - 1,)),
            dma((nx - 1,)),
            dma((nz - 1,)),
            dma((nz - 1,)),
            dma((nx - 1,)),
            dma((nx - 1,)),
            dma,
            dma,
        ],
        compiler_params=pltpu.CompilerParams(collective_id=1, has_side_effects=True),
    )(
        inputs,
        gates,
        rate_real,
        rate_imag,
        log_step[None],
        input_real.reshape(modes, channels),
        input_imag.reshape(modes, channels),
        output_real.reshape(width, states),
        output_imag.reshape(width, states),
        skip_weight[None],
        decay_offset.reshape(rows, groups),
        channel_gain[None],
        out_weight,
    )


def solution(mesh):
    torus = Mesh(
        mesh.devices.reshape(mesh.shape["grp"], 16, 4, mesh.shape["tp"]),
        ("grp", "sp_0", "sp_1", "tp"),
    )
    return build(torus)


def build(torus):
    in_specs = (
        P("grp", SP_TP, None),
        P(),
        P(None, "tp"),
        P(None, "tp"),
        P("tp", None),
        P("tp", None),
        P("tp"),
        P("tp", None, None),
        P("tp", None, None),
        P("tp", None, None),
        P("tp", None, None),
        P("tp"),
        P("grp", SP, "tp"),
        P(),
        P("tp", None),
    )
    out_specs = P("grp", SP_TP, None)
    return jax.shard_map(shards, mesh=torus, in_specs=in_specs, out_specs=out_specs, check_vma=False)
```

```python
import functools
import math

import jax
import jax.numpy as jnp
from jax import lax
from jax.experimental import pallas as pl
from jax.experimental.pallas import tpu as pltpu
from jax.sharding import Mesh
from jax.sharding import PartitionSpec as P

SP = ("sp_0", "sp_1")
SP_TP = ("sp_0", "sp_1", "tp")
MESH = pl.DeviceIdType.MESH
F32 = jnp.float32
BF16 = jnp.bfloat16
EPS = 1e-06
LANES = 128
CHUNKS = 8


def dot(a, b):
    return jnp.dot(a, b, preferred_element_type=F32)


def dot_t(a, b):
    return lax.dot_general(a, b, (((1,), (1,)), ((), ())), preferred_element_type=F32)


def iota(shape, dim):
    return lax.broadcasted_iota(jnp.int32, shape, dim)


def one_hot(cond):
    return jnp.where(cond, 1.0, 0.0).astype(BF16)


def split(value):
    high = value.astype(BF16)
    rest = value - high.astype(F32)
    middle = rest.astype(BF16)
    low = (rest - middle.astype(F32)).astype(BF16)
    return high, middle, low


def exact_dot(value, table):
    high, middle, low = split(value)
    return dot(high, table) + dot(middle, table) + dot(low, table)


def cmul(a, b):
    return a[0] * b[0] - a[1] * b[1], a[0] * b[1] + a[1] * b[0]


def small_expm1(x):
    series = x * (1.0 + x * (1 / 2 + x * (1 / 6 + x * (1 / 24 + x * (1 / 120 + x * (1 / 720 + x / 5040))))))
    return jnp.where(x > -0.3, series, jnp.exp(x) - 1.0)


def scan_order(rows):
    steps = rows // CHUNKS
    at = iota((rows, rows), 0)
    return one_hot(iota((rows, rows), 1) == (at & (CHUNKS - 1)) * steps + (at >> 3))


def natural_order(rows):
    steps = rows // CHUNKS
    at = iota((rows, rows), 1)
    return one_hot(iota((rows, rows), 0) == (at & (CHUNKS - 1)) * steps + (at >> 3))


def small_sine(x):
    q = x * x
    return x * (1.0 + q * (-1 / 6 + q * (1 / 120 + q * (-1 / 5040 + q * (1 / 362880 - q / 39916800)))))


def small_cosine(x):
    q = x * x
    return 1.0 + q * (-1 / 2 + q * (1 / 24 + q * (-1 / 720 + q * (1 / 40320 + q * (-1 / 3628800 + q / 479001600)))))


def mixer_kernel(
    x_hbm,
    in_w_hbm,
    gate_w_hbm,
    out_w_hbm,
    norm_gain_hbm,
    rate_re_hbm,
    rate_im_hbm,
    log_step_hbm,
    table_re_hbm,
    table_im_hbm,
    read_re_hbm,
    read_im_hbm,
    skip_hbm,
    offset_hbm,
    gain_hbm,
    out_ref,
    tokens,
    in_w,
    gate_w,
    out_w,
    norm_gain_ref,
    rate_re_ref,
    rate_im_ref,
    log_step_ref,
    table_re_ref,
    table_im_ref,
    read_re_ref,
    read_im_ref,
    skip_ref,
    offset_ref,
    gain_ref,
    normed,
    raw_in,
    raw_gate,
    inputs,
    opened,
    mags,
    wide_re,
    wide_im,
    drive_re,
    drive_im,
    states_re,
    states_im,
    lift_re,
    lift_im,
    vec,
    ends,
    before,
    init,
    log_pack,
    log_x,
    log_row,
    log_z,
    sum_stage,
    sum_pack,
    sum_x,
    sum_row,
    sum_z,
    carry_pack,
    carry_x,
    lam_pack,
    act,
    act_in,
    near_sum,
    load_sem,
    x_send,
    x_recv,
    w_send,
    w_recv,
    lx_send,
    lx_recv,
    lz_send,
    lz_recv,
    sx_send,
    sx_recv,
    sz_send,
    sz_recv,
    cx_send,
    cx_recv,
    a_send,
    a_recv,
):
    nz, nx = lax.axis_size("sp_0"), lax.axis_size("sp_1")
    mz, mx, tp = lax.axis_index("sp_0"), lax.axis_index("sp_1"), lax.axis_index("tp")
    sequences, own, depth = x_hbm.shape
    width = in_w_hbm.shape[1]
    rows = sequences * 2 * own
    groups, states = rate_re_hbm.shape
    channels = width // groups
    modes = groups * states
    steps = rows // CHUNKS
    quarters = CHUNKS // sequences
    part = modes // nx
    blocks = part // LANES
    tile = sequences * blocks
    half = modes // 2
    hw = width // 2
    mine = pl.ds(pl.multiple_of(tp * own, own), own)
    theirs = pl.ds(pl.multiple_of((1 - tp) * own, own), own)
    partner = {"tp": 1 - tp}

    loads = [
        pltpu.make_async_copy(source, target, load_sem.at[i])
        for i, (source, target) in enumerate(
            (
                (x_hbm, tokens.at[:, mine, :]),
                (offset_hbm, offset_ref),
                (rate_re_hbm, rate_re_ref),
                (rate_im_hbm, rate_im_ref),
                (log_step_hbm, log_step_ref),
                (norm_gain_hbm, norm_gain_ref),
                (table_re_hbm, table_re_ref),
                (table_im_hbm, table_im_ref),
                (in_w_hbm, in_w),
                (gate_w_hbm, gate_w),
                (read_re_hbm, read_re_ref),
                (read_im_hbm, read_im_ref),
                (skip_hbm, skip_ref),
                (gain_hbm, gain_ref),
                (out_w_hbm, out_w.at[tp]),
            )
        )
    ]
    for copy in loads:
        copy.start()

    log_z[...] = jnp.zeros_like(log_z)
    sum_z[...] = jnp.zeros_like(sum_z)
    barrier = pltpu.get_barrier_semaphore()
    pl.semaphore_signal(barrier, inc=1, device_id=partner, device_id_type=MESH)
    for d in range(1, nx):
        pl.semaphore_signal(barrier, inc=1, device_id={"sp_1": lax.rem(mx + d, nx)}, device_id_type=MESH)
    far_first = sorted(range(1, nz), key=lambda d: -min(d, nz - d))
    for d in far_first:
        pl.semaphore_signal(barrier, inc=1, device_id={"sp_0": lax.rem(mz + d, nz)}, device_id_type=MESH)

    def remote(source, target, send, recv, device):
        return pltpu.make_async_remote_copy(
            src_ref=source, dst_ref=target, send_sem=send, recv_sem=recv, device_id=device, device_id_type=MESH
        )

    def to_x(source, target, send, recv):
        made = []
        for d in range(1, nx):
            k = lax.rem(mx + d, nx)
            made.append(remote(source.at[k], target.at[mx], send.at[d - 1], recv.at[d - 1], {"sp_1": k}))
        return made

    def to_z(source, target, send, recv):
        return {
            d: remote(source, target.at[d - 1], send.at[d - 1], recv.at[d - 1], {"sp_0": lax.rem(mz + d, nz)})
            for d in far_first
        }

    def start_z(made):
        for d, copy in made.items():
            pl.when(mz + d < nz)(copy.start)

    def recv_z(made):
        for d, copy in made.items():
            pl.when(d <= mz)(copy.wait_recv)

    def sent_z(made):
        for d, copy in made.items():
            pl.when(mz + d < nz)(copy.wait_send)

    for copy in loads[1:6]:
        copy.wait()
    spread_g = one_hot((iota((groups, modes), 1) >> 6) == iota((groups, modes), 0))
    spread_p = one_hot((iota((states, modes), 1) & (states - 1)) == iota((states, modes), 0))
    offsets = jnp.concatenate([offset_ref[s].T for s in range(sequences)], axis=0)
    sums = jnp.sum(offsets.reshape(CHUNKS, steps, groups), axis=1)
    step_size = jnp.broadcast_to(jnp.exp(log_step_ref[...]), (8, groups))
    spread = exact_dot(jnp.concatenate([sums, step_size], axis=0), spread_g)
    chunk_logs, step = spread[:CHUNKS], spread[CHUNKS : CHUNKS + 1]
    vec[pl.ds(16, CHUNKS), :] = chunk_logs
    for s in range(sequences):
        total = jnp.sum(chunk_logs[s * quarters : (s + 1) * quarters], axis=0, keepdims=True)
        for k in range(nx):
            for b in range(blocks):
                lo = k * part + b * LANES
                row = s * blocks + b
                log_pack[k, row : row + 1, :] = total[:, lo : lo + LANES]

    pl.semaphore_wait(barrier, nx + nz - 1)
    x_copy = remote(x_hbm, tokens.at[:, mine, :], x_send, x_recv, partner)
    x_copy.start()
    log_sends = to_x(log_pack, log_x, lx_send, lx_recv)
    for copy in log_sends:
        copy.start()
    log_x[pl.ds(mx, 1)] = log_pack[pl.ds(mx, 1)]

    def norm(side):
        per = own // 16

        @pl.loop(0, sequences * per)
        def _(i):
            s = i // per
            row = pl.multiple_of(side * own + (i % per) * 16, 16)
            wide = tokens[s, pl.ds(row, 16), :].astype(F32)
            scale = lax.rsqrt(jnp.mean(wide * wide, axis=-1, keepdims=True) + EPS)
            at = pl.ds(pl.multiple_of(i * 16, 16), 16)
            normed[side, at, :] = (wide * scale * norm_gain_ref[...]).astype(BF16)

    def project(side, weight, out):
        @pl.loop(0, width // 256)
        def _(c):
            lanes = pl.ds(pl.multiple_of(c * 256, 256), 256)
            product = dot(normed[side], weight[:, lanes])
            at = pl.ds(pl.multiple_of(side * own, own), own)
            out[:, at, lanes] = product.reshape(sequences, own, 256).astype(BF16)

    loads[0].wait()
    norm(tp)
    loads[8].wait()
    project(tp, in_w, raw_in)

    on_group = (iota((groups, modes), 1) >> 6) == iota((groups, modes), 0)
    rates = exact_dot(jnp.concatenate([rate_re_ref[...], rate_im_ref[...]], axis=0), spread_p)
    rate_re = jnp.sum(jnp.where(on_group, rates[:groups], 0.0), axis=0, keepdims=True)
    rate_im = jnp.sum(jnp.where(on_group, rates[groups:], 0.0), axis=0, keepdims=True)
    real_step, angle = rate_re * step, rate_im * step
    size = jnp.exp(real_step)
    cosine, sine = small_cosine(angle), small_sine(angle)
    half_sine = small_sine(0.5 * angle)
    top_re = small_expm1(real_step) * cosine - 2.0 * half_sine * half_sine
    top_im = size * sine
    inverse = 1.0 / (rate_re * rate_re + rate_im * rate_im)
    coef_re = (top_re * rate_re + top_im * rate_im) * inverse
    coef_im = (top_im * rate_re - top_re * rate_im) * inverse
    lam = (size * cosine, size * sine)
    power = lam
    for _ in range(int(math.log2(steps))):
        power = cmul(power, power)
    lam_chunk = power
    for _ in range(int(math.log2(quarters))):
        power = cmul(power, power)
    for i, value in enumerate((*lam, *lam_chunk, *power, coef_re, coef_im)):
        vec[i : i + 1, :] = value

    order = scan_order(rows)
    pieces = [dot(order, piece) for piece in split(jnp.exp(offsets))]
    spread_3 = one_hot((iota((3 * groups, modes), 1) >> 6) == (iota((3 * groups, modes), 0) & (groups - 1)))
    mags[...] = dot(jnp.concatenate(pieces, axis=1).astype(BF16), spread_3)

    per_tile = LANES // states

    def doubled(value):
        return jnp.concatenate([value.astype(F32)] * per_tile, axis=1)

    on_lane = iota((channels, LANES), 1) // states

    def block_diagonal(target, value):
        target[...] = jnp.zeros_like(target)
        for g in range(groups):
            at = slice(g * channels, (g + 1) * channels)
            lo = (g % (groups // 2)) // per_tile * LANES
            kept = jnp.where(on_lane == g % per_tile, value(g, at), 0.0)
            target[at, lo : lo + LANES] = kept.astype(BF16)

    for copy in loads[6:8]:
        copy.wait()
    two_re, two_im = doubled(table_re_ref[...]), doubled(table_im_ref[...])
    block_diagonal(wide_re, lambda g, at: two_re[at])
    block_diagonal(wide_im, lambda g, at: two_im[at])

    x_copy.wait()
    norm(1 - tp)
    project(1 - tp, in_w, raw_in)
    inputs[...] = dot(order, raw_in[...].reshape(rows, width)).astype(BF16)

    for h in range(2):
        use, lanes = slice(h * hw, (h + 1) * hw), slice(h * half, (h + 1) * half)
        drive_re[:, lanes] = dot(inputs[:, use], wide_re[use, :])
        drive_im[:, lanes] = dot(inputs[:, use], wide_im[use, :])

    span = 512

    def scan(first, keep):
        @pl.loop(0, modes // span)
        def _(c):
            lanes = pl.ds(pl.multiple_of(c * span, span), span)
            lr = jnp.broadcast_to(vec[0:1, lanes], (CHUNKS, span))
            li = jnp.broadcast_to(vec[1:2, lanes], (CHUNKS, span))
            if first is None:
                start = (jnp.zeros((CHUNKS, span), F32), jnp.zeros((CHUNKS, span), F32))
            else:
                start = (first[0, :, lanes], first[1, :, lanes])

            def body(t, now):
                re, im = now
                at = pl.ds(pl.multiple_of(t * 16, 16), 16)
                m, dr, di = mags[at, lanes], drive_re[at, lanes], drive_im[at, lanes]
                kept = []
                for u in range(2):
                    use = slice(u * CHUNKS, (u + 1) * CHUNKS)
                    ar, ai = m[use] * lr, m[use] * li
                    re, im = ar * re - ai * im + dr[use], ar * im + ai * re + di[use]
                    kept.append((re, im))
                if keep:
                    states_re[at, lanes] = jnp.concatenate([k[0] for k in kept], axis=0).astype(BF16)
                    states_im[at, lanes] = jnp.concatenate([k[1] for k in kept], axis=0).astype(BF16)
                return re, im

            re, im = lax.fori_loop(0, steps // 2, body, start)
            if not keep:
                ends[0, :, lanes] = re
                ends[1, :, lanes] = im

    scan(None, False)

    place = iota((CHUNKS, modes), 0) & (quarters - 1)
    grown = jnp.exp(vec[pl.ds(16, CHUNKS), :])
    a = (grown * vec[2:3, :], grown * vec[3:4, :])
    b = (ends[0], ends[1])
    d = 1
    while d < quarters:
        ok = place >= d
        a_old = tuple(pltpu.roll(v, d, axis=0) for v in a)
        b_old = tuple(pltpu.roll(v, d, axis=0) for v in b)
        add = cmul(a, b_old)
        new_a = cmul(a, a_old)
        b = tuple(jnp.where(ok, v + w, v) for v, w in zip(b, add))
        a = tuple(jnp.where(ok, w, v) for v, w in zip(a, new_a))
        d *= 2
    for c in range(2):
        for s in range(sequences):
            last = (s + 1) * quarters - 1
            for k in range(nx):
                for blk in range(blocks):
                    lo = k * part + blk * LANES
                    row = c * tile + s * blocks + blk
                    sum_stage[k, row : row + 1, :] = b[c][last : last + 1, lo : lo + LANES]
    sum_pack[...] = sum_stage[...].astype(BF16)
    for i, (value, empty) in enumerate(((a[0], 1.0), (a[1], 0.0), (b[0], 0.0), (b[1], 0.0))):
        before[i] = jnp.where(place == 0, empty, pltpu.roll(value, 1, axis=0))
    sum_sends = to_x(sum_pack, sum_x, sx_send, sx_recv)
    for copy in sum_sends:
        copy.start()
    sum_x[pl.ds(mx, 1)] = sum_pack[pl.ds(mx, 1)]

    for copy in log_sends:
        copy.wait()
    log_row[...] = jnp.sum(log_x[...], axis=0)
    log_z_sends = to_z(log_row, log_z, lz_send, lz_recv)
    start_z(log_z_sends)
    for c in range(2):
        for blk in range(blocks):
            lanes = pl.ds(pl.multiple_of(mx * part + blk * LANES, LANES), LANES)
            value = vec[4 + c : 5 + c, lanes]
            for s in range(sequences):
                row = s * blocks + blk
                lam_pack[c, row : row + 1, :] = value
    lam_dev = (lam_pack[0], lam_pack[1])
    one = (jnp.ones((tile, LANES), F32), jnp.zeros((tile, LANES), F32))
    lam_pow = [one]
    for _ in range(nx):
        lam_pow.append(cmul(lam_pow[-1], lam_dev))

    def grow(logs, base):
        size = jnp.exp(logs)
        return size * base[0], size * base[1]

    def halves(value):
        wide = value.astype(F32)
        return wide[:tile], wide[tile:]

    def plus(u, v):
        return u[0] + v[0], u[1] + v[1]

    logs = [log_x[k] for k in range(nx)]
    to_end, to_start = [None] * nx, [None] * nx
    gone = jnp.zeros((tile, LANES), F32)
    for k in range(nx - 1, -1, -1):
        to_end[k] = grow(gone, lam_pow[nx - 1 - k])
        gone = gone + logs[k]
    gone = jnp.zeros((tile, LANES), F32)
    for k in range(nx):
        to_start[k] = grow(gone, lam_pow[k])
        gone = gone + logs[k]

    loads[9].wait()
    project(tp, gate_w, raw_gate)

    for copy in sum_sends:
        copy.wait()
    came = [halves(sum_x[k]) for k in range(nx)]
    total = cmul(to_end[0], came[0])
    for k in range(1, nx):
        total = plus(total, cmul(to_end[k], came[k]))
    sum_row[...] = jnp.concatenate(total, axis=0).astype(BF16)
    sum_z_sends = to_z(sum_row, sum_z, sz_send, sz_recv)
    start_z(sum_z_sends)
    w_copy = remote(out_w_hbm, out_w.at[tp], w_send, w_recv, partner)
    w_copy.start()

    project(1 - tp, gate_w, raw_gate)
    gates = dot(scan_order(rows), raw_gate[...].reshape(rows, width))
    opened[...] = 1.0 / (1.0 + jnp.exp(-gates))

    for copy in loads[10:14]:
        copy.wait()
    two_re, two_im = doubled(read_re_ref[...]), doubled(read_im_ref[...])

    def coef(g):
        lo = g // per_tile * LANES
        return vec[6:7, lo : lo + LANES], vec[7:8, lo : lo + LANES]

    def lifted_re(g, at):
        kr, ki = coef(g)
        return two_re[at] * kr - two_im[at] * ki

    def lifted_im(g, at):
        kr, ki = coef(g)
        return -(two_re[at] * ki + two_im[at] * kr)

    block_diagonal(lift_re, lifted_re)
    block_diagonal(lift_im, lifted_im)

    inside = [None] * nx
    inside[0] = (jnp.zeros((tile, LANES), F32), jnp.zeros((tile, LANES), F32))
    for k in range(1, nx):
        inside[k] = plus(cmul(inside[k - 1], grow(logs[k - 1], lam_dev)), came[k - 1])
    recv_z(log_z_sends)
    weights = {}
    gone, power = jnp.zeros((tile, LANES), F32), one
    for d in range(1, nz):
        weights[d] = grow(gone, power)
        gone = gone + log_z[d - 1]
        power = cmul(power, lam_pow[nx])

    recv_z(sum_z_sends)
    carry = inside[0]
    for d in range(1, nz):
        carry = plus(carry, cmul(weights[d], halves(sum_z[d - 1])))
    for k in range(nx):
        carry_pack[k] = jnp.concatenate(plus(cmul(carry, to_start[k]), inside[k]), axis=0).astype(BF16)
    carry_sends = to_x(carry_pack, carry_x, cx_send, cx_recv)
    for copy in carry_sends:
        copy.start()
    carry_x[pl.ds(mx, 1)] = carry_pack[pl.ds(mx, 1)]
    for copy in carry_sends:
        copy.wait()
    upper = iota((CHUNKS, LANES), 0) < quarters
    for k in range(nx):
        got = carry_x[k].astype(F32)
        for blk in range(blocks):
            lo = k * part + blk * LANES
            lanes = slice(lo, lo + LANES)
            into = tuple(
                jnp.where(upper, got[c * tile + blk][None], got[c * tile + blocks + blk][None]) for c in range(2)
            )
            moved = cmul((before[0, :, lanes], before[1, :, lanes]), into)
            init[0, :, lanes] = before[2, :, lanes] + moved[0]
            init[1, :, lanes] = before[3, :, lanes] + moved[1]

    scan(init, True)

    parts = []
    for h in range(2):
        use = slice(h * hw, (h + 1) * hw)
        lanes = slice(h * half, (h + 1) * half)
        mixed = dot_t(states_re[:, lanes], lift_re[use, :]) + dot_t(states_im[:, lanes], lift_im[use, :])
        mixed = mixed + skip_ref[:, use] * inputs[:, use].astype(F32)
        gelu = 0.5 * mixed * (1.0 + lax.erf(mixed * math.sqrt(0.5)))
        parts.append((gelu * opened[:, use]).astype(BF16))
    back = natural_order(rows)
    for h in range(2):
        act[:, :, h * hw : (h + 1) * hw] = dot(back, parts[h]).astype(BF16).reshape(sequences, 2 * own, hw)
    a_copy = remote(act.at[:, theirs, :], act_in, a_send, a_recv, partner)
    a_copy.start()
    near = act[:, mine, :].astype(F32).reshape(sequences * own, width)
    near_square = jnp.sum(near * near, axis=-1, keepdims=True)
    near = (near * gain_ref[:, pl.ds(pl.multiple_of(tp * width, width), width)]).astype(BF16)
    loads[14].wait()
    for c in range(depth // 256):
        lanes = slice(c * 256, (c + 1) * 256)
        near_sum[:, lanes] = dot(near, out_w[tp, :, lanes])
    w_copy.wait()
    a_copy.wait()
    far = act_in[...].astype(F32).reshape(sequences * own, width)
    scale = lax.rsqrt((near_square + jnp.sum(far * far, axis=-1, keepdims=True)) * (0.5 / width) + EPS)
    far = (far * gain_ref[:, pl.ds(pl.multiple_of((1 - tp) * width, width), width)]).astype(BF16)
    for c in range(depth // 256):
        lanes = slice(c * 256, (c + 1) * 256)
        result = (near_sum[:, lanes] + dot(far, out_w[1 - tp, :, lanes])) * scale
        out_ref[:, :, lanes] = result.astype(BF16).reshape(sequences, own, 256)

    sent_z(log_z_sends)
    sent_z(sum_z_sends)


def vmem():
    return pl.BlockSpec(memory_space=pltpu.VMEM)


def hbm():
    return pl.BlockSpec(memory_space=pl.ANY)


def shards(
    layer_input,
    norm_gain,
    in_weight,
    gate_weight,
    rate_real,
    rate_imag,
    log_step,
    input_real,
    input_imag,
    output_real,
    output_imag,
    skip_weight,
    decay_offset,
    channel_gain,
    out_weight,
):
    nz, nx = lax.axis_size("sp_0"), lax.axis_size("sp_1")
    sequences, own, depth = layer_input.shape
    width = in_weight.shape[1]
    groups, states = rate_real.shape
    modes = groups * states
    rows = sequences * 2 * own
    dma = pltpu.SemaphoreType.DMA
    tile = sequences * (modes // nx // LANES)
    f32 = functools.partial(pltpu.VMEM, dtype=F32)
    b16 = functools.partial(pltpu.VMEM, dtype=BF16)
    return pl.pallas_call(
        mixer_kernel,
        name="mixer",
        out_shape=jax.ShapeDtypeStruct((sequences, own, depth), BF16),
        in_specs=[hbm()] * 15,
        out_specs=vmem(),
        scratch_shapes=[
            b16((sequences, 2 * own, depth)),
            b16((depth, width)),
            b16((depth, width)),
            b16((2, width, depth)),
            f32((1, depth)),
            f32((groups, states)),
            f32((groups, states)),
            f32((1, groups)),
            b16((width, states)),
            b16((width, states)),
            b16((width, states)),
            b16((width, states)),
            f32((1, width)),
            f32((sequences, groups, 2 * own)),
            f32((1, 2 * width)),
            b16((2, sequences * own, depth)),
            b16((sequences, 2 * own, width)),
            b16((sequences, 2 * own, width)),
            b16((rows, width)),
            f32((rows, width)),
            f32((rows, modes)),
            b16((width, modes // 2)),
            b16((width, modes // 2)),
            f32((rows, modes)),
            f32((rows, modes)),
            b16((rows, modes)),
            b16((rows, modes)),
            b16((width, modes // 2)),
            b16((width, modes // 2)),
            f32((24, modes)),
            f32((2, CHUNKS, modes)),
            f32((4, CHUNKS, modes)),
            f32((2, CHUNKS, modes)),
            f32((nx, tile, LANES)),
            f32((nx, tile, LANES)),
            f32((tile, LANES)),
            f32((nz - 1, tile, LANES)),
            f32((nx, 2 * tile, LANES)),
            b16((nx, 2 * tile, LANES)),
            b16((nx, 2 * tile, LANES)),
            b16((2 * tile, LANES)),
            b16((nz - 1, 2 * tile, LANES)),
            b16((nx, 2 * tile, LANES)),
            b16((nx, 2 * tile, LANES)),
            f32((2, tile, LANES)),
            b16((sequences, 2 * own, width)),
            b16((sequences, own, width)),
            f32((sequences * own, depth)),
            dma((15,)),
            dma,
            dma,
            dma,
            dma,
            dma((nx - 1,)),
            dma((nx - 1,)),
            dma((nz - 1,)),
            dma((nz - 1,)),
            dma((nx - 1,)),
            dma((nx - 1,)),
            dma((nz - 1,)),
            dma((nz - 1,)),
            dma((nx - 1,)),
            dma((nx - 1,)),
            dma,
            dma,
        ],
        compiler_params=pltpu.CompilerParams(collective_id=0, has_side_effects=True),
    )(
        layer_input,
        in_weight,
        gate_weight,
        out_weight,
        norm_gain[None],
        rate_real,
        rate_imag,
        log_step[None],
        jnp.swapaxes(input_real, 1, 2).reshape(width, states),
        jnp.swapaxes(input_imag, 1, 2).reshape(width, states),
        output_real.reshape(width, states),
        output_imag.reshape(width, states),
        skip_weight[None],
        jnp.swapaxes(decay_offset, 1, 2),
        channel_gain[None],
    )


def solution(mesh):
    torus = Mesh(
        mesh.devices.reshape(mesh.shape["grp"], 16, 4, mesh.shape["tp"]),
        ("grp", "sp_0", "sp_1", "tp"),
    )
    return build(torus)


def build(torus):
    in_specs = (
        P("grp", SP_TP, None),
        P(),
        P(None, "tp"),
        P(None, "tp"),
        P("tp", None),
        P("tp", None),
        P("tp"),
        P("tp", None, None),
        P("tp", None, None),
        P("tp", None, None),
        P("tp", None, None),
        P("tp"),
        P("grp", SP, "tp"),
        P(),
        P("tp", None),
    )
    out_specs = P("grp", SP_TP, None)
    return jax.shard_map(shards, mesh=torus, in_specs=in_specs, out_specs=out_specs, check_vma=False)
```

```python
import functools
import math

import jax
import jax.numpy as jnp
from jax import lax
from jax.experimental import pallas as pl
from jax.experimental.pallas import tpu as pltpu
from jax.sharding import Mesh
from jax.sharding import PartitionSpec as P

SP = ("sp_0", "sp_1")
SP_TP = ("sp_0", "sp_1", "tp")
MESH = pl.DeviceIdType.MESH
F32 = jnp.float32
BF16 = jnp.bfloat16
EPS = 1e-06
LANES = 128
CHUNKS = 8


def dot(a, b):
    return jnp.dot(a, b, preferred_element_type=F32)


def dot_t(a, b):
    return lax.dot_general(a, b, (((1,), (1,)), ((), ())), preferred_element_type=F32)


def iota(shape, dim):
    return lax.broadcasted_iota(jnp.int32, shape, dim)


def one_hot(cond):
    return jnp.where(cond, 1.0, 0.0).astype(BF16)


def split(value):
    high = value.astype(BF16)
    rest = value - high.astype(F32)
    middle = rest.astype(BF16)
    low = (rest - middle.astype(F32)).astype(BF16)
    return high, middle, low


def exact_dot(value, table):
    high, middle, low = split(value)
    return dot(high, table) + dot(middle, table) + dot(low, table)


def cmul(a, b):
    return a[0] * b[0] - a[1] * b[1], a[0] * b[1] + a[1] * b[0]


def small_expm1(x):
    series = x * (1.0 + x * (1 / 2 + x * (1 / 6 + x * (1 / 24 + x * (1 / 120 + x * (1 / 720 + x / 5040))))))
    return jnp.where(x > -0.3, series, jnp.exp(x) - 1.0)


def scan_order(rows):
    steps = rows // CHUNKS
    at = iota((rows, rows), 0)
    return one_hot(iota((rows, rows), 1) == (at & (CHUNKS - 1)) * steps + (at >> 3))


def natural_order(rows):
    steps = rows // CHUNKS
    at = iota((rows, rows), 1)
    return one_hot(iota((rows, rows), 0) == (at & (CHUNKS - 1)) * steps + (at >> 3))


def small_sine(x):
    q = x * x
    return x * (1.0 + q * (-1 / 6 + q * (1 / 120 + q * (-1 / 5040 + q * (1 / 362880 - q / 39916800)))))


def small_cosine(x):
    q = x * x
    return 1.0 + q * (-1 / 2 + q * (1 / 24 + q * (-1 / 720 + q * (1 / 40320 + q * (-1 / 3628800 + q / 479001600)))))


def mixer_kernel(
    x_hbm,
    in_w_hbm,
    gate_w_hbm,
    out_w_hbm,
    norm_gain_hbm,
    rate_re_hbm,
    rate_im_hbm,
    log_step_hbm,
    table_re_hbm,
    table_im_hbm,
    read_re_hbm,
    read_im_hbm,
    skip_hbm,
    offset_hbm,
    near_ref,
    far_ref,
    far_w_ref,
    tokens,
    in_w,
    gate_w,
    norm_gain_ref,
    rate_re_ref,
    rate_im_ref,
    log_step_ref,
    table_re_ref,
    table_im_ref,
    read_re_ref,
    read_im_ref,
    skip_ref,
    offset_ref,
    normed,
    scales,
    raw_in,
    raw_gate,
    inputs,
    opened,
    mags,
    wide_re,
    wide_im,
    drive_re,
    drive_im,
    states_re,
    states_im,
    lift_re,
    lift_im,
    vec,
    ends,
    before,
    init,
    log_pack,
    log_x,
    log_row,
    log_z,
    sum_stage,
    sum_pack,
    sum_x,
    sum_row,
    sum_z,
    carry_pack,
    carry_x,
    lam_pack,
    act,
    load_sem,
    x_send,
    x_recv,
    w_send,
    w_recv,
    lx_send,
    lx_recv,
    lz_send,
    lz_recv,
    sx_send,
    sx_recv,
    sz_send,
    sz_recv,
    cx_send,
    cx_recv,
    a_send,
    a_recv,
):
    nz, nx = lax.axis_size("sp_0"), lax.axis_size("sp_1")
    mz, mx, tp = lax.axis_index("sp_0"), lax.axis_index("sp_1"), lax.axis_index("tp")
    sequences, own, depth = x_hbm.shape
    width = in_w_hbm.shape[1]
    rows = sequences * 2 * own
    groups, states = rate_re_hbm.shape
    channels = width // groups
    modes = groups * states
    steps = rows // CHUNKS
    quarters = CHUNKS // sequences
    part = modes // nx
    blocks = part // LANES
    tile = sequences * blocks
    half = modes // 2
    hw = width // 2
    mine = pl.ds(pl.multiple_of(tp * own, own), own)
    theirs = pl.ds(pl.multiple_of((1 - tp) * own, own), own)
    partner = {"tp": 1 - tp}

    loads = [
        pltpu.make_async_copy(source, target, load_sem.at[i])
        for i, (source, target) in enumerate(
            (
                (x_hbm, tokens.at[:, mine, :]),
                (offset_hbm, offset_ref),
                (rate_re_hbm, rate_re_ref),
                (rate_im_hbm, rate_im_ref),
                (log_step_hbm, log_step_ref),
                (norm_gain_hbm, norm_gain_ref),
                (table_re_hbm, table_re_ref),
                (table_im_hbm, table_im_ref),
                (in_w_hbm, in_w),
                (gate_w_hbm, gate_w),
                (read_re_hbm, read_re_ref),
                (read_im_hbm, read_im_ref),
                (skip_hbm, skip_ref),
            )
        )
    ]
    for copy in loads:
        copy.start()

    log_z[...] = jnp.zeros_like(log_z)
    sum_z[...] = jnp.zeros_like(sum_z)
    barrier = pltpu.get_barrier_semaphore()
    pl.semaphore_signal(barrier, inc=1, device_id=partner, device_id_type=MESH)
    for d in range(1, nx):
        pl.semaphore_signal(barrier, inc=1, device_id={"sp_1": lax.rem(mx + d, nx)}, device_id_type=MESH)
    far_first = sorted(range(1, nz), key=lambda d: -min(d, nz - d))
    for d in far_first:
        pl.semaphore_signal(barrier, inc=1, device_id={"sp_0": lax.rem(mz + d, nz)}, device_id_type=MESH)

    def remote(source, target, send, recv, device):
        return pltpu.make_async_remote_copy(
            src_ref=source, dst_ref=target, send_sem=send, recv_sem=recv, device_id=device, device_id_type=MESH
        )

    def to_x(source, target, send, recv):
        made = []
        for d in range(1, nx):
            k = lax.rem(mx + d, nx)
            made.append(remote(source.at[k], target.at[mx], send.at[d - 1], recv.at[d - 1], {"sp_1": k}))
        return made

    def to_z(source, target, send, recv):
        return {
            d: remote(source, target.at[d - 1], send.at[d - 1], recv.at[d - 1], {"sp_0": lax.rem(mz + d, nz)})
            for d in far_first
        }

    def start_z(made):
        for d, copy in made.items():
            pl.when(mz + d < nz)(copy.start)

    def recv_z(made):
        for d, copy in made.items():
            pl.when(d <= mz)(copy.wait_recv)

    def sent_z(made):
        for d, copy in made.items():
            pl.when(mz + d < nz)(copy.wait_send)

    for copy in loads[1:6]:
        copy.wait()
    spread_g = one_hot((iota((groups, modes), 1) >> 6) == iota((groups, modes), 0))
    spread_p = one_hot((iota((states, modes), 1) & (states - 1)) == iota((states, modes), 0))
    offsets = jnp.concatenate([offset_ref[s].T for s in range(sequences)], axis=0)
    sums = jnp.sum(offsets.reshape(CHUNKS, steps, groups), axis=1)
    step_size = jnp.broadcast_to(jnp.exp(log_step_ref[...]), (8, groups))
    spread = exact_dot(jnp.concatenate([sums, step_size], axis=0), spread_g)
    chunk_logs, step = spread[:CHUNKS], spread[CHUNKS : CHUNKS + 1]
    vec[pl.ds(16, CHUNKS), :] = chunk_logs
    for s in range(sequences):
        total = jnp.sum(chunk_logs[s * quarters : (s + 1) * quarters], axis=0, keepdims=True)
        for k in range(nx):
            for b in range(blocks):
                lo = k * part + b * LANES
                row = s * blocks + b
                log_pack[k, row : row + 1, :] = total[:, lo : lo + LANES]

    def norm(side):
        per = own // 32

        @pl.loop(0, sequences * per)
        def _(i):
            s = i // per
            row = pl.multiple_of(side * own + (i % per) * 32, 32)
            wide = tokens[s, pl.ds(row, 32), :].astype(F32)
            at = pl.ds(pl.multiple_of(i * 32, 32), 32)
            normed[side, at, :] = (wide * norm_gain_ref[...]).astype(BF16)
            scale = lax.rsqrt(jnp.mean(wide * wide, axis=-1, keepdims=True) + EPS)
            scales[side, at, :] = jnp.broadcast_to(scale, (32, 256))

    def project(side, weight, out):
        @pl.loop(0, width // 256)
        def _(c):
            lanes = pl.ds(pl.multiple_of(c * 256, 256), 256)
            product = dot(normed[side], weight[:, lanes]) * scales[side]
            at = pl.ds(pl.multiple_of(side * own, own), own)
            out[:, at, lanes] = product.reshape(sequences, own, 256).astype(BF16)

    loads[0].wait()
    norm(tp)
    loads[8].wait()
    project(tp, in_w, raw_in)

    on_group = (iota((groups, modes), 1) >> 6) == iota((groups, modes), 0)
    rates = exact_dot(jnp.concatenate([rate_re_ref[...], rate_im_ref[...]], axis=0), spread_p)
    rate_re = jnp.sum(jnp.where(on_group, rates[:groups], 0.0), axis=0, keepdims=True)
    rate_im = jnp.sum(jnp.where(on_group, rates[groups:], 0.0), axis=0, keepdims=True)
    real_step, angle = rate_re * step, rate_im * step
    size = jnp.exp(real_step)
    cosine, sine = small_cosine(angle), small_sine(angle)
    half_sine = small_sine(0.5 * angle)
    top_re = small_expm1(real_step) * cosine - 2.0 * half_sine * half_sine
    top_im = size * sine
    inverse = 1.0 / (rate_re * rate_re + rate_im * rate_im)
    coef_re = (top_re * rate_re + top_im * rate_im) * inverse
    coef_im = (top_im * rate_re - top_re * rate_im) * inverse
    lam = (size * cosine, size * sine)
    power = lam
    for _ in range(int(math.log2(steps))):
        power = cmul(power, power)
    lam_chunk = power
    for _ in range(int(math.log2(quarters))):
        power = cmul(power, power)
    for i, value in enumerate((*lam, *lam_chunk, *power, coef_re, coef_im)):
        vec[i : i + 1, :] = value

    order = scan_order(rows)
    pieces = [dot(order, piece) for piece in split(jnp.exp(offsets))]
    spread_3 = one_hot((iota((3 * groups, modes), 1) >> 6) == (iota((3 * groups, modes), 0) & (groups - 1)))
    mags[...] = dot(jnp.concatenate(pieces, axis=1).astype(BF16), spread_3)

    per_tile = LANES // states

    def doubled(value):
        return jnp.concatenate([value.astype(F32)] * per_tile, axis=1)

    on_lane = iota((channels, LANES), 1) // states

    def block_diagonal(target, value):
        target[...] = jnp.zeros_like(target)
        for g in range(groups):
            at = slice(g * channels, (g + 1) * channels)
            lo = (g % (groups // 2)) // per_tile * LANES
            kept = jnp.where(on_lane == g % per_tile, value(g, at), 0.0)
            target[at, lo : lo + LANES] = kept.astype(BF16)

    for copy in loads[6:8]:
        copy.wait()
    two_re, two_im = doubled(table_re_ref[...]), doubled(table_im_ref[...])
    block_diagonal(wide_re, lambda g, at: two_re[at])
    block_diagonal(wide_im, lambda g, at: two_im[at])

    pl.semaphore_wait(barrier, nx + nz - 1)
    x_copy = remote(x_hbm, tokens.at[:, mine, :], x_send, x_recv, partner)
    x_copy.start()
    log_sends = to_x(log_pack, log_x, lx_send, lx_recv)
    for copy in log_sends:
        copy.start()
    log_x[pl.ds(mx, 1)] = log_pack[pl.ds(mx, 1)]

    x_copy.wait()
    norm(1 - tp)
    project(1 - tp, in_w, raw_in)
    inputs[...] = dot(order, raw_in[...].reshape(rows, width)).astype(BF16)

    for h in range(2):
        use, lanes = slice(h * hw, (h + 1) * hw), slice(h * half, (h + 1) * half)
        drive_re[:, lanes] = dot(inputs[:, use], wide_re[use, :])
        drive_im[:, lanes] = dot(inputs[:, use], wide_im[use, :])

    for copy in log_sends:
        copy.wait()
    log_row[...] = jnp.sum(log_x[...], axis=0)
    log_z_sends = to_z(log_row, log_z, lz_send, lz_recv)
    start_z(log_z_sends)

    span = 512

    def scan(first, keep):
        @pl.loop(0, modes // span)
        def _(c):
            lanes = pl.ds(pl.multiple_of(c * span, span), span)
            lr = jnp.broadcast_to(vec[0:1, lanes], (CHUNKS, span))
            li = jnp.broadcast_to(vec[1:2, lanes], (CHUNKS, span))
            if first is None:
                start = (jnp.zeros((CHUNKS, span), F32), jnp.zeros((CHUNKS, span), F32))
            else:
                start = (first[0, :, lanes], first[1, :, lanes])

            def body(t, now):
                re, im = now
                at = pl.ds(pl.multiple_of(t * 4 * CHUNKS, 4 * CHUNKS), 4 * CHUNKS)
                m, dr, di = mags[at, lanes], drive_re[at, lanes], drive_im[at, lanes]
                kept = []
                for u in range(4):
                    use = slice(u * CHUNKS, (u + 1) * CHUNKS)
                    ar, ai = m[use] * lr, m[use] * li
                    re, im = ar * re - ai * im + dr[use], ar * im + ai * re + di[use]
                    kept.append((re, im))
                if keep:
                    states_re[at, lanes] = jnp.concatenate([k[0] for k in kept], axis=0).astype(BF16)
                    states_im[at, lanes] = jnp.concatenate([k[1] for k in kept], axis=0).astype(BF16)
                return re, im

            re, im = lax.fori_loop(0, steps // 4, body, start)
            if not keep:
                ends[0, :, lanes] = re
                ends[1, :, lanes] = im

    scan(None, False)

    place = iota((CHUNKS, modes), 0) & (quarters - 1)
    grown = jnp.exp(vec[pl.ds(16, CHUNKS), :])
    a = (grown * vec[2:3, :], grown * vec[3:4, :])
    b = (ends[0], ends[1])
    d = 1
    while d < quarters:
        ok = place >= d
        a_old = tuple(pltpu.roll(v, d, axis=0) for v in a)
        b_old = tuple(pltpu.roll(v, d, axis=0) for v in b)
        add = cmul(a, b_old)
        new_a = cmul(a, a_old)
        b = tuple(jnp.where(ok, v + w, v) for v, w in zip(b, add))
        a = tuple(jnp.where(ok, w, v) for v, w in zip(a, new_a))
        d *= 2
    for c in range(2):
        for s in range(sequences):
            last = (s + 1) * quarters - 1
            for k in range(nx):
                for blk in range(blocks):
                    lo = k * part + blk * LANES
                    row = c * tile + s * blocks + blk
                    sum_stage[k, row : row + 1, :] = b[c][last : last + 1, lo : lo + LANES]
    sum_pack[...] = sum_stage[...].astype(BF16)
    for i, (value, empty) in enumerate(((a[0], 1.0), (a[1], 0.0), (b[0], 0.0), (b[1], 0.0))):
        before[i] = jnp.where(place == 0, empty, pltpu.roll(value, 1, axis=0))
    sum_sends = to_x(sum_pack, sum_x, sx_send, sx_recv)
    for copy in sum_sends:
        copy.start()
    sum_x[pl.ds(mx, 1)] = sum_pack[pl.ds(mx, 1)]

    for c in range(2):
        for blk in range(blocks):
            lanes = pl.ds(pl.multiple_of(mx * part + blk * LANES, LANES), LANES)
            value = vec[4 + c : 5 + c, lanes]
            for s in range(sequences):
                row = s * blocks + blk
                lam_pack[c, row : row + 1, :] = value
    lam_dev = (lam_pack[0], lam_pack[1])
    one = (jnp.ones((tile, LANES), F32), jnp.zeros((tile, LANES), F32))
    lam_pow = [one]
    for _ in range(nx):
        lam_pow.append(cmul(lam_pow[-1], lam_dev))

    def grow(logs, base):
        size = jnp.exp(logs)
        return size * base[0], size * base[1]

    def halves(value):
        wide = value.astype(F32)
        return wide[:tile], wide[tile:]

    def plus(u, v):
        return u[0] + v[0], u[1] + v[1]

    logs = [log_x[k] for k in range(nx)]
    to_end, to_start = [None] * nx, [None] * nx
    gone = jnp.zeros((tile, LANES), F32)
    for k in range(nx - 1, -1, -1):
        to_end[k] = grow(gone, lam_pow[nx - 1 - k])
        gone = gone + logs[k]
    gone = jnp.zeros((tile, LANES), F32)
    for k in range(nx):
        to_start[k] = grow(gone, lam_pow[k])
        gone = gone + logs[k]

    loads[9].wait()
    project(tp, gate_w, raw_gate)
    project(1 - tp, gate_w, raw_gate)
    gates = dot(scan_order(rows), raw_gate[...].reshape(rows, width))
    opened[...] = 1.0 / (1.0 + jnp.exp(-gates))

    for copy in loads[10:13]:
        copy.wait()
    two_re, two_im = doubled(read_re_ref[...]), doubled(read_im_ref[...])

    def coef(g):
        lo = g // per_tile * LANES
        return vec[6:7, lo : lo + LANES], vec[7:8, lo : lo + LANES]

    def lifted_re(g, at):
        kr, ki = coef(g)
        return two_re[at] * kr - two_im[at] * ki

    def lifted_im(g, at):
        kr, ki = coef(g)
        return -(two_re[at] * ki + two_im[at] * kr)

    block_diagonal(lift_re, lifted_re)
    block_diagonal(lift_im, lifted_im)

    for copy in sum_sends:
        copy.wait()
    came = [halves(sum_x[k]) for k in range(nx)]
    total = cmul(to_end[0], came[0])
    for k in range(1, nx):
        total = plus(total, cmul(to_end[k], came[k]))
    sum_row[...] = jnp.concatenate(total, axis=0).astype(BF16)
    sum_z_sends = to_z(sum_row, sum_z, sz_send, sz_recv)
    start_z(sum_z_sends)
    w_copy = remote(out_w_hbm, far_w_ref, w_send, w_recv, partner)
    w_copy.start()

    inside = [None] * nx
    inside[0] = (jnp.zeros((tile, LANES), F32), jnp.zeros((tile, LANES), F32))
    for k in range(1, nx):
        inside[k] = plus(cmul(inside[k - 1], grow(logs[k - 1], lam_dev)), came[k - 1])
    recv_z(log_z_sends)
    weights = {}
    gone, power = jnp.zeros((tile, LANES), F32), one
    for d in range(1, nz):
        weights[d] = grow(gone, power)
        gone = gone + log_z[d - 1]
        power = cmul(power, lam_pow[nx])

    recv_z(sum_z_sends)
    carry = inside[0]
    for d in range(1, nz):
        carry = plus(carry, cmul(weights[d], halves(sum_z[d - 1])))
    for k in range(nx):
        carry_pack[k] = jnp.concatenate(plus(cmul(carry, to_start[k]), inside[k]), axis=0).astype(BF16)
    carry_sends = to_x(carry_pack, carry_x, cx_send, cx_recv)
    for copy in carry_sends:
        copy.start()
    carry_x[pl.ds(mx, 1)] = carry_pack[pl.ds(mx, 1)]
    for copy in carry_sends:
        copy.wait()
    upper = iota((CHUNKS, LANES), 0) < quarters
    for k in range(nx):
        got = carry_x[k].astype(F32)
        for blk in range(blocks):
            lo = k * part + blk * LANES
            lanes = slice(lo, lo + LANES)
            into = tuple(
                jnp.where(upper, got[c * tile + blk][None], got[c * tile + blocks + blk][None]) for c in range(2)
            )
            moved = cmul((before[0, :, lanes], before[1, :, lanes]), into)
            init[0, :, lanes] = before[2, :, lanes] + moved[0]
            init[1, :, lanes] = before[3, :, lanes] + moved[1]

    scan(init, True)

    parts = []
    for h in range(2):
        use = slice(h * hw, (h + 1) * hw)
        lanes = slice(h * half, (h + 1) * half)
        mixed = dot_t(states_re[:, lanes], lift_re[use, :]) + dot_t(states_im[:, lanes], lift_im[use, :])
        mixed = mixed + skip_ref[:, use] * inputs[:, use].astype(F32)
        gelu = 0.5 * mixed * (1.0 + lax.erf(mixed * math.sqrt(0.5)))
        parts.append((gelu * opened[:, use]).astype(BF16))
    back = natural_order(rows)
    for h in range(2):
        act[:, :, h * hw : (h + 1) * hw] = dot(back, parts[h]).astype(BF16).reshape(sequences, 2 * own, hw)
    a_copy = remote(act.at[:, theirs, :], far_ref, a_send, a_recv, partner)
    a_copy.start()
    near_ref[...] = act[:, mine, :]
    w_copy.wait()
    a_copy.wait()

    sent_z(log_z_sends)
    sent_z(sum_z_sends)


def finish_kernel(near_ref, far_ref, gain_ref, near_w_ref, far_w_ref, out_hbm, staged, sem):
    tp = lax.axis_index("tp")
    sequences, own, width = near_ref.shape
    depth = near_w_ref.shape[1]

    def side(ref, which):
        wide = ref[...].astype(F32).reshape(sequences * own, width)
        gain = gain_ref[:, pl.ds(pl.multiple_of(which * width, width), width)]
        return (wide * gain).astype(BF16), jnp.sum(wide * wide, axis=-1, keepdims=True)

    near, near_square = side(near_ref, tp)
    far, far_square = side(far_ref, 1 - tp)
    scale = lax.rsqrt((near_square + far_square) * (0.5 / width) + EPS)
    copies = []
    for c in range(depth // 512):
        lanes = slice(c * 512, (c + 1) * 512)
        result = (dot(near, near_w_ref[:, lanes]) + dot(far, far_w_ref[:, lanes])) * scale
        staged[:, :, lanes] = result.astype(BF16).reshape(sequences, own, 512)
        copies.append(pltpu.make_async_copy(staged.at[:, :, lanes], out_hbm.at[:, :, lanes], sem.at[c]))
        copies[-1].start()
    for copy in copies:
        copy.wait()


def vmem():
    return pl.BlockSpec(memory_space=pltpu.VMEM)


def hbm():
    return pl.BlockSpec(memory_space=pl.ANY)


def shards(
    layer_input,
    norm_gain,
    in_weight,
    gate_weight,
    rate_real,
    rate_imag,
    log_step,
    input_real,
    input_imag,
    output_real,
    output_imag,
    skip_weight,
    decay_offset,
    channel_gain,
    out_weight,
):
    nz, nx = lax.axis_size("sp_0"), lax.axis_size("sp_1")
    sequences, own, depth = layer_input.shape
    width = in_weight.shape[1]
    groups, states = rate_real.shape
    modes = groups * states
    rows = sequences * 2 * own
    dma = pltpu.SemaphoreType.DMA
    tile = sequences * (modes // nx // LANES)
    f32 = functools.partial(pltpu.VMEM, dtype=F32)
    b16 = functools.partial(pltpu.VMEM, dtype=BF16)
    near, far, far_w = pl.pallas_call(
        mixer_kernel,
        name="mixer",
        out_shape=[
            pltpu.VMEM((sequences, own, width), BF16),
            pltpu.VMEM((sequences, own, width), BF16),
            pltpu.VMEM((width, depth), BF16),
        ],
        in_specs=[pl.BlockSpec(memory_space=pltpu.HBM)] * 14,
        out_specs=[vmem()] * 3,
        scratch_shapes=[
            b16((sequences, 2 * own, depth)),
            b16((depth, width)),
            b16((depth, width)),
            f32((1, depth)),
            f32((groups, states)),
            f32((groups, states)),
            f32((1, groups)),
            b16((width, states)),
            b16((width, states)),
            b16((width, states)),
            b16((width, states)),
            f32((1, width)),
            f32((sequences, groups, 2 * own)),
            b16((2, sequences * own, depth)),
            f32((2, sequences * own, 256)),
            b16((sequences, 2 * own, width)),
            b16((sequences, 2 * own, width)),
            b16((rows, width)),
            f32((rows, width)),
            f32((rows, modes)),
            b16((width, modes // 2)),
            b16((width, modes // 2)),
            f32((rows, modes)),
            f32((rows, modes)),
            b16((rows, modes)),
            b16((rows, modes)),
            b16((width, modes // 2)),
            b16((width, modes // 2)),
            f32((24, modes)),
            f32((2, CHUNKS, modes)),
            f32((4, CHUNKS, modes)),
            f32((2, CHUNKS, modes)),
            f32((nx, tile, LANES)),
            f32((nx, tile, LANES)),
            f32((tile, LANES)),
            f32((nz - 1, tile, LANES)),
            f32((nx, 2 * tile, LANES)),
            b16((nx, 2 * tile, LANES)),
            b16((nx, 2 * tile, LANES)),
            b16((2 * tile, LANES)),
            b16((nz - 1, 2 * tile, LANES)),
            b16((nx, 2 * tile, LANES)),
            b16((nx, 2 * tile, LANES)),
            f32((2, tile, LANES)),
            b16((sequences, 2 * own, width)),
            dma((13,)),
            dma,
            dma,
            dma,
            dma,
            dma((nx - 1,)),
            dma((nx - 1,)),
            dma((nz - 1,)),
            dma((nz - 1,)),
            dma((nx - 1,)),
            dma((nx - 1,)),
            dma((nz - 1,)),
            dma((nz - 1,)),
            dma((nx - 1,)),
            dma((nx - 1,)),
            dma,
            dma,
        ],
        compiler_params=pltpu.CompilerParams(collective_id=0, has_side_effects=True, vmem_limit_bytes=60 << 20),
    )(
        layer_input,
        in_weight,
        gate_weight,
        out_weight,
        norm_gain[None],
        rate_real,
        rate_imag,
        log_step[None],
        jnp.swapaxes(input_real, 1, 2).reshape(width, states),
        jnp.swapaxes(input_imag, 1, 2).reshape(width, states),
        output_real.reshape(width, states),
        output_imag.reshape(width, states),
        skip_weight[None],
        jnp.swapaxes(decay_offset, 1, 2),
    )
    return pl.pallas_call(
        finish_kernel,
        name="finish",
        out_shape=jax.ShapeDtypeStruct((sequences, own, depth), BF16),
        in_specs=[vmem()] * 5,
        out_specs=hbm(),
        scratch_shapes=[b16((sequences, own, depth)), dma((depth // 512,))],
        compiler_params=pltpu.CompilerParams(vmem_limit_bytes=16 << 20),
    )(near, far, channel_gain[None], out_weight, far_w)


def solution(mesh):
    torus = Mesh(
        mesh.devices.reshape(mesh.shape["grp"], 16, 4, mesh.shape["tp"]),
        ("grp", "sp_0", "sp_1", "tp"),
    )
    return build(torus)


def build(torus):
    in_specs = (
        P("grp", SP_TP, None),
        P(),
        P(None, "tp"),
        P(None, "tp"),
        P("tp", None),
        P("tp", None),
        P("tp"),
        P("tp", None, None),
        P("tp", None, None),
        P("tp", None, None),
        P("tp", None, None),
        P("tp"),
        P("grp", SP, "tp"),
        P(),
        P("tp", None),
    )
    out_specs = P("grp", SP_TP, None)
    return jax.shard_map(shards, mesh=torus, in_specs=in_specs, out_specs=out_specs, check_vma=False)
```

```python
import functools
import math

import jax
import jax.numpy as jnp
from jax import lax
from jax.experimental import pallas as pl
from jax.experimental.pallas import tpu as pltpu
from jax.sharding import Mesh
from jax.sharding import PartitionSpec as P

SP = ("sp_0", "sp_1")
SP_TP = ("sp_0", "sp_1", "tp")
MESH = pl.DeviceIdType.MESH
F32 = jnp.float32
BF16 = jnp.bfloat16
EPS = 1e-06
LANES = 128
CHUNKS = 8


def dot(a, b):
    return jnp.dot(a, b, preferred_element_type=F32)


def dot_t(a, b):
    return lax.dot_general(a, b, (((1,), (1,)), ((), ())), preferred_element_type=F32)


def iota(shape, dim):
    return lax.broadcasted_iota(jnp.int32, shape, dim)


def one_hot(cond):
    return jnp.where(cond, 1.0, 0.0).astype(BF16)


def split(value):
    high = value.astype(BF16)
    rest = value - high.astype(F32)
    middle = rest.astype(BF16)
    low = (rest - middle.astype(F32)).astype(BF16)
    return high, middle, low


def exact_dot(value, table):
    high, middle, low = split(value)
    return dot(high, table) + dot(middle, table) + dot(low, table)


def cmul(a, b):
    return a[0] * b[0] - a[1] * b[1], a[0] * b[1] + a[1] * b[0]


def small_expm1(x):
    series = x * (1.0 + x * (1 / 2 + x * (1 / 6 + x * (1 / 24 + x * (1 / 120 + x * (1 / 720 + x / 5040))))))
    return jnp.where(x > -0.3, series, jnp.exp(x) - 1.0)


def scan_order(rows):
    steps = rows // CHUNKS
    at = iota((rows, rows), 0)
    return one_hot(iota((rows, rows), 1) == (at & (CHUNKS - 1)) * steps + (at >> 3))


def natural_order(rows):
    steps = rows // CHUNKS
    at = iota((rows, rows), 1)
    return one_hot(iota((rows, rows), 0) == (at & (CHUNKS - 1)) * steps + (at >> 3))


def small_sine(x):
    q = x * x
    return x * (1.0 + q * (-1 / 6 + q * (1 / 120 + q * (-1 / 5040 + q * (1 / 362880 - q / 39916800)))))


def small_cosine(x):
    q = x * x
    return 1.0 + q * (-1 / 2 + q * (1 / 24 + q * (-1 / 720 + q * (1 / 40320 + q * (-1 / 3628800 + q / 479001600)))))


def mixer_kernel(
    x_hbm,
    in_w_hbm,
    gate_w_hbm,
    out_w_hbm,
    norm_gain_hbm,
    rate_re_hbm,
    rate_im_hbm,
    log_step_hbm,
    table_re_hbm,
    table_im_hbm,
    read_re_hbm,
    read_im_hbm,
    skip_hbm,
    offset_hbm,
    gain_hbm,
    near_ref,
    square_ref,
    far_ref,
    far_w_ref,
    tokens,
    in_w,
    gate_w,
    norm_gain_ref,
    rate_re_ref,
    rate_im_ref,
    log_step_ref,
    table_re_ref,
    table_im_ref,
    read_re_ref,
    read_im_ref,
    skip_ref,
    offset_ref,
    gain_ref,
    out_w,
    normed,
    scales,
    raw_in,
    raw_gate,
    inputs,
    opened,
    mags,
    wide_re,
    wide_im,
    drive_re,
    drive_im,
    states_re,
    states_im,
    lift_re,
    lift_im,
    vec,
    ends,
    before,
    init,
    log_pack,
    log_x,
    log_row,
    log_z,
    sum_stage,
    sum_pack,
    sum_x,
    sum_row,
    sum_z,
    carry_pack,
    carry_x,
    lam_pack,
    act,
    load_sem,
    x_send,
    x_recv,
    w_send,
    w_recv,
    lx_send,
    lx_recv,
    lz_send,
    lz_recv,
    sx_send,
    sx_recv,
    sz_send,
    sz_recv,
    cx_send,
    cx_recv,
    a_send,
    a_recv,
):
    nz, nx = lax.axis_size("sp_0"), lax.axis_size("sp_1")
    mz, mx, tp = lax.axis_index("sp_0"), lax.axis_index("sp_1"), lax.axis_index("tp")
    sequences, own, depth = x_hbm.shape
    width = in_w_hbm.shape[1]
    rows = sequences * 2 * own
    groups, states = rate_re_hbm.shape
    channels = width // groups
    modes = groups * states
    steps = rows // CHUNKS
    quarters = CHUNKS // sequences
    part = modes // nx
    blocks = part // LANES
    tile = sequences * blocks
    half = modes // 2
    hw = width // 2
    mine = pl.ds(pl.multiple_of(tp * own, own), own)
    theirs = pl.ds(pl.multiple_of((1 - tp) * own, own), own)
    partner = {"tp": 1 - tp}

    loads = [
        pltpu.make_async_copy(source, target, load_sem.at[i])
        for i, (source, target) in enumerate(
            (
                (x_hbm, tokens.at[:, mine, :]),
                (offset_hbm, offset_ref),
                (rate_re_hbm, rate_re_ref),
                (rate_im_hbm, rate_im_ref),
                (log_step_hbm, log_step_ref),
                (norm_gain_hbm, norm_gain_ref),
                (table_re_hbm, table_re_ref),
                (table_im_hbm, table_im_ref),
                (in_w_hbm, in_w),
                (gate_w_hbm, gate_w),
                (read_re_hbm, read_re_ref),
                (read_im_hbm, read_im_ref),
                (skip_hbm, skip_ref),
                (gain_hbm, gain_ref),
                (out_w_hbm, out_w),
            )
        )
    ]
    for copy in loads:
        copy.start()

    log_z[...] = jnp.zeros_like(log_z)
    sum_z[...] = jnp.zeros_like(sum_z)
    barrier = pltpu.get_barrier_semaphore()
    pl.semaphore_signal(barrier, inc=1, device_id=partner, device_id_type=MESH)
    for d in range(1, nx):
        pl.semaphore_signal(barrier, inc=1, device_id={"sp_1": lax.rem(mx + d, nx)}, device_id_type=MESH)
    far_first = sorted(range(1, nz), key=lambda d: -min(d, nz - d))
    for d in far_first:
        pl.semaphore_signal(barrier, inc=1, device_id={"sp_0": lax.rem(mz + d, nz)}, device_id_type=MESH)

    def remote(source, target, send, recv, device):
        return pltpu.make_async_remote_copy(
            src_ref=source, dst_ref=target, send_sem=send, recv_sem=recv, device_id=device, device_id_type=MESH
        )

    def to_x(source, target, send, recv):
        made = []
        for d in range(1, nx):
            k = lax.rem(mx + d, nx)
            made.append(remote(source.at[k], target.at[mx], send.at[d - 1], recv.at[d - 1], {"sp_1": k}))
        return made

    def to_z(source, target, send, recv):
        return {
            d: remote(source, target.at[d - 1], send.at[d - 1], recv.at[d - 1], {"sp_0": lax.rem(mz + d, nz)})
            for d in far_first
        }

    def start_z(made):
        for d, copy in made.items():
            pl.when(mz + d < nz)(copy.start)

    def recv_z(made):
        for d, copy in made.items():
            pl.when(d <= mz)(copy.wait_recv)

    def sent_z(made):
        for d, copy in made.items():
            pl.when(mz + d < nz)(copy.wait_send)

    for copy in loads[1:6]:
        copy.wait()
    spread_g = one_hot((iota((groups, modes), 1) >> 6) == iota((groups, modes), 0))
    spread_p = one_hot((iota((states, modes), 1) & (states - 1)) == iota((states, modes), 0))
    offsets = jnp.concatenate([offset_ref[s].T for s in range(sequences)], axis=0)
    sums = jnp.sum(offsets.reshape(CHUNKS, steps, groups), axis=1)
    step_size = jnp.broadcast_to(jnp.exp(log_step_ref[...]), (8, groups))
    spread = exact_dot(jnp.concatenate([sums, step_size], axis=0), spread_g)
    chunk_logs, step = spread[:CHUNKS], spread[CHUNKS : CHUNKS + 1]
    vec[pl.ds(16, CHUNKS), :] = chunk_logs
    for s in range(sequences):
        total = jnp.sum(chunk_logs[s * quarters : (s + 1) * quarters], axis=0, keepdims=True)
        for k in range(nx):
            for b in range(blocks):
                lo = k * part + b * LANES
                row = s * blocks + b
                log_pack[k, row : row + 1, :] = total[:, lo : lo + LANES]

    def norm(side):
        for s in range(sequences):
            for r in range(0, own, 32):
                wide = tokens[s, pl.ds(pl.multiple_of(side * own + r, 32), 32), :].astype(F32)
                at = slice(s * own + r, s * own + r + 32)
                normed[side, at, :] = (wide * norm_gain_ref[...]).astype(BF16)
                scale = lax.rsqrt(jnp.mean(wide * wide, axis=-1, keepdims=True) + EPS)
                scales[side, at, :] = jnp.broadcast_to(scale, (32, 256))

    def project(side, weight, out):
        @pl.loop(0, width // 256)
        def _(c):
            lanes = pl.ds(pl.multiple_of(c * 256, 256), 256)
            product = dot(normed[side], weight[:, lanes]) * scales[side]
            at = pl.ds(pl.multiple_of(side * own, own), own)
            out[:, at, lanes] = product.reshape(sequences, own, 256).astype(BF16)

    loads[0].wait()
    norm(tp)
    loads[8].wait()
    project(tp, in_w, raw_in)

    pl.semaphore_wait(barrier, nx + nz - 1)
    log_sends = to_x(log_pack, log_x, lx_send, lx_recv)
    for copy in log_sends:
        copy.start()
    x_copy = remote(tokens.at[:, mine, :], tokens.at[:, mine, :], x_send, x_recv, partner)
    x_copy.start()
    log_x[pl.ds(mx, 1)] = log_pack[pl.ds(mx, 1)]

    on_group = (iota((groups, modes), 1) >> 6) == iota((groups, modes), 0)
    rates = exact_dot(jnp.concatenate([rate_re_ref[...], rate_im_ref[...]], axis=0), spread_p)
    rate_re = jnp.sum(jnp.where(on_group, rates[:groups], 0.0), axis=0, keepdims=True)
    rate_im = jnp.sum(jnp.where(on_group, rates[groups:], 0.0), axis=0, keepdims=True)
    real_step, angle = rate_re * step, rate_im * step
    size = jnp.exp(real_step)
    cosine, sine = small_cosine(angle), small_sine(angle)
    half_sine = small_sine(0.5 * angle)
    top_re = small_expm1(real_step) * cosine - 2.0 * half_sine * half_sine
    top_im = size * sine
    inverse = 1.0 / (rate_re * rate_re + rate_im * rate_im)
    coef_re = (top_re * rate_re + top_im * rate_im) * inverse
    coef_im = (top_im * rate_re - top_re * rate_im) * inverse
    lam = (size * cosine, size * sine)
    power = lam
    for _ in range(int(math.log2(steps))):
        power = cmul(power, power)
    lam_chunk = power
    for _ in range(int(math.log2(quarters))):
        power = cmul(power, power)
    for i, value in enumerate((*lam, *lam_chunk, *power, coef_re, coef_im)):
        vec[i : i + 1, :] = value

    order = scan_order(rows)
    pieces = [dot(order, piece) for piece in split(jnp.exp(offsets))]
    spread_3 = one_hot((iota((3 * groups, modes), 1) >> 6) == (iota((3 * groups, modes), 0) & (groups - 1)))
    mags[...] = dot(jnp.concatenate(pieces, axis=1).astype(BF16), spread_3)

    per_tile = LANES // states

    def doubled(value):
        return jnp.concatenate([value.astype(F32)] * per_tile, axis=1)

    on_lane = iota((channels, LANES), 1) // states

    def block_diagonal(target, value):
        target[...] = jnp.zeros_like(target)
        for g in range(groups):
            at = slice(g * channels, (g + 1) * channels)
            lo = (g % (groups // 2)) // per_tile * LANES
            kept = jnp.where(on_lane == g % per_tile, value(g, at), 0.0)
            target[at, lo : lo + LANES] = kept.astype(BF16)

    for copy in loads[6:8]:
        copy.wait()
    two_re, two_im = doubled(table_re_ref[...]), doubled(table_im_ref[...])
    block_diagonal(wide_re, lambda g, at: two_re[at])
    block_diagonal(wide_im, lambda g, at: two_im[at])

    x_copy.wait()
    w_copies = [
        remote(out_w_hbm.at[at], far_w_ref.at[at], w_send.at[i], w_recv.at[i], partner)
        for i, at in enumerate((pl.ds(0, hw), pl.ds(hw, hw)))
    ]
    w_copies[0].start()
    norm(1 - tp)
    project(1 - tp, in_w, raw_in)
    inputs[...] = dot(order, raw_in[...].reshape(rows, width)).astype(BF16)

    for h in range(2):
        use, lanes = slice(h * hw, (h + 1) * hw), slice(h * half, (h + 1) * half)
        drive_re[:, lanes] = dot(inputs[:, use], wide_re[use, :])
        drive_im[:, lanes] = dot(inputs[:, use], wide_im[use, :])

    span = 512

    def scan(first, keep):
        @pl.loop(0, modes // span)
        def _(c):
            lanes = pl.ds(pl.multiple_of(c * span, span), span)
            lr = jnp.broadcast_to(vec[0:1, lanes], (CHUNKS, span))
            li = jnp.broadcast_to(vec[1:2, lanes], (CHUNKS, span))
            if first is None:
                start = (jnp.zeros((CHUNKS, span), F32), jnp.zeros((CHUNKS, span), F32))
            else:
                start = (first[0, :, lanes], first[1, :, lanes])

            def body(t, now):
                re, im = now
                at = pl.ds(pl.multiple_of(t * 4 * CHUNKS, 4 * CHUNKS), 4 * CHUNKS)
                m, dr, di = mags[at, lanes], drive_re[at, lanes], drive_im[at, lanes]
                kept = []
                for u in range(4):
                    use = slice(u * CHUNKS, (u + 1) * CHUNKS)
                    ar, ai = m[use] * lr, m[use] * li
                    re, im = ar * re - ai * im + dr[use], ar * im + ai * re + di[use]
                    kept.append((re, im))
                if keep:
                    states_re[at, lanes] = jnp.concatenate([k[0] for k in kept], axis=0).astype(BF16)
                    states_im[at, lanes] = jnp.concatenate([k[1] for k in kept], axis=0).astype(BF16)
                return re, im

            re, im = lax.fori_loop(0, steps // 4, body, start)
            if not keep:
                ends[0, :, lanes] = re
                ends[1, :, lanes] = im

    scan(None, False)

    place = iota((CHUNKS, modes), 0) & (quarters - 1)
    grown = jnp.exp(vec[pl.ds(16, CHUNKS), :])
    a = (grown * vec[2:3, :], grown * vec[3:4, :])
    b = (ends[0], ends[1])
    d = 1
    while d < quarters:
        ok = place >= d
        a_old = tuple(pltpu.roll(v, d, axis=0) for v in a)
        b_old = tuple(pltpu.roll(v, d, axis=0) for v in b)
        add = cmul(a, b_old)
        new_a = cmul(a, a_old)
        b = tuple(jnp.where(ok, v + w, v) for v, w in zip(b, add))
        a = tuple(jnp.where(ok, w, v) for v, w in zip(a, new_a))
        d *= 2
    for c in range(2):
        for s in range(sequences):
            last = (s + 1) * quarters - 1
            for k in range(nx):
                for blk in range(blocks):
                    lo = k * part + blk * LANES
                    row = c * tile + s * blocks + blk
                    sum_stage[k, row : row + 1, :] = b[c][last : last + 1, lo : lo + LANES]
    sum_pack[...] = sum_stage[...].astype(BF16)
    for i, (value, empty) in enumerate(((a[0], 1.0), (a[1], 0.0), (b[0], 0.0), (b[1], 0.0))):
        before[i] = jnp.where(place == 0, empty, pltpu.roll(value, 1, axis=0))
    sum_sends = to_x(sum_pack, sum_x, sx_send, sx_recv)
    for copy in sum_sends:
        copy.start()
    sum_x[pl.ds(mx, 1)] = sum_pack[pl.ds(mx, 1)]

    for copy in log_sends:
        copy.wait()
    log_row[...] = jnp.sum(log_x[...], axis=0)
    log_z_sends = to_z(log_row, log_z, lz_send, lz_recv)
    start_z(log_z_sends)
    for c in range(2):
        for blk in range(blocks):
            lanes = pl.ds(pl.multiple_of(mx * part + blk * LANES, LANES), LANES)
            value = vec[4 + c : 5 + c, lanes]
            for s in range(sequences):
                row = s * blocks + blk
                lam_pack[c, row : row + 1, :] = value
    lam_dev = (lam_pack[0], lam_pack[1])
    one = (jnp.ones((tile, LANES), F32), jnp.zeros((tile, LANES), F32))
    lam_pow = [one]
    for _ in range(nx):
        lam_pow.append(cmul(lam_pow[-1], lam_dev))

    def grow(logs, base):
        size = jnp.exp(logs)
        return size * base[0], size * base[1]

    def halves(value):
        wide = value.astype(F32)
        return wide[:tile], wide[tile:]

    def plus(u, v):
        return u[0] + v[0], u[1] + v[1]

    logs = [log_x[k] for k in range(nx)]
    to_end, to_start = [None] * nx, [None] * nx
    gone = jnp.zeros((tile, LANES), F32)
    for k in range(nx - 1, -1, -1):
        to_end[k] = grow(gone, lam_pow[nx - 1 - k])
        gone = gone + logs[k]
    gone = jnp.zeros((tile, LANES), F32)
    for k in range(nx):
        to_start[k] = grow(gone, lam_pow[k])
        gone = gone + logs[k]

    loads[9].wait()
    project(tp, gate_w, raw_gate)
    project(1 - tp, gate_w, raw_gate)
    gates = dot(scan_order(rows), raw_gate[...].reshape(rows, width))
    opened[...] = 1.0 / (1.0 + jnp.exp(-gates))

    for copy in loads[10:14]:
        copy.wait()
    two_re, two_im = doubled(read_re_ref[...]), doubled(read_im_ref[...])

    def coef(g):
        lo = g // per_tile * LANES
        return vec[6:7, lo : lo + LANES], vec[7:8, lo : lo + LANES]

    def lifted_re(g, at):
        kr, ki = coef(g)
        return two_re[at] * kr - two_im[at] * ki

    def lifted_im(g, at):
        kr, ki = coef(g)
        return -(two_re[at] * ki + two_im[at] * kr)

    block_diagonal(lift_re, lifted_re)
    block_diagonal(lift_im, lifted_im)

    for copy in sum_sends:
        copy.wait()
    came = [halves(sum_x[k]) for k in range(nx)]
    total = cmul(to_end[0], came[0])
    for k in range(1, nx):
        total = plus(total, cmul(to_end[k], came[k]))
    sum_row[...] = jnp.concatenate(total, axis=0).astype(BF16)
    sum_z_sends = to_z(sum_row, sum_z, sz_send, sz_recv)
    start_z(sum_z_sends)

    inside = [None] * nx
    inside[0] = (jnp.zeros((tile, LANES), F32), jnp.zeros((tile, LANES), F32))
    for k in range(1, nx):
        inside[k] = plus(cmul(inside[k - 1], grow(logs[k - 1], lam_dev)), came[k - 1])
    recv_z(log_z_sends)
    weights = {}
    gone, power = jnp.zeros((tile, LANES), F32), one
    for d in range(1, nz):
        weights[d] = grow(gone, power)
        gone = gone + log_z[d - 1]
        power = cmul(power, lam_pow[nx])

    recv_z(sum_z_sends)
    carry = inside[0]
    for d in range(1, nz):
        carry = plus(carry, cmul(weights[d], halves(sum_z[d - 1])))
    for k in range(nx):
        carry_pack[k] = jnp.concatenate(plus(cmul(carry, to_start[k]), inside[k]), axis=0).astype(BF16)
    carry_sends = to_x(carry_pack, carry_x, cx_send, cx_recv)
    for copy in carry_sends:
        copy.start()
    carry_x[pl.ds(mx, 1)] = carry_pack[pl.ds(mx, 1)]
    for copy in carry_sends:
        copy.wait()
    upper = iota((CHUNKS, LANES), 0) < quarters
    for k in range(nx):
        got = carry_x[k].astype(F32)
        for blk in range(blocks):
            lo = k * part + blk * LANES
            lanes = slice(lo, lo + LANES)
            into = tuple(
                jnp.where(upper, got[c * tile + blk][None], got[c * tile + blocks + blk][None]) for c in range(2)
            )
            moved = cmul((before[0, :, lanes], before[1, :, lanes]), into)
            init[0, :, lanes] = before[2, :, lanes] + moved[0]
            init[1, :, lanes] = before[3, :, lanes] + moved[1]

    w_copies[1].start()
    scan(init, True)

    parts = []
    for h in range(2):
        use = slice(h * hw, (h + 1) * hw)
        lanes = slice(h * half, (h + 1) * half)
        mixed = dot_t(states_re[:, lanes], lift_re[use, :]) + dot_t(states_im[:, lanes], lift_im[use, :])
        mixed = mixed + skip_ref[:, use] * inputs[:, use].astype(F32)
        gelu = 0.5 * mixed * (1.0 + lax.erf(mixed * math.sqrt(0.5)))
        parts.append((gelu * opened[:, use]).astype(BF16))
    back = natural_order(rows)
    for h in range(2):
        act[:, :, h * hw : (h + 1) * hw] = dot(back, parts[h]).astype(BF16).reshape(sequences, 2 * own, hw)
    a_copy = remote(act.at[:, theirs, :], far_ref, a_send, a_recv, partner)
    a_copy.start()
    near = act[:, mine, :].astype(F32).reshape(sequences * own, width)
    square_ref[...] = jnp.broadcast_to(jnp.sum(near * near, axis=-1, keepdims=True), square_ref.shape)
    near = (near * gain_ref[:, pl.ds(pl.multiple_of(tp * width, width), width)]).astype(BF16)
    loads[14].wait()
    for c in range(depth // 512):
        lanes = slice(c * 512, (c + 1) * 512)
        near_ref[:, lanes] = dot(near, out_w[:, lanes])
    for copy in w_copies:
        copy.wait()
    a_copy.wait()

    sent_z(log_z_sends)
    sent_z(sum_z_sends)


def finish_kernel(near_ref, square_ref, far_ref, gain_ref, far_w_ref, out_hbm, staged, sem):
    tp = lax.axis_index("tp")
    sequences, own, width = far_ref.shape
    depth = far_w_ref.shape[1]

    far = far_ref[...].astype(F32).reshape(sequences * own, width)
    square = square_ref[:, :1] + jnp.sum(far * far, axis=-1, keepdims=True)
    scale = lax.rsqrt(square * (0.5 / width) + EPS)
    far = (far * gain_ref[:, pl.ds(pl.multiple_of((1 - tp) * width, width), width)]).astype(BF16)
    copies = []
    for c in range(depth // 512):
        lanes = slice(c * 512, (c + 1) * 512)
        result = (near_ref[:, lanes] + dot(far, far_w_ref[:, lanes])) * scale
        staged[:, :, lanes] = result.astype(BF16).reshape(sequences, own, 512)
        copies.append(pltpu.make_async_copy(staged.at[:, :, lanes], out_hbm.at[:, :, lanes], sem.at[c]))
        copies[-1].start()
    for copy in copies:
        copy.wait()


def vmem():
    return pl.BlockSpec(memory_space=pltpu.VMEM)


def hbm():
    return pl.BlockSpec(memory_space=pl.ANY)


def shards(
    layer_input,
    norm_gain,
    in_weight,
    gate_weight,
    rate_real,
    rate_imag,
    log_step,
    input_real,
    input_imag,
    output_real,
    output_imag,
    skip_weight,
    decay_offset,
    channel_gain,
    out_weight,
):
    nz, nx = lax.axis_size("sp_0"), lax.axis_size("sp_1")
    sequences, own, depth = layer_input.shape
    width = in_weight.shape[1]
    groups, states = rate_real.shape
    modes = groups * states
    rows = sequences * 2 * own
    dma = pltpu.SemaphoreType.DMA
    tile = sequences * (modes // nx // LANES)
    f32 = functools.partial(pltpu.VMEM, dtype=F32)
    b16 = functools.partial(pltpu.VMEM, dtype=BF16)
    near, square, far, far_w = pl.pallas_call(
        mixer_kernel,
        name="mixer",
        out_shape=[
            pltpu.VMEM((sequences * own, depth), F32),
            pltpu.VMEM((sequences * own, LANES), F32),
            pltpu.VMEM((sequences, own, width), BF16),
            pltpu.VMEM((width, depth), BF16),
        ],
        in_specs=[pl.BlockSpec(memory_space=pltpu.HBM)] * 15,
        out_specs=[vmem()] * 4,
        scratch_shapes=[
            b16((sequences, 2 * own, depth)),
            b16((depth, width)),
            b16((depth, width)),
            f32((1, depth)),
            f32((groups, states)),
            f32((groups, states)),
            f32((1, groups)),
            b16((width, states)),
            b16((width, states)),
            b16((width, states)),
            b16((width, states)),
            f32((1, width)),
            f32((sequences, groups, 2 * own)),
            f32((1, 2 * width)),
            b16((width, depth)),
            b16((2, sequences * own, depth)),
            f32((2, sequences * own, 256)),
            b16((sequences, 2 * own, width)),
            b16((sequences, 2 * own, width)),
            b16((rows, width)),
            f32((rows, width)),
            f32((rows, modes)),
            b16((width, modes // 2)),
            b16((width, modes // 2)),
            f32((rows, modes)),
            f32((rows, modes)),
            b16((rows, modes)),
            b16((rows, modes)),
            b16((width, modes // 2)),
            b16((width, modes // 2)),
            f32((24, modes)),
            f32((2, CHUNKS, modes)),
            f32((4, CHUNKS, modes)),
            f32((2, CHUNKS, modes)),
            f32((nx, tile, LANES)),
            f32((nx, tile, LANES)),
            f32((tile, LANES)),
            f32((nz - 1, tile, LANES)),
            f32((nx, 2 * tile, LANES)),
            b16((nx, 2 * tile, LANES)),
            b16((nx, 2 * tile, LANES)),
            b16((2 * tile, LANES)),
            b16((nz - 1, 2 * tile, LANES)),
            b16((nx, 2 * tile, LANES)),
            b16((nx, 2 * tile, LANES)),
            f32((2, tile, LANES)),
            b16((sequences, 2 * own, width)),
            dma((15,)),
            dma,
            dma,
            dma((2,)),
            dma((2,)),
            dma((nx - 1,)),
            dma((nx - 1,)),
            dma((nz - 1,)),
            dma((nz - 1,)),
            dma((nx - 1,)),
            dma((nx - 1,)),
            dma((nz - 1,)),
            dma((nz - 1,)),
            dma((nx - 1,)),
            dma((nx - 1,)),
            dma,
            dma,
        ],
        compiler_params=pltpu.CompilerParams(collective_id=0, has_side_effects=True, vmem_limit_bytes=67043328 - (5 << 20)),
    )(
        layer_input,
        in_weight,
        gate_weight,
        out_weight,
        norm_gain[None],
        rate_real,
        rate_imag,
        log_step[None],
        jnp.swapaxes(input_real, 1, 2).reshape(width, states),
        jnp.swapaxes(input_imag, 1, 2).reshape(width, states),
        output_real.reshape(width, states),
        output_imag.reshape(width, states),
        skip_weight[None],
        jnp.swapaxes(decay_offset, 1, 2),
        channel_gain[None],
    )
    return pl.pallas_call(
        finish_kernel,
        name="finish",
        out_shape=jax.ShapeDtypeStruct((sequences, own, depth), BF16),
        in_specs=[vmem()] * 5,
        out_specs=hbm(),
        scratch_shapes=[b16((sequences, own, depth)), dma((depth // 512,))],
        compiler_params=pltpu.CompilerParams(vmem_limit_bytes=16 << 20),
    )(near, square, far, channel_gain[None], far_w)


def solution(mesh):
    torus = Mesh(
        mesh.devices.reshape(mesh.shape["grp"], 16, 4, mesh.shape["tp"]),
        ("grp", "sp_0", "sp_1", "tp"),
    )
    return build(torus)


def build(torus):
    in_specs = (
        P("grp", SP_TP, None),
        P(),
        P(None, "tp"),
        P(None, "tp"),
        P("tp", None),
        P("tp", None),
        P("tp"),
        P("tp", None, None),
        P("tp", None, None),
        P("tp", None, None),
        P("tp", None, None),
        P("tp"),
        P("grp", SP, "tp"),
        P(),
        P("tp", None),
    )
    out_specs = P("grp", SP_TP, None)
    return jax.shard_map(shards, mesh=torus, in_specs=in_specs, out_specs=out_specs, check_vma=False)
```

```python
import functools
import math

import jax
import jax.numpy as jnp
from jax import lax
from jax.experimental import pallas as pl
from jax.experimental.pallas import tpu as pltpu
from jax.sharding import Mesh
from jax.sharding import PartitionSpec as P

SP = ("sp_0", "sp_1")
SP_TP = ("sp_0", "sp_1", "tp")
MESH = pl.DeviceIdType.MESH
F32 = jnp.float32
BF16 = jnp.bfloat16
EPS = 1e-06
LANES = 128
CHUNKS = 8
BLOCK = 4


def dot(a, b):
    return jnp.dot(a, b, preferred_element_type=F32)


def dot_t(a, b):
    return lax.dot_general(a, b, (((1,), (1,)), ((), ())), preferred_element_type=F32)


def iota(shape, dim):
    return lax.broadcasted_iota(jnp.int32, shape, dim)


def one_hot(cond):
    return jnp.where(cond, 1.0, 0.0).astype(BF16)


def split(value):
    high = value.astype(BF16)
    rest = value - high.astype(F32)
    middle = rest.astype(BF16)
    low = (rest - middle.astype(F32)).astype(BF16)
    return high, middle, low


def exact_dot(value, table):
    high, middle, low = split(value)
    return dot(high, table) + dot(middle, table) + dot(low, table)


def cmul(a, b):
    return a[0] * b[0] - a[1] * b[1], a[0] * b[1] + a[1] * b[0]


def small_expm1(x):
    series = x * (1.0 + x * (1 / 2 + x * (1 / 6 + x * (1 / 24 + x * (1 / 120 + x * (1 / 720 + x / 5040))))))
    return jnp.where(x > -0.3, series, jnp.exp(x) - 1.0)


def scan_order(rows):
    steps = rows // CHUNKS
    at = iota((rows, rows), 0)
    return one_hot(iota((rows, rows), 1) == (at & (CHUNKS - 1)) * steps + (at >> 3))


def natural_order(rows):
    steps = rows // CHUNKS
    at = iota((rows, rows), 1)
    return one_hot(iota((rows, rows), 0) == (at & (CHUNKS - 1)) * steps + (at >> 3))


def small_sine(x):
    q = x * x
    return x * (1.0 + q * (-1 / 6 + q * (1 / 120 + q * (-1 / 5040 + q * (1 / 362880 - q / 39916800)))))


def small_cosine(x):
    q = x * x
    return 1.0 + q * (-1 / 2 + q * (1 / 24 + q * (-1 / 720 + q * (1 / 40320 + q * (-1 / 3628800 + q / 479001600)))))


def mixer_kernel(
    x_hbm,
    in_w_hbm,
    gate_w_hbm,
    out_w_hbm,
    norm_gain_hbm,
    rate_re_hbm,
    rate_im_hbm,
    log_step_hbm,
    table_re_hbm,
    table_im_hbm,
    read_re_hbm,
    read_im_hbm,
    skip_hbm,
    offset_hbm,
    gain_hbm,
    near_ref,
    square_ref,
    far_ref,
    far_w_ref,
    tokens,
    in_w,
    gate_w,
    norm_gain_ref,
    rate_re_ref,
    rate_im_ref,
    log_step_ref,
    table_re_ref,
    table_im_ref,
    read_re_ref,
    read_im_ref,
    skip_ref,
    offset_ref,
    gain_ref,
    out_w,
    normed,
    scales,
    raw_in,
    raw_gate,
    inputs,
    opened,
    mags,
    wide_re,
    wide_im,
    drive_re,
    drive_im,
    states_re,
    states_im,
    lift_re,
    lift_im,
    vec,
    ends,
    before,
    init,
    log_pack,
    log_x,
    log_row,
    log_z,
    log_block,
    log_far,
    sum_stage,
    sum_pack,
    sum_x,
    sum_row,
    sum_z,
    sum_block,
    sum_far,
    carry_pack,
    carry_x,
    lam_pack,
    act,
    load_sem,
    x_send,
    x_recv,
    w_send,
    w_recv,
    lx_send,
    lx_recv,
    lz_send,
    lz_recv,
    lf_send,
    lf_recv,
    sx_send,
    sx_recv,
    sz_send,
    sz_recv,
    sf_send,
    sf_recv,
    cx_send,
    cx_recv,
    a_send,
    a_recv,
):
    nz, nx = lax.axis_size("sp_0"), lax.axis_size("sp_1")
    mz, mx, tp = lax.axis_index("sp_0"), lax.axis_index("sp_1"), lax.axis_index("tp")
    sequences, own, depth = x_hbm.shape
    width = in_w_hbm.shape[1]
    rows = sequences * 2 * own
    groups, states = rate_re_hbm.shape
    channels = width // groups
    modes = groups * states
    steps = rows // CHUNKS
    quarters = CHUNKS // sequences
    part = modes // nx
    blocks = part // LANES
    tile = sequences * blocks
    half = modes // 2
    hw = width // 2
    mine = pl.ds(pl.multiple_of(tp * own, own), own)
    theirs = pl.ds(pl.multiple_of((1 - tp) * own, own), own)
    partner = {"tp": 1 - tp}

    loads = [
        pltpu.make_async_copy(source, target, load_sem.at[i])
        for i, (source, target) in enumerate(
            (
                (x_hbm, tokens.at[:, mine, :]),
                (offset_hbm, offset_ref),
                (rate_re_hbm, rate_re_ref),
                (rate_im_hbm, rate_im_ref),
                (log_step_hbm, log_step_ref),
                (norm_gain_hbm, norm_gain_ref),
                (table_re_hbm, table_re_ref),
                (table_im_hbm, table_im_ref),
                (in_w_hbm, in_w),
                (gate_w_hbm, gate_w),
                (read_re_hbm, read_re_ref),
                (read_im_hbm, read_im_ref),
                (skip_hbm, skip_ref),
                (gain_hbm, gain_ref),
                (out_w_hbm, out_w),
            )
        )
    ]
    for copy in loads:
        copy.start()

    for ref in (log_z, sum_z, log_far, sum_far):
        ref[...] = jnp.zeros_like(ref)
    barrier = pltpu.get_barrier_semaphore()
    pl.semaphore_signal(barrier, inc=1, device_id=partner, device_id_type=MESH)
    for d in range(1, nx):
        pl.semaphore_signal(barrier, inc=1, device_id={"sp_1": lax.rem(mx + d, nx)}, device_id_type=MESH)
    count = nz // BLOCK
    block, place_z = mz // BLOCK, mz % BLOCK
    ends_block = place_z == BLOCK - 1

    def signal_z(z):
        pl.semaphore_signal(barrier, inc=1, device_id={"sp_0": z}, device_id_type=MESH)

    for d in range(1, BLOCK):
        pl.when(d <= place_z)(lambda d=d: signal_z(mz - d))
    for e in range(1, count):
        pl.when(e <= block)(lambda e=e: signal_z((block - e) * BLOCK + BLOCK - 1))

    def remote(source, target, send, recv, device):
        return pltpu.make_async_remote_copy(
            src_ref=source, dst_ref=target, send_sem=send, recv_sem=recv, device_id=device, device_id_type=MESH
        )

    def to_x(source, target, send, recv):
        made = []
        for d in range(1, nx):
            k = lax.rem(mx + d, nx)
            made.append(remote(source.at[k], target.at[mx], send.at[d - 1], recv.at[d - 1], {"sp_1": k}))
        return made

    def to_block(source, target, send, recv):
        return {
            d: remote(source, target.at[d - 1], send.at[d - 1], recv.at[d - 1], {"sp_0": lax.rem(mz + d, nz)})
            for d in range(1, BLOCK)
        }

    def to_later(source, target, send, recv):
        made = {}
        for d in sorted(range(1, nz - BLOCK + 1), key=lambda d: -min(d, nz - d)):
            e = (d + BLOCK - 1) // BLOCK - 1
            made[d] = remote(source, target.at[e], send.at[d - 1], recv.at[e], {"sp_0": lax.rem(mz + d, nz)})
        return made

    def start_block(made):
        for d, copy in made.items():
            pl.when(place_z + d < BLOCK)(copy.start)

    def start_later(made):
        @pl.when(ends_block)
        def _():
            for d, copy in made.items():
                pl.when(mz + d < nz)(copy.start)

    def recv_block(made):
        for d, copy in made.items():
            pl.when(d <= place_z)(copy.wait_recv)

    def recv_later(made):
        for e in range(1, count):
            pl.when(e <= block)(made[(e - 1) * BLOCK + 1].wait_recv)

    def sent_block(made):
        for d, copy in made.items():
            pl.when(place_z + d < BLOCK)(copy.wait_send)

    def sent_later(made):
        @pl.when(ends_block)
        def _():
            for d, copy in made.items():
                pl.when(mz + d < nz)(copy.wait_send)

    for copy in loads[1:6]:
        copy.wait()
    spread_g = one_hot((iota((groups, modes), 1) >> 6) == iota((groups, modes), 0))
    spread_p = one_hot((iota((states, modes), 1) & (states - 1)) == iota((states, modes), 0))
    offsets = jnp.concatenate([offset_ref[s].T for s in range(sequences)], axis=0)
    sums = jnp.sum(offsets.reshape(CHUNKS, steps, groups), axis=1)
    step_size = jnp.broadcast_to(jnp.exp(log_step_ref[...]), (8, groups))
    spread = exact_dot(jnp.concatenate([sums, step_size], axis=0), spread_g)
    chunk_logs, step = spread[:CHUNKS], spread[CHUNKS : CHUNKS + 1]
    vec[pl.ds(16, CHUNKS), :] = chunk_logs
    for s in range(sequences):
        total = jnp.sum(chunk_logs[s * quarters : (s + 1) * quarters], axis=0, keepdims=True)
        for k in range(nx):
            for b in range(blocks):
                lo = k * part + b * LANES
                row = s * blocks + b
                log_pack[k, row : row + 1, :] = total[:, lo : lo + LANES]

    def norm(side):
        for s in range(sequences):
            for r in range(0, own, 32):
                wide = tokens[s, pl.ds(pl.multiple_of(side * own + r, 32), 32), :].astype(F32)
                at = slice(s * own + r, s * own + r + 32)
                normed[side, at, :] = (wide * norm_gain_ref[...]).astype(BF16)
                scale = lax.rsqrt(jnp.mean(wide * wide, axis=-1, keepdims=True) + EPS)
                scales[side, at, :] = jnp.broadcast_to(scale, (32, 256))

    def project(side, weight, out):
        @pl.loop(0, width // 256)
        def _(c):
            lanes = pl.ds(pl.multiple_of(c * 256, 256), 256)
            product = dot(normed[side], weight[:, lanes]) * scales[side]
            at = pl.ds(pl.multiple_of(side * own, own), own)
            out[:, at, lanes] = product.reshape(sequences, own, 256).astype(BF16)

    loads[0].wait()
    norm(tp)
    loads[8].wait()
    project(tp, in_w, raw_in)

    later = jnp.where(ends_block, nz - 1 - mz, 0)
    pl.semaphore_wait(barrier, nx + BLOCK - 1 - place_z + later)
    log_sends = to_x(log_pack, log_x, lx_send, lx_recv)
    for copy in log_sends:
        copy.start()
    x_copy = remote(tokens.at[:, mine, :], tokens.at[:, mine, :], x_send, x_recv, partner)
    x_copy.start()
    log_x[pl.ds(mx, 1)] = log_pack[pl.ds(mx, 1)]

    on_group = (iota((groups, modes), 1) >> 6) == iota((groups, modes), 0)
    rates = exact_dot(jnp.concatenate([rate_re_ref[...], rate_im_ref[...]], axis=0), spread_p)
    rate_re = jnp.sum(jnp.where(on_group, rates[:groups], 0.0), axis=0, keepdims=True)
    rate_im = jnp.sum(jnp.where(on_group, rates[groups:], 0.0), axis=0, keepdims=True)
    real_step, angle = rate_re * step, rate_im * step
    size = jnp.exp(real_step)
    cosine, sine = small_cosine(angle), small_sine(angle)
    half_sine = small_sine(0.5 * angle)
    top_re = small_expm1(real_step) * cosine - 2.0 * half_sine * half_sine
    top_im = size * sine
    inverse = 1.0 / (rate_re * rate_re + rate_im * rate_im)
    coef_re = (top_re * rate_re + top_im * rate_im) * inverse
    coef_im = (top_im * rate_re - top_re * rate_im) * inverse
    lam = (size * cosine, size * sine)
    power = lam
    for _ in range(int(math.log2(steps))):
        power = cmul(power, power)
    lam_chunk = power
    for _ in range(int(math.log2(quarters))):
        power = cmul(power, power)
    for i, value in enumerate((*lam, *lam_chunk, *power, coef_re, coef_im)):
        vec[i : i + 1, :] = value

    order = scan_order(rows)
    pieces = [dot(order, piece) for piece in split(jnp.exp(offsets))]
    spread_3 = one_hot((iota((3 * groups, modes), 1) >> 6) == (iota((3 * groups, modes), 0) & (groups - 1)))
    mags[...] = dot(jnp.concatenate(pieces, axis=1).astype(BF16), spread_3)

    per_tile = LANES // states

    def doubled(value):
        return jnp.concatenate([value.astype(F32)] * per_tile, axis=1)

    on_lane = iota((channels, LANES), 1) // states

    def block_diagonal(target, value):
        target[...] = jnp.zeros_like(target)
        for g in range(groups):
            at = slice(g * channels, (g + 1) * channels)
            lo = (g % (groups // 2)) // per_tile * LANES
            kept = jnp.where(on_lane == g % per_tile, value(g, at), 0.0)
            target[at, lo : lo + LANES] = kept.astype(BF16)

    for copy in loads[6:8]:
        copy.wait()
    two_re, two_im = doubled(table_re_ref[...]), doubled(table_im_ref[...])
    block_diagonal(wide_re, lambda g, at: two_re[at])
    block_diagonal(wide_im, lambda g, at: two_im[at])

    x_copy.wait()
    w_copies = [
        remote(out_w_hbm.at[at], far_w_ref.at[at], w_send.at[i], w_recv.at[i], partner)
        for i, at in enumerate((pl.ds(0, hw), pl.ds(hw, hw)))
    ]
    w_copies[0].start()
    norm(1 - tp)
    project(1 - tp, in_w, raw_in)
    inputs[...] = dot(order, raw_in[...].reshape(rows, width)).astype(BF16)

    for h in range(2):
        use, lanes = slice(h * hw, (h + 1) * hw), slice(h * half, (h + 1) * half)
        drive_re[:, lanes] = dot(inputs[:, use], wide_re[use, :])
        drive_im[:, lanes] = dot(inputs[:, use], wide_im[use, :])

    span = 512

    def scan(first, keep):
        @pl.loop(0, modes // span)
        def _(c):
            lanes = pl.ds(pl.multiple_of(c * span, span), span)
            lr = jnp.broadcast_to(vec[0:1, lanes], (CHUNKS, span))
            li = jnp.broadcast_to(vec[1:2, lanes], (CHUNKS, span))
            if first is None:
                start = (jnp.zeros((CHUNKS, span), F32), jnp.zeros((CHUNKS, span), F32))
            else:
                start = (first[0, :, lanes], first[1, :, lanes])

            def body(t, now):
                re, im = now
                at = pl.ds(pl.multiple_of(t * 4 * CHUNKS, 4 * CHUNKS), 4 * CHUNKS)
                m, dr, di = mags[at, lanes], drive_re[at, lanes], drive_im[at, lanes]
                kept = []
                for u in range(4):
                    use = slice(u * CHUNKS, (u + 1) * CHUNKS)
                    ar, ai = m[use] * lr, m[use] * li
                    re, im = ar * re - ai * im + dr[use], ar * im + ai * re + di[use]
                    kept.append((re, im))
                if keep:
                    states_re[at, lanes] = jnp.concatenate([k[0] for k in kept], axis=0).astype(BF16)
                    states_im[at, lanes] = jnp.concatenate([k[1] for k in kept], axis=0).astype(BF16)
                return re, im

            re, im = lax.fori_loop(0, steps // 4, body, start)
            if not keep:
                ends[0, :, lanes] = re
                ends[1, :, lanes] = im

    scan(None, False)

    place = iota((CHUNKS, modes), 0) & (quarters - 1)
    grown = jnp.exp(vec[pl.ds(16, CHUNKS), :])
    a = (grown * vec[2:3, :], grown * vec[3:4, :])
    b = (ends[0], ends[1])
    d = 1
    while d < quarters:
        ok = place >= d
        a_old = tuple(pltpu.roll(v, d, axis=0) for v in a)
        b_old = tuple(pltpu.roll(v, d, axis=0) for v in b)
        add = cmul(a, b_old)
        new_a = cmul(a, a_old)
        b = tuple(jnp.where(ok, v + w, v) for v, w in zip(b, add))
        a = tuple(jnp.where(ok, w, v) for v, w in zip(a, new_a))
        d *= 2
    for c in range(2):
        for s in range(sequences):
            last = (s + 1) * quarters - 1
            for k in range(nx):
                for blk in range(blocks):
                    lo = k * part + blk * LANES
                    row = c * tile + s * blocks + blk
                    sum_stage[k, row : row + 1, :] = b[c][last : last + 1, lo : lo + LANES]
    sum_pack[...] = sum_stage[...].astype(BF16)
    for i, (value, empty) in enumerate(((a[0], 1.0), (a[1], 0.0), (b[0], 0.0), (b[1], 0.0))):
        before[i] = jnp.where(place == 0, empty, pltpu.roll(value, 1, axis=0))
    sum_sends = to_x(sum_pack, sum_x, sx_send, sx_recv)
    for copy in sum_sends:
        copy.start()
    sum_x[pl.ds(mx, 1)] = sum_pack[pl.ds(mx, 1)]

    for copy in log_sends:
        copy.wait()
    log_row[...] = jnp.sum(log_x[...], axis=0)
    log_z_sends = to_block(log_row, log_z, lz_send, lz_recv)
    start_block(log_z_sends)
    for c in range(2):
        for blk in range(blocks):
            lanes = pl.ds(pl.multiple_of(mx * part + blk * LANES, LANES), LANES)
            value = vec[4 + c : 5 + c, lanes]
            for s in range(sequences):
                row = s * blocks + blk
                lam_pack[c, row : row + 1, :] = value
    lam_dev = (lam_pack[0], lam_pack[1])
    one = (jnp.ones((tile, LANES), F32), jnp.zeros((tile, LANES), F32))
    lam_pow = [one]
    for _ in range(nx):
        lam_pow.append(cmul(lam_pow[-1], lam_dev))

    def grow(logs, base):
        size = jnp.exp(logs)
        return size * base[0], size * base[1]

    def halves(value):
        wide = value.astype(F32)
        return wide[:tile], wide[tile:]

    def plus(u, v):
        return u[0] + v[0], u[1] + v[1]

    logs = [log_x[k] for k in range(nx)]
    to_end, to_start = [None] * nx, [None] * nx
    gone = jnp.zeros((tile, LANES), F32)
    for k in range(nx - 1, -1, -1):
        to_end[k] = grow(gone, lam_pow[nx - 1 - k])
        gone = gone + logs[k]
    gone = jnp.zeros((tile, LANES), F32)
    for k in range(nx):
        to_start[k] = grow(gone, lam_pow[k])
        gone = gone + logs[k]

    loads[9].wait()
    project(tp, gate_w, raw_gate)
    project(1 - tp, gate_w, raw_gate)
    gates = dot(scan_order(rows), raw_gate[...].reshape(rows, width))
    opened[...] = 1.0 / (1.0 + jnp.exp(-gates))

    for copy in loads[10:14]:
        copy.wait()
    two_re, two_im = doubled(read_re_ref[...]), doubled(read_im_ref[...])

    def coef(g):
        lo = g // per_tile * LANES
        return vec[6:7, lo : lo + LANES], vec[7:8, lo : lo + LANES]

    def lifted_re(g, at):
        kr, ki = coef(g)
        return two_re[at] * kr - two_im[at] * ki

    def lifted_im(g, at):
        kr, ki = coef(g)
        return -(two_re[at] * ki + two_im[at] * kr)

    block_diagonal(lift_re, lifted_re)
    block_diagonal(lift_im, lifted_im)

    for copy in sum_sends:
        copy.wait()
    came = [halves(sum_x[k]) for k in range(nx)]
    total = cmul(to_end[0], came[0])
    for k in range(1, nx):
        total = plus(total, cmul(to_end[k], came[k]))
    sum_row[...] = jnp.concatenate(total, axis=0).astype(BF16)
    sum_z_sends = to_block(sum_row, sum_z, sz_send, sz_recv)
    start_block(sum_z_sends)

    inside = [None] * nx
    inside[0] = (jnp.zeros((tile, LANES), F32), jnp.zeros((tile, LANES), F32))
    for k in range(1, nx):
        inside[k] = plus(cmul(inside[k - 1], grow(logs[k - 1], lam_dev)), came[k - 1])
    recv_block(log_z_sends)
    zero = jnp.zeros((tile, LANES), F32)
    gone, power, weights = zero, one, {}
    for d in range(1, BLOCK):
        weights[d] = grow(gone, power)
        gone = gone + log_z[d - 1]
        power = tuple(jnp.where(d <= place_z, n, o) for n, o in zip(cmul(power, lam_pow[nx]), power))
    through = grow(gone, power)
    log_block[...] = gone + jnp.sum(log_x[...], axis=0)
    log_far_sends = to_later(log_block, log_far, lf_send, lf_recv)
    start_later(log_far_sends)
    lam_block = one
    for _ in range(BLOCK):
        lam_block = cmul(lam_block, lam_pow[nx])

    recv_block(sum_z_sends)
    carry = (zero, zero)
    for d in range(1, BLOCK):
        carry = plus(carry, cmul(weights[d], halves(sum_z[d - 1])))
    filled = plus(cmul(carry, grow(jnp.sum(log_x[...], axis=0), lam_pow[nx])), total)
    sum_block[...] = jnp.concatenate(filled, axis=0).astype(BF16)
    sum_far_sends = to_later(sum_block, sum_far, sf_send, sf_recv)
    start_later(sum_far_sends)

    recv_later(log_far_sends)
    gone, power = zero, one
    for e in range(1, count):
        weights[e] = cmul(through, grow(gone, power))
        gone = gone + log_far[e - 1]
        power = cmul(power, lam_block)
    recv_later(sum_far_sends)
    for e in range(1, count):
        carry = plus(carry, cmul(weights[e], halves(sum_far[e - 1])))
    for k in range(nx):
        carry_pack[k] = jnp.concatenate(plus(cmul(carry, to_start[k]), inside[k]), axis=0).astype(BF16)
    carry_sends = to_x(carry_pack, carry_x, cx_send, cx_recv)
    for copy in carry_sends:
        copy.start()
    carry_x[pl.ds(mx, 1)] = carry_pack[pl.ds(mx, 1)]
    for copy in carry_sends:
        copy.wait()
    upper = iota((CHUNKS, LANES), 0) < quarters
    for k in range(nx):
        got = carry_x[k].astype(F32)
        for blk in range(blocks):
            lo = k * part + blk * LANES
            lanes = slice(lo, lo + LANES)
            into = tuple(
                jnp.where(upper, got[c * tile + blk][None], got[c * tile + blocks + blk][None]) for c in range(2)
            )
            moved = cmul((before[0, :, lanes], before[1, :, lanes]), into)
            init[0, :, lanes] = before[2, :, lanes] + moved[0]
            init[1, :, lanes] = before[3, :, lanes] + moved[1]

    w_copies[1].start()
    scan(init, True)

    parts = []
    for h in range(2):
        use = slice(h * hw, (h + 1) * hw)
        lanes = slice(h * half, (h + 1) * half)
        mixed = dot_t(states_re[:, lanes], lift_re[use, :]) + dot_t(states_im[:, lanes], lift_im[use, :])
        mixed = mixed + skip_ref[:, use] * inputs[:, use].astype(F32)
        gelu = 0.5 * mixed * (1.0 + lax.erf(mixed * math.sqrt(0.5)))
        parts.append((gelu * opened[:, use]).astype(BF16))
    back = natural_order(rows)
    for h in range(2):
        act[:, :, h * hw : (h + 1) * hw] = dot(back, parts[h]).astype(BF16).reshape(sequences, 2 * own, hw)
    a_copy = remote(act.at[:, theirs, :], far_ref, a_send, a_recv, partner)
    a_copy.start()
    near = act[:, mine, :].astype(F32).reshape(sequences * own, width)
    square_ref[...] = jnp.broadcast_to(jnp.sum(near * near, axis=-1, keepdims=True), square_ref.shape)
    near = (near * gain_ref[:, pl.ds(pl.multiple_of(tp * width, width), width)]).astype(BF16)
    loads[14].wait()
    for c in range(depth // 512):
        lanes = slice(c * 512, (c + 1) * 512)
        near_ref[:, lanes] = dot(near, out_w[:, lanes])
    for copy in w_copies:
        copy.wait()
    a_copy.wait()

    sent_block(log_z_sends)
    sent_block(sum_z_sends)
    sent_later(log_far_sends)
    sent_later(sum_far_sends)


def finish_kernel(near_ref, square_ref, far_ref, gain_ref, far_w_ref, out_hbm, staged, sem):
    tp = lax.axis_index("tp")
    sequences, own, width = far_ref.shape
    depth = far_w_ref.shape[1]

    far = far_ref[...].astype(F32).reshape(sequences * own, width)
    square = square_ref[:, :1] + jnp.sum(far * far, axis=-1, keepdims=True)
    scale = lax.rsqrt(square * (0.5 / width) + EPS)
    far = (far * gain_ref[:, pl.ds(pl.multiple_of((1 - tp) * width, width), width)]).astype(BF16)
    copies = []
    for c in range(depth // 512):
        lanes = slice(c * 512, (c + 1) * 512)
        result = (near_ref[:, lanes] + dot(far, far_w_ref[:, lanes])) * scale
        staged[:, :, lanes] = result.astype(BF16).reshape(sequences, own, 512)
        copies.append(pltpu.make_async_copy(staged.at[:, :, lanes], out_hbm.at[:, :, lanes], sem.at[c]))
        copies[-1].start()
    for copy in copies:
        copy.wait()


def vmem():
    return pl.BlockSpec(memory_space=pltpu.VMEM)


def hbm():
    return pl.BlockSpec(memory_space=pl.ANY)


def shards(
    layer_input,
    norm_gain,
    in_weight,
    gate_weight,
    rate_real,
    rate_imag,
    log_step,
    input_real,
    input_imag,
    output_real,
    output_imag,
    skip_weight,
    decay_offset,
    channel_gain,
    out_weight,
):
    nz, nx = lax.axis_size("sp_0"), lax.axis_size("sp_1")
    sequences, own, depth = layer_input.shape
    width = in_weight.shape[1]
    groups, states = rate_real.shape
    modes = groups * states
    rows = sequences * 2 * own
    dma = pltpu.SemaphoreType.DMA
    later = nz // BLOCK - 1
    tile = sequences * (modes // nx // LANES)
    f32 = functools.partial(pltpu.VMEM, dtype=F32)
    b16 = functools.partial(pltpu.VMEM, dtype=BF16)
    near, square, far, far_w = pl.pallas_call(
        mixer_kernel,
        name="mixer",
        out_shape=[
            pltpu.VMEM((sequences * own, depth), F32),
            pltpu.VMEM((sequences * own, LANES), F32),
            pltpu.VMEM((sequences, own, width), BF16),
            pltpu.VMEM((width, depth), BF16),
        ],
        in_specs=[pl.BlockSpec(memory_space=pltpu.HBM)] * 15,
        out_specs=[vmem()] * 4,
        scratch_shapes=[
            b16((sequences, 2 * own, depth)),
            b16((depth, width)),
            b16((depth, width)),
            f32((1, depth)),
            f32((groups, states)),
            f32((groups, states)),
            f32((1, groups)),
            b16((width, states)),
            b16((width, states)),
            b16((width, states)),
            b16((width, states)),
            f32((1, width)),
            f32((sequences, groups, 2 * own)),
            f32((1, 2 * width)),
            b16((width, depth)),
            b16((2, sequences * own, depth)),
            f32((2, sequences * own, 256)),
            b16((sequences, 2 * own, width)),
            b16((sequences, 2 * own, width)),
            b16((rows, width)),
            f32((rows, width)),
            f32((rows, modes)),
            b16((width, modes // 2)),
            b16((width, modes // 2)),
            f32((rows, modes)),
            f32((rows, modes)),
            b16((rows, modes)),
            b16((rows, modes)),
            b16((width, modes // 2)),
            b16((width, modes // 2)),
            f32((24, modes)),
            f32((2, CHUNKS, modes)),
            f32((4, CHUNKS, modes)),
            f32((2, CHUNKS, modes)),
            f32((nx, tile, LANES)),
            f32((nx, tile, LANES)),
            f32((tile, LANES)),
            f32((BLOCK - 1, tile, LANES)),
            f32((tile, LANES)),
            f32((later, tile, LANES)),
            f32((nx, 2 * tile, LANES)),
            b16((nx, 2 * tile, LANES)),
            b16((nx, 2 * tile, LANES)),
            b16((2 * tile, LANES)),
            b16((BLOCK - 1, 2 * tile, LANES)),
            b16((2 * tile, LANES)),
            b16((later, 2 * tile, LANES)),
            b16((nx, 2 * tile, LANES)),
            b16((nx, 2 * tile, LANES)),
            f32((2, tile, LANES)),
            b16((sequences, 2 * own, width)),
            dma((15,)),
            dma,
            dma,
            dma((2,)),
            dma((2,)),
            dma((nx - 1,)),
            dma((nx - 1,)),
            dma((BLOCK - 1,)),
            dma((BLOCK - 1,)),
            dma((nz - BLOCK,)),
            dma((later,)),
            dma((nx - 1,)),
            dma((nx - 1,)),
            dma((BLOCK - 1,)),
            dma((BLOCK - 1,)),
            dma((nz - BLOCK,)),
            dma((later,)),
            dma((nx - 1,)),
            dma((nx - 1,)),
            dma,
            dma,
        ],
        compiler_params=pltpu.CompilerParams(collective_id=0, has_side_effects=True, vmem_limit_bytes=67043328 - (5 << 20)),
    )(
        layer_input,
        in_weight,
        gate_weight,
        out_weight,
        norm_gain[None],
        rate_real,
        rate_imag,
        log_step[None],
        jnp.swapaxes(input_real, 1, 2).reshape(width, states),
        jnp.swapaxes(input_imag, 1, 2).reshape(width, states),
        output_real.reshape(width, states),
        output_imag.reshape(width, states),
        skip_weight[None],
        jnp.swapaxes(decay_offset, 1, 2),
        channel_gain[None],
    )
    return pl.pallas_call(
        finish_kernel,
        name="finish",
        out_shape=jax.ShapeDtypeStruct((sequences, own, depth), BF16),
        in_specs=[vmem()] * 5,
        out_specs=hbm(),
        scratch_shapes=[b16((sequences, own, depth)), dma((depth // 512,))],
        compiler_params=pltpu.CompilerParams(vmem_limit_bytes=16 << 20),
    )(near, square, far, channel_gain[None], far_w)


def solution(mesh):
    torus = Mesh(
        mesh.devices.reshape(mesh.shape["grp"], 16, 4, mesh.shape["tp"]),
        ("grp", "sp_0", "sp_1", "tp"),
    )
    return build(torus)


def build(torus):
    in_specs = (
        P("grp", SP_TP, None),
        P(),
        P(None, "tp"),
        P(None, "tp"),
        P("tp", None),
        P("tp", None),
        P("tp"),
        P("tp", None, None),
        P("tp", None, None),
        P("tp", None, None),
        P("tp", None, None),
        P("tp"),
        P("grp", SP, "tp"),
        P(),
        P("tp", None),
    )
    out_specs = P("grp", SP_TP, None)
    return jax.shard_map(shards, mesh=torus, in_specs=in_specs, out_specs=out_specs, check_vma=False)
```

```python
import functools
import math

import jax
import jax.numpy as jnp
from jax import lax
from jax.experimental import pallas as pl
from jax.experimental.pallas import tpu as pltpu
from jax.sharding import Mesh
from jax.sharding import PartitionSpec as P

SP = ("sp_0", "sp_1")
SP_TP = ("sp_0", "sp_1", "tp")
MESH = pl.DeviceIdType.MESH
F32 = jnp.float32
BF16 = jnp.bfloat16
EPS = 1e-06
LANES = 128
CHUNKS = 8
BLOCK = 4
UNROLL = 8


def dot(a, b):
    return jnp.dot(a, b, preferred_element_type=F32)


def dot_t(a, b):
    return lax.dot_general(a, b, (((1,), (1,)), ((), ())), preferred_element_type=F32)


def iota(shape, dim):
    return lax.broadcasted_iota(jnp.int32, shape, dim)


def one_hot(cond):
    return jnp.where(cond, 1.0, 0.0).astype(BF16)


def split(value):
    high = value.astype(BF16)
    rest = value - high.astype(F32)
    middle = rest.astype(BF16)
    low = (rest - middle.astype(F32)).astype(BF16)
    return high, middle, low


def exact_dot(value, table):
    high, middle, low = split(value)
    return dot(high, table) + dot(middle, table) + dot(low, table)


def cmul(a, b):
    return a[0] * b[0] - a[1] * b[1], a[0] * b[1] + a[1] * b[0]


def small_expm1(x):
    series = x * (1.0 + x * (1 / 2 + x * (1 / 6 + x * (1 / 24 + x * (1 / 120 + x * (1 / 720 + x / 5040))))))
    return jnp.where(x > -0.3, series, jnp.exp(x) - 1.0)


def scan_order(rows):
    steps = rows // CHUNKS
    at = iota((rows, rows), 0)
    return one_hot(iota((rows, rows), 1) == (at & (CHUNKS - 1)) * steps + (at >> 3))


def natural_order(rows):
    steps = rows // CHUNKS
    at = iota((rows, rows), 1)
    return one_hot(iota((rows, rows), 0) == (at & (CHUNKS - 1)) * steps + (at >> 3))


def small_sine(x):
    q = x * x
    return x * (1.0 + q * (-1 / 6 + q * (1 / 120 + q * (-1 / 5040 + q * (1 / 362880 - q / 39916800)))))


def small_cosine(x):
    q = x * x
    return 1.0 + q * (-1 / 2 + q * (1 / 24 + q * (-1 / 720 + q * (1 / 40320 + q * (-1 / 3628800 + q / 479001600)))))


def mixer_kernel(
    x_hbm,
    in_w_hbm,
    gate_w_hbm,
    out_w_hbm,
    norm_gain_hbm,
    rate_re_hbm,
    rate_im_hbm,
    log_step_hbm,
    table_re_hbm,
    table_im_hbm,
    read_re_hbm,
    read_im_hbm,
    skip_hbm,
    offset_hbm,
    gain_hbm,
    near_ref,
    square_ref,
    far_ref,
    far_w_ref,
    tokens,
    in_w,
    gate_w,
    norm_gain_ref,
    rate_re_ref,
    rate_im_ref,
    log_step_ref,
    table_re_ref,
    table_im_ref,
    read_re_ref,
    read_im_ref,
    skip_ref,
    offset_ref,
    gain_ref,
    out_w,
    normed,
    scales,
    raw_in,
    raw_gate,
    inputs,
    opened,
    mags,
    trans_re,
    trans_im,
    wide_re,
    wide_im,
    drive_re,
    drive_im,
    states_re,
    states_im,
    lift_re,
    lift_im,
    vec,
    ends,
    before,
    init,
    log_pack,
    log_x,
    log_row,
    log_z,
    log_block,
    log_far,
    sum_stage,
    sum_pack,
    sum_x,
    sum_row,
    sum_z,
    sum_block,
    sum_far,
    lam_pack,
    act,
    load_sem,
    x_send,
    x_recv,
    w_send,
    w_recv,
    lx_send,
    lx_recv,
    lz_send,
    lz_recv,
    lf_send,
    lf_recv,
    sx_send,
    sx_recv,
    sz_send,
    sz_recv,
    sf_send,
    sf_recv,
    a_send,
    a_recv,
):
    nz, nx = lax.axis_size("sp_0"), lax.axis_size("sp_1")
    mz, mx, tp = lax.axis_index("sp_0"), lax.axis_index("sp_1"), lax.axis_index("tp")
    sequences, own, depth = x_hbm.shape
    width = in_w_hbm.shape[1]
    rows = sequences * 2 * own
    groups, states = rate_re_hbm.shape
    channels = width // groups
    modes = groups * states
    steps = rows // CHUNKS
    quarters = CHUNKS // sequences
    tile = CHUNKS
    blocks = tile // sequences
    part = blocks * LANES
    packs = modes // part
    half = modes // 2
    hw = width // 2
    mine = pl.ds(pl.multiple_of(tp * own, own), own)
    theirs = pl.ds(pl.multiple_of((1 - tp) * own, own), own)
    partner = {"tp": 1 - tp}

    loads = [
        pltpu.make_async_copy(source, target, load_sem.at[i])
        for i, (source, target) in enumerate(
            (
                (x_hbm, tokens.at[:, mine, :]),
                (offset_hbm, offset_ref),
                (rate_re_hbm, rate_re_ref),
                (rate_im_hbm, rate_im_ref),
                (log_step_hbm, log_step_ref),
                (norm_gain_hbm, norm_gain_ref),
                (table_re_hbm, table_re_ref),
                (table_im_hbm, table_im_ref),
                (in_w_hbm, in_w),
                (gate_w_hbm, gate_w),
                (read_re_hbm, read_re_ref),
                (read_im_hbm, read_im_ref),
                (skip_hbm, skip_ref),
                (gain_hbm, gain_ref),
                (out_w_hbm, out_w),
            )
        )
    ]
    for copy in loads:
        copy.start()

    for ref in (log_z, sum_z, log_far, sum_far):
        ref[...] = jnp.zeros_like(ref)
    barrier = pltpu.get_barrier_semaphore()
    pl.semaphore_signal(barrier, inc=1, device_id=partner, device_id_type=MESH)
    for d in range(1, nx):
        pl.semaphore_signal(barrier, inc=1, device_id={"sp_1": lax.rem(mx + d, nx)}, device_id_type=MESH)
    count = nz // BLOCK
    block, place_z = mz // BLOCK, mz % BLOCK
    ends_block = place_z == BLOCK - 1

    def signal_z(z):
        pl.semaphore_signal(barrier, inc=1, device_id={"sp_0": z}, device_id_type=MESH)

    for d in range(1, BLOCK):
        pl.when(d <= place_z)(lambda d=d: signal_z(mz - d))
    for e in range(1, count):
        pl.when(e <= block)(lambda e=e: signal_z((block - e) * BLOCK + BLOCK - 1))

    def remote(source, target, send, recv, device):
        return pltpu.make_async_remote_copy(
            src_ref=source, dst_ref=target, send_sem=send, recv_sem=recv, device_id=device, device_id_type=MESH
        )

    def to_x(source, target, send, recv):
        made = []
        for d in sorted(range(1, nx), key=lambda d: -min(d, nx - d)):
            k = lax.rem(mx + d, nx)
            made.append(remote(source, target.at[mx], send.at[d - 1], recv.at[d - 1], {"sp_1": k}))
        return made

    def to_block(source, target, send, recv):
        return {
            d: remote(source, target.at[d - 1], send.at[d - 1], recv.at[d - 1], {"sp_0": lax.rem(mz + d, nz)})
            for d in range(1, BLOCK)
        }

    def to_later(source, target, send, recv):
        made = {}
        for d in sorted(range(1, nz - BLOCK + 1), key=lambda d: min(d, nz - d)):
            e = (d + BLOCK - 1) // BLOCK - 1
            made[d] = remote(source, target.at[e], send.at[d - 1], recv.at[e], {"sp_0": lax.rem(mz + d, nz)})
        return made

    def start_block(made):
        for d, copy in made.items():
            pl.when(place_z + d < BLOCK)(copy.start)

    def start_later(made):
        @pl.when(ends_block)
        def _():
            for d, copy in made.items():
                pl.when(mz + d < nz)(copy.start)

    def recv_block(made):
        for d, copy in made.items():
            pl.when(d <= place_z)(copy.wait_recv)

    def recv_later(made):
        for e in range(1, count):
            pl.when(e <= block)(made[(e - 1) * BLOCK + 1].wait_recv)

    def sent_block(made):
        for d, copy in made.items():
            pl.when(place_z + d < BLOCK)(copy.wait_send)

    def sent_later(made):
        @pl.when(ends_block)
        def _():
            for d, copy in made.items():
                pl.when(mz + d < nz)(copy.wait_send)

    for ref in (wide_re, wide_im, lift_re, lift_im):
        ref[...] = jnp.zeros_like(ref)

    for copy in loads[1:6]:
        copy.wait()
    spread_g = one_hot((iota((groups, modes), 1) >> 6) == iota((groups, modes), 0))
    spread_p = one_hot((iota((states, modes), 1) & (states - 1)) == iota((states, modes), 0))
    offsets = jnp.concatenate([offset_ref[s].T for s in range(sequences)], axis=0)
    sums = jnp.sum(offsets.reshape(CHUNKS, steps, groups), axis=1)
    step_size = jnp.broadcast_to(jnp.exp(log_step_ref[...]), (8, groups))
    spread = exact_dot(jnp.concatenate([sums, step_size], axis=0), spread_g)
    chunk_logs, step = spread[:CHUNKS], spread[CHUNKS : CHUNKS + 1]
    vec[pl.ds(16, CHUNKS), :] = chunk_logs
    for s in range(sequences):
        total = jnp.sum(chunk_logs[s * quarters : (s + 1) * quarters], axis=0, keepdims=True)
        for k in range(packs):
            for b in range(blocks):
                lo = k * part + b * LANES
                row = s * blocks + b
                log_pack[k, row : row + 1, :] = total[:, lo : lo + LANES]

    def norm(side):
        for s in range(sequences):
            for r in range(0, own, 32):
                wide = tokens[s, pl.ds(pl.multiple_of(side * own + r, 32), 32), :].astype(F32)
                at = slice(s * own + r, s * own + r + 32)
                normed[side, at, :] = (wide * norm_gain_ref[...]).astype(BF16)
                scale = lax.rsqrt(jnp.mean(wide * wide, axis=-1, keepdims=True) + EPS)
                scales[side, at, :] = jnp.broadcast_to(scale, (32, 256))

    def project(side, weight, out):
        @pl.loop(0, width // 256)
        def _(c):
            lanes = pl.ds(pl.multiple_of(c * 256, 256), 256)
            product = dot(normed[side], weight[:, lanes]) * scales[side]
            at = pl.ds(pl.multiple_of(side * own, own), own)
            out[:, at, lanes] = product.reshape(sequences, own, 256).astype(BF16)

    later = jnp.where(ends_block, nz - 1 - mz, 0)
    loads[0].wait()
    pl.semaphore_wait(barrier, nx + BLOCK - 1 - place_z + later)
    log_sends = to_x(log_pack, log_x, lx_send, lx_recv)
    for copy in log_sends:
        copy.start()
    x_copy = remote(tokens.at[:, mine, :], tokens.at[:, mine, :], x_send, x_recv, partner)
    x_copy.start()
    log_x[mx] = log_pack[...]
    norm(tp)

    on_group = (iota((groups, modes), 1) >> 6) == iota((groups, modes), 0)
    rates = exact_dot(jnp.concatenate([rate_re_ref[...], rate_im_ref[...]], axis=0), spread_p)
    rate_re = jnp.sum(jnp.where(on_group, rates[:groups], 0.0), axis=0, keepdims=True)
    rate_im = jnp.sum(jnp.where(on_group, rates[groups:], 0.0), axis=0, keepdims=True)
    real_step, angle = rate_re * step, rate_im * step
    size = jnp.exp(real_step)
    cosine, sine = small_cosine(angle), small_sine(angle)
    half_sine = small_sine(0.5 * angle)
    top_re = small_expm1(real_step) * cosine - 2.0 * half_sine * half_sine
    top_im = size * sine
    inverse = 1.0 / (rate_re * rate_re + rate_im * rate_im)
    coef_re = (top_re * rate_re + top_im * rate_im) * inverse
    coef_im = (top_im * rate_re - top_re * rate_im) * inverse
    lam = (size * cosine, size * sine)
    power = lam
    for _ in range(int(math.log2(steps))):
        power = cmul(power, power)
    lam_chunk = power
    for _ in range(int(math.log2(quarters))):
        power = cmul(power, power)
    for i, value in enumerate((*lam, *lam_chunk, *power, coef_re, coef_im)):
        vec[i : i + 1, :] = value

    order = scan_order(rows)
    pieces = [dot(order, piece) for piece in split(jnp.exp(offsets))]
    spread_3 = one_hot((iota((3 * groups, modes), 1) >> 6) == (iota((3 * groups, modes), 0) & (groups - 1)))
    mags[...] = dot(jnp.concatenate(pieces, axis=1).astype(BF16), spread_3)

    per_tile = LANES // states

    def doubled(value):
        return jnp.concatenate([value.astype(F32)] * per_tile, axis=1)

    on_lane = iota((channels, LANES), 1) // states

    def block_diagonal(target, value):
        for g in range(groups):
            at = slice(g * channels, (g + 1) * channels)
            lo = (g % (groups // 2)) // per_tile * LANES
            kept = jnp.where(on_lane == g % per_tile, value(g, at), 0.0)
            target[at, lo : lo + LANES] = kept.astype(BF16)

    for copy in loads[6:8]:
        copy.wait()
    two_re, two_im = doubled(table_re_ref[...]), doubled(table_im_ref[...])
    block_diagonal(wide_re, lambda g, at: two_re[at])
    block_diagonal(wide_im, lambda g, at: two_im[at])

    loads[8].wait()
    project(tp, in_w, raw_in)

    x_copy.wait()
    w_copies = [
        remote(out_w_hbm.at[at], far_w_ref.at[at], w_send.at[i], w_recv.at[i], partner)
        for i, at in enumerate((pl.ds(0, 3 * width // 4), pl.ds(3 * width // 4, width // 4)))
    ]
    w_copies[0].start()
    norm(1 - tp)
    project(1 - tp, in_w, raw_in)
    inputs[...] = dot(order, raw_in[...].reshape(rows, width)).astype(BF16)

    for h in range(2):
        use, lanes = slice(h * hw, (h + 1) * hw), slice(h * half, (h + 1) * half)
        drive_re[:, lanes] = dot(inputs[:, use], wide_re[use, :])
        drive_im[:, lanes] = dot(inputs[:, use], wide_im[use, :])

    span = 512

    def scan(first, keep):
        @pl.loop(0, modes // span)
        def _(c):
            lanes = pl.ds(pl.multiple_of(c * span, span), span)
            lr = jnp.broadcast_to(vec[0:1, lanes], (UNROLL * CHUNKS, span))
            li = jnp.broadcast_to(vec[1:2, lanes], (UNROLL * CHUNKS, span))
            if first is None:
                start = (jnp.zeros((CHUNKS, span), F32), jnp.zeros((CHUNKS, span), F32))
            else:
                start = (first[0, :, lanes], first[1, :, lanes])

            def body(t, now):
                re, im = now
                at = pl.ds(pl.multiple_of(t * UNROLL * CHUNKS, UNROLL * CHUNKS), UNROLL * CHUNKS)
                dr, di = drive_re[at, lanes], drive_im[at, lanes]
                if keep:
                    ar, ai = trans_re[at, lanes], trans_im[at, lanes]
                else:
                    m = mags[at, lanes]
                    ar, ai = m * lr, m * li
                    trans_re[at, lanes] = ar
                    trans_im[at, lanes] = ai
                kept = []
                for u in range(UNROLL):
                    use = slice(u * CHUNKS, (u + 1) * CHUNKS)
                    re, im = (
                        ar[use] * re - ai[use] * im + dr[use],
                        ar[use] * im + ai[use] * re + di[use],
                    )
                    kept.append((re, im))
                if keep:
                    states_re[at, lanes] = jnp.concatenate([k[0] for k in kept], axis=0).astype(BF16)
                    states_im[at, lanes] = jnp.concatenate([k[1] for k in kept], axis=0).astype(BF16)
                return re, im

            re, im = lax.fori_loop(0, steps // UNROLL, body, start)
            if not keep:
                ends[0, :, lanes] = re
                ends[1, :, lanes] = im

    scan(None, False)

    place = iota((CHUNKS, modes), 0) & (quarters - 1)
    grown = jnp.exp(vec[pl.ds(16, CHUNKS), :])
    a = (grown * vec[2:3, :], grown * vec[3:4, :])
    b = (ends[0], ends[1])
    d = 1
    while d < quarters:
        ok = place >= d
        a_old = tuple(pltpu.roll(v, d, axis=0) for v in a)
        b_old = tuple(pltpu.roll(v, d, axis=0) for v in b)
        add = cmul(a, b_old)
        new_a = cmul(a, a_old)
        b = tuple(jnp.where(ok, v + w, v) for v, w in zip(b, add))
        a = tuple(jnp.where(ok, w, v) for v, w in zip(a, new_a))
        d *= 2
    for c in range(2):
        for s in range(sequences):
            last = (s + 1) * quarters - 1
            for k in range(packs):
                for blk in range(blocks):
                    lo = k * part + blk * LANES
                    row = c * tile + s * blocks + blk
                    sum_stage[k, row : row + 1, :] = b[c][last : last + 1, lo : lo + LANES]
    sum_pack[...] = sum_stage[...].astype(BF16)
    for i, (value, empty) in enumerate(((a[0], 1.0), (a[1], 0.0), (b[0], 0.0), (b[1], 0.0))):
        before[i] = jnp.where(place == 0, empty, pltpu.roll(value, 1, axis=0))
    sum_sends = to_x(sum_pack, sum_x, sx_send, sx_recv)
    for copy in sum_sends:
        copy.start()
    sum_x[mx] = sum_pack[...]

    for copy in log_sends:
        copy.wait()
    log_row[...] = jnp.sum(log_x[...], axis=0)
    log_z_sends = to_block(log_row, log_z, lz_send, lz_recv)
    start_block(log_z_sends)
    for c in range(2):
        for k in range(packs):
            for blk in range(blocks):
                lo = k * part + blk * LANES
                for s in range(sequences):
                    row = s * blocks + blk
                    lam_pack[c, k, row : row + 1, :] = vec[4 + c : 5 + c, lo : lo + LANES]
    lam_dev = (lam_pack[0], lam_pack[1])
    zero = jnp.zeros((packs, tile, LANES), F32)
    one = (jnp.ones((packs, tile, LANES), F32), zero)
    lam_pow = [one]
    for _ in range(nx):
        lam_pow.append(cmul(lam_pow[-1], lam_dev))

    def grow(logs, base):
        size = jnp.exp(logs)
        return size * base[0], size * base[1]

    def halves(value):
        wide = value.astype(F32)
        return wide[:, :tile], wide[:, tile:]

    def plus(u, v):
        return u[0] + v[0], u[1] + v[1]

    logs = [log_x[k] for k in range(nx)]
    to_end = [None] * nx
    gone = zero
    for k in range(nx - 1, -1, -1):
        to_end[k] = grow(gone, lam_pow[nx - 1 - k])
        gone = gone + logs[k]
    row_logs = gone
    gone, power = zero, one
    for k in range(nx - 1):
        gone = jnp.where(k < mx, gone + logs[k], gone)
        power = tuple(jnp.where(k < mx, n, o) for n, o in zip(lam_pow[k + 1], power))
    to_own = grow(gone, power)

    loads[9].wait()
    project(tp, gate_w, raw_gate)
    project(1 - tp, gate_w, raw_gate)
    gates = dot(scan_order(rows), raw_gate[...].reshape(rows, width))
    opened[...] = 1.0 / (1.0 + jnp.exp(-gates))

    for copy in loads[10:14]:
        copy.wait()
    two_re, two_im = doubled(read_re_ref[...]), doubled(read_im_ref[...])

    def coef(g):
        lo = g // per_tile * LANES
        return vec[6:7, lo : lo + LANES], vec[7:8, lo : lo + LANES]

    def lifted_re(g, at):
        kr, ki = coef(g)
        return two_re[at] * kr - two_im[at] * ki

    def lifted_im(g, at):
        kr, ki = coef(g)
        return -(two_re[at] * ki + two_im[at] * kr)

    block_diagonal(lift_re, lifted_re)
    block_diagonal(lift_im, lifted_im)

    recv_block(log_z_sends)
    gone, power, weights = zero, one, {}
    for d in range(1, BLOCK):
        weights[d] = grow(gone, power)
        gone = gone + log_z[d - 1]
        power = tuple(jnp.where(d <= place_z, n, o) for n, o in zip(cmul(power, lam_pow[nx]), power))
    through = grow(gone, power)
    log_block[...] = gone + row_logs
    log_far_sends = to_later(log_block, log_far, lf_send, lf_recv)
    start_later(log_far_sends)
    lam_block = one
    for _ in range(BLOCK):
        lam_block = cmul(lam_block, lam_pow[nx])

    for copy in sum_sends:
        copy.wait()
    came = [halves(sum_x[k]) for k in range(nx)]
    total = cmul(to_end[0], came[0])
    for k in range(1, nx):
        total = plus(total, cmul(to_end[k], came[k]))
    sum_row[...] = jnp.concatenate(total, axis=1).astype(BF16)
    sum_z_sends = to_block(sum_row, sum_z, sz_send, sz_recv)
    start_block(sum_z_sends)

    inside = (zero, zero)
    for k in range(nx - 1):
        new = plus(cmul(inside, grow(logs[k], lam_dev)), came[k])
        inside = tuple(jnp.where(k < mx, n, o) for n, o in zip(new, inside))
    recv_block(sum_z_sends)
    carry = (zero, zero)
    for d in range(1, BLOCK):
        carry = plus(carry, cmul(weights[d], halves(sum_z[d - 1])))
    filled = plus(cmul(carry, grow(row_logs, lam_pow[nx])), total)
    sum_block[...] = jnp.concatenate(filled, axis=1).astype(BF16)
    sum_far_sends = to_later(sum_block, sum_far, sf_send, sf_recv)
    start_later(sum_far_sends)

    recv_later(log_far_sends)
    gone, power = zero, one
    for e in range(1, count):
        weights[e] = cmul(through, grow(gone, power))
        gone = gone + log_far[e - 1]
        power = cmul(power, lam_block)
    recv_later(sum_far_sends)
    for e in range(1, count):
        carry = plus(carry, cmul(weights[e], halves(sum_far[e - 1])))
    carry = plus(cmul(carry, to_own), inside)
    upper = iota((CHUNKS, LANES), 0) < quarters
    for k in range(packs):
        for blk in range(blocks):
            lo = k * part + blk * LANES
            lanes = slice(lo, lo + LANES)
            into = tuple(
                jnp.where(upper, v[k, blk : blk + 1, :], v[k, blocks + blk : blocks + blk + 1, :]) for v in carry
            )
            moved = cmul((before[0, :, lanes], before[1, :, lanes]), into)
            init[0, :, lanes] = before[2, :, lanes] + moved[0]
            init[1, :, lanes] = before[3, :, lanes] + moved[1]

    w_copies[1].start()
    scan(init, True)

    parts = []
    for h in range(2):
        use = slice(h * hw, (h + 1) * hw)
        lanes = slice(h * half, (h + 1) * half)
        mixed = dot_t(states_re[:, lanes], lift_re[use, :]) + dot_t(states_im[:, lanes], lift_im[use, :])
        mixed = mixed + skip_ref[:, use] * inputs[:, use].astype(F32)
        gelu = 0.5 * mixed * (1.0 + lax.erf(mixed * math.sqrt(0.5)))
        parts.append((gelu * opened[:, use]).astype(BF16))
    back = natural_order(rows)
    for h in range(2):
        act[:, :, h * hw : (h + 1) * hw] = dot(back, parts[h]).astype(BF16).reshape(sequences, 2 * own, hw)
    a_copy = remote(act.at[:, theirs, :], far_ref, a_send, a_recv, partner)
    a_copy.start()
    near = act[:, mine, :].astype(F32).reshape(sequences * own, width)
    square_ref[...] = jnp.broadcast_to(jnp.sum(near * near, axis=-1, keepdims=True), square_ref.shape)
    near = (near * gain_ref[:, pl.ds(pl.multiple_of(tp * width, width), width)]).astype(BF16)
    loads[14].wait()
    for c in range(depth // 512):
        lanes = slice(c * 512, (c + 1) * 512)
        near_ref[:, lanes] = dot(near, out_w[:, lanes])
    for copy in w_copies:
        copy.wait()
    a_copy.wait()

    sent_block(log_z_sends)
    sent_block(sum_z_sends)
    sent_later(log_far_sends)
    sent_later(sum_far_sends)


def finish_kernel(near_ref, square_ref, far_ref, gain_ref, far_w_ref, out_hbm, staged, sem):
    tp = lax.axis_index("tp")
    sequences, own, width = far_ref.shape
    depth = far_w_ref.shape[1]

    far = far_ref[...].astype(F32).reshape(sequences * own, width)
    square = square_ref[:, :1] + jnp.sum(far * far, axis=-1, keepdims=True)
    scale = lax.rsqrt(square * (0.5 / width) + EPS)
    far = (far * gain_ref[:, pl.ds(pl.multiple_of((1 - tp) * width, width), width)]).astype(BF16)
    copies = []
    for c in range(depth // 512):
        lanes = slice(c * 512, (c + 1) * 512)
        result = (near_ref[:, lanes] + dot(far, far_w_ref[:, lanes])) * scale
        staged[:, :, lanes] = result.astype(BF16).reshape(sequences, own, 512)
        copies.append(pltpu.make_async_copy(staged.at[:, :, lanes], out_hbm.at[:, :, lanes], sem.at[c]))
        copies[-1].start()
    for copy in copies:
        copy.wait()


def vmem():
    return pl.BlockSpec(memory_space=pltpu.VMEM)


def hbm():
    return pl.BlockSpec(memory_space=pl.ANY)


def shards(
    layer_input,
    norm_gain,
    in_weight,
    gate_weight,
    rate_real,
    rate_imag,
    log_step,
    input_real,
    input_imag,
    output_real,
    output_imag,
    skip_weight,
    decay_offset,
    channel_gain,
    out_weight,
):
    nz, nx = lax.axis_size("sp_0"), lax.axis_size("sp_1")
    sequences, own, depth = layer_input.shape
    width = in_weight.shape[1]
    groups, states = rate_real.shape
    modes = groups * states
    rows = sequences * 2 * own
    dma = pltpu.SemaphoreType.DMA
    later = nz // BLOCK - 1
    tile = CHUNKS
    packs = modes // (tile // sequences * LANES)
    f32 = functools.partial(pltpu.VMEM, dtype=F32)
    b16 = functools.partial(pltpu.VMEM, dtype=BF16)
    near, square, far, far_w = pl.pallas_call(
        mixer_kernel,
        name="mixer",
        out_shape=[
            pltpu.VMEM((sequences * own, depth), F32),
            pltpu.VMEM((sequences * own, LANES), F32),
            pltpu.VMEM((sequences, own, width), BF16),
            pltpu.VMEM((width, depth), BF16),
        ],
        in_specs=[pl.BlockSpec(memory_space=pltpu.HBM)] * 15,
        out_specs=[vmem()] * 4,
        scratch_shapes=[
            b16((sequences, 2 * own, depth)),
            b16((depth, width)),
            b16((depth, width)),
            f32((1, depth)),
            f32((groups, states)),
            f32((groups, states)),
            f32((1, groups)),
            b16((width, states)),
            b16((width, states)),
            b16((width, states)),
            b16((width, states)),
            f32((1, width)),
            f32((sequences, groups, 2 * own)),
            f32((1, 2 * width)),
            b16((width, depth)),
            b16((2, sequences * own, depth)),
            f32((2, sequences * own, 256)),
            b16((sequences, 2 * own, width)),
            b16((sequences, 2 * own, width)),
            b16((rows, width)),
            f32((rows, width)),
            f32((rows, modes)),
            f32((rows, modes)),
            f32((rows, modes)),
            b16((width, modes // 2)),
            b16((width, modes // 2)),
            f32((rows, modes)),
            f32((rows, modes)),
            b16((rows, modes)),
            b16((rows, modes)),
            b16((width, modes // 2)),
            b16((width, modes // 2)),
            f32((24, modes)),
            f32((2, CHUNKS, modes)),
            f32((4, CHUNKS, modes)),
            f32((2, CHUNKS, modes)),
            f32((packs, tile, LANES)),
            f32((nx, packs, tile, LANES)),
            f32((packs, tile, LANES)),
            f32((BLOCK - 1, packs, tile, LANES)),
            f32((packs, tile, LANES)),
            f32((later, packs, tile, LANES)),
            f32((packs, 2 * tile, LANES)),
            b16((packs, 2 * tile, LANES)),
            b16((nx, packs, 2 * tile, LANES)),
            b16((packs, 2 * tile, LANES)),
            b16((BLOCK - 1, packs, 2 * tile, LANES)),
            b16((packs, 2 * tile, LANES)),
            b16((later, packs, 2 * tile, LANES)),
            f32((2, packs, tile, LANES)),
            b16((sequences, 2 * own, width)),
            dma((15,)),
            dma,
            dma,
            dma((2,)),
            dma((2,)),
            dma((nx - 1,)),
            dma((nx - 1,)),
            dma((BLOCK - 1,)),
            dma((BLOCK - 1,)),
            dma((nz - BLOCK,)),
            dma((later,)),
            dma((nx - 1,)),
            dma((nx - 1,)),
            dma((BLOCK - 1,)),
            dma((BLOCK - 1,)),
            dma((nz - BLOCK,)),
            dma((later,)),
            dma,
            dma,
        ],
        compiler_params=pltpu.CompilerParams(collective_id=0, has_side_effects=True, vmem_limit_bytes=67043328 - (5 << 20)),
    )(
        layer_input,
        in_weight,
        gate_weight,
        out_weight,
        norm_gain[None],
        rate_real,
        rate_imag,
        log_step[None],
        jnp.swapaxes(input_real, 1, 2).reshape(width, states),
        jnp.swapaxes(input_imag, 1, 2).reshape(width, states),
        output_real.reshape(width, states),
        output_imag.reshape(width, states),
        skip_weight[None],
        jnp.swapaxes(decay_offset, 1, 2),
        channel_gain[None],
    )
    return pl.pallas_call(
        finish_kernel,
        name="finish",
        out_shape=jax.ShapeDtypeStruct((sequences, own, depth), BF16),
        in_specs=[vmem()] * 5,
        out_specs=hbm(),
        scratch_shapes=[b16((sequences, own, depth)), dma((depth // 512,))],
        compiler_params=pltpu.CompilerParams(vmem_limit_bytes=16 << 20),
    )(near, square, far, channel_gain[None], far_w)


def solution(mesh):
    torus = Mesh(
        mesh.devices.reshape(mesh.shape["grp"], 16, 4, mesh.shape["tp"]),
        ("grp", "sp_0", "sp_1", "tp"),
    )
    return build(torus)


def build(torus):
    in_specs = (
        P("grp", SP_TP, None),
        P(),
        P(None, "tp"),
        P(None, "tp"),
        P("tp", None),
        P("tp", None),
        P("tp"),
        P("tp", None, None),
        P("tp", None, None),
        P("tp", None, None),
        P("tp", None, None),
        P("tp"),
        P("grp", SP, "tp"),
        P(),
        P("tp", None),
    )
    out_specs = P("grp", SP_TP, None)
    return jax.shard_map(shards, mesh=torus, in_specs=in_specs, out_specs=out_specs, check_vma=False)
```

```python
import functools
import math

import jax
import jax.numpy as jnp
from jax import lax
from jax.experimental import pallas as pl
from jax.experimental.pallas import tpu as pltpu
from jax.sharding import Mesh
from jax.sharding import PartitionSpec as P

SP = ("sp_0", "sp_1")
SP_TP = ("sp_0", "sp_1", "tp")
MESH = pl.DeviceIdType.MESH
F32 = jnp.float32
BF16 = jnp.bfloat16
EPS = 1e-06
LANES = 128
CHUNKS = 8
BLOCK = 4
UNROLL = 8


def dot(a, b):
    return jnp.dot(a, b, preferred_element_type=F32)


def dot_t(a, b):
    return lax.dot_general(a, b, (((1,), (1,)), ((), ())), preferred_element_type=F32)


def iota(shape, dim):
    return lax.broadcasted_iota(jnp.int32, shape, dim)


def one_hot(cond):
    return jnp.where(cond, 1.0, 0.0).astype(BF16)


def split(value):
    high = value.astype(BF16)
    rest = value - high.astype(F32)
    middle = rest.astype(BF16)
    low = (rest - middle.astype(F32)).astype(BF16)
    return high, middle, low


def exact_dot(value, table):
    high, middle, low = split(value)
    return dot(high, table) + dot(middle, table) + dot(low, table)


def cmul(a, b):
    return a[0] * b[0] - a[1] * b[1], a[0] * b[1] + a[1] * b[0]


def small_expm1(x):
    series = x * (1.0 + x * (1 / 2 + x * (1 / 6 + x * (1 / 24 + x * (1 / 120 + x * (1 / 720 + x / 5040))))))
    return jnp.where(x > -0.3, series, jnp.exp(x) - 1.0)


def scan_order(rows):
    steps = rows // CHUNKS
    at = iota((rows, rows), 0)
    return one_hot(iota((rows, rows), 1) == (at & (CHUNKS - 1)) * steps + (at >> 3))


def natural_order(rows):
    steps = rows // CHUNKS
    at = iota((rows, rows), 1)
    return one_hot(iota((rows, rows), 0) == (at & (CHUNKS - 1)) * steps + (at >> 3))


def small_sine(x):
    q = x * x
    return x * (1.0 + q * (-1 / 6 + q * (1 / 120 + q * (-1 / 5040 + q * (1 / 362880 - q / 39916800)))))


def small_cosine(x):
    q = x * x
    return 1.0 + q * (-1 / 2 + q * (1 / 24 + q * (-1 / 720 + q * (1 / 40320 + q * (-1 / 3628800 + q / 479001600)))))


def mixer_kernel(
    x_hbm,
    in_w_hbm,
    gate_w_hbm,
    out_w_hbm,
    norm_gain_hbm,
    rate_re_hbm,
    rate_im_hbm,
    log_step_hbm,
    table_re_hbm,
    table_im_hbm,
    read_re_hbm,
    read_im_hbm,
    skip_hbm,
    offset_hbm,
    gain_hbm,
    near_ref,
    square_ref,
    far_ref,
    far_w_ref,
    tokens,
    in_w,
    gate_w,
    norm_gain_ref,
    rate_re_ref,
    rate_im_ref,
    log_step_ref,
    table_re_ref,
    table_im_ref,
    read_re_ref,
    read_im_ref,
    skip_ref,
    offset_ref,
    gain_ref,
    out_w,
    normed,
    scales,
    raw_in,
    raw_gate,
    inputs,
    opened,
    mags,
    trans_re,
    trans_im,
    wide_re,
    wide_im,
    drive_re,
    drive_im,
    states_re,
    states_im,
    lift_re,
    lift_im,
    vec,
    ends,
    before,
    init,
    log_pack,
    log_x,
    log_row,
    log_z,
    log_block,
    log_far,
    sum_stage,
    sum_pack,
    sum_x,
    sum_row,
    sum_z,
    sum_block,
    sum_far,
    lam_pack,
    act,
    load_sem,
    x_send,
    x_recv,
    w_send,
    w_recv,
    lx_send,
    lx_recv,
    lz_send,
    lz_recv,
    lf_send,
    lf_recv,
    sx_send,
    sx_recv,
    sz_send,
    sz_recv,
    sf_send,
    sf_recv,
    a_send,
    a_recv,
):
    nz, nx = lax.axis_size("sp_0"), lax.axis_size("sp_1")
    mz, mx, tp = lax.axis_index("sp_0"), lax.axis_index("sp_1"), lax.axis_index("tp")
    sequences, own, depth = x_hbm.shape
    width = in_w_hbm.shape[1]
    rows = sequences * 2 * own
    groups, states = rate_re_hbm.shape
    channels = width // groups
    modes = groups * states
    steps = rows // CHUNKS
    quarters = CHUNKS // sequences
    tile = CHUNKS
    blocks = tile // sequences
    part = blocks * LANES
    packs = modes // part
    half = modes // 2
    hw = width // 2
    mine = pl.ds(pl.multiple_of(tp * own, own), own)
    theirs = pl.ds(pl.multiple_of((1 - tp) * own, own), own)
    partner = {"tp": 1 - tp}

    loads = [
        pltpu.make_async_copy(source, target, load_sem.at[i])
        for i, (source, target) in enumerate(
            (
                (x_hbm, tokens.at[:, mine, :]),
                (offset_hbm, offset_ref),
                (rate_re_hbm, rate_re_ref),
                (rate_im_hbm, rate_im_ref),
                (log_step_hbm, log_step_ref),
                (norm_gain_hbm, norm_gain_ref),
                (table_re_hbm, table_re_ref),
                (table_im_hbm, table_im_ref),
                (in_w_hbm, in_w),
                (gate_w_hbm, gate_w),
                (read_re_hbm, read_re_ref),
                (read_im_hbm, read_im_ref),
                (skip_hbm, skip_ref),
                (gain_hbm, gain_ref),
                (out_w_hbm, out_w),
            )
        )
    ]
    for copy in loads:
        copy.start()

    for ref in (log_z, sum_z, log_far, sum_far):
        ref[...] = jnp.zeros_like(ref)
    barrier = pltpu.get_barrier_semaphore()
    pl.semaphore_signal(barrier, inc=1, device_id=partner, device_id_type=MESH)
    for d in range(1, nx):
        pl.semaphore_signal(barrier, inc=1, device_id={"sp_1": lax.rem(mx + d, nx)}, device_id_type=MESH)
    count = nz // BLOCK
    block, place_z = mz // BLOCK, mz % BLOCK
    ends_block = place_z == BLOCK - 1

    def signal_z(z):
        pl.semaphore_signal(barrier, inc=1, device_id={"sp_0": z}, device_id_type=MESH)

    for d in range(1, BLOCK):
        pl.when(d <= place_z)(lambda d=d: signal_z(mz - d))
    for e in range(1, count):
        pl.when(e <= block)(lambda e=e: signal_z((block - e) * BLOCK + BLOCK - 1))

    def remote(source, target, send, recv, device):
        return pltpu.make_async_remote_copy(
            src_ref=source, dst_ref=target, send_sem=send, recv_sem=recv, device_id=device, device_id_type=MESH
        )

    def to_x(source, target, send, recv):
        made = []
        for d in sorted(range(1, nx), key=lambda d: -min(d, nx - d)):
            k = lax.rem(mx + d, nx)
            made.append(remote(source, target.at[mx], send.at[d - 1], recv.at[d - 1], {"sp_1": k}))
        return made

    def to_block(source, target, send, recv):
        return {
            d: remote(source, target.at[d - 1], send.at[d - 1], recv.at[d - 1], {"sp_0": lax.rem(mz + d, nz)})
            for d in range(1, BLOCK)
        }

    def to_later(source, target, send, recv):
        made = {}
        for d in sorted(range(1, nz - BLOCK + 1), key=lambda d: min(d, nz - d)):
            e = (d + BLOCK - 1) // BLOCK - 1
            made[d] = remote(source, target.at[e], send.at[d - 1], recv.at[e], {"sp_0": lax.rem(mz + d, nz)})
        return made

    def start_block(made):
        for d, copy in made.items():
            pl.when(place_z + d < BLOCK)(copy.start)

    def start_later(made):
        @pl.when(ends_block)
        def _():
            for d, copy in made.items():
                pl.when(mz + d < nz)(copy.start)

    def recv_block(made):
        for d, copy in made.items():
            pl.when(d <= place_z)(copy.wait_recv)

    def recv_later(made):
        for e in range(1, count):
            pl.when(e <= block)(made[(e - 1) * BLOCK + 1].wait_recv)

    def sent_block(made):
        for d, copy in made.items():
            pl.when(place_z + d < BLOCK)(copy.wait_send)

    def sent_later(made):
        @pl.when(ends_block)
        def _():
            for d, copy in made.items():
                pl.when(mz + d < nz)(copy.wait_send)

    for ref in (wide_re, wide_im, lift_re, lift_im):
        ref[...] = jnp.zeros_like(ref)

    for copy in loads[1:6]:
        copy.wait()
    spread_g = one_hot((iota((groups, modes), 1) >> 6) == iota((groups, modes), 0))
    spread_p = one_hot((iota((states, modes), 1) & (states - 1)) == iota((states, modes), 0))
    offsets = jnp.concatenate([offset_ref[s].T for s in range(sequences)], axis=0)
    sums = jnp.sum(offsets.reshape(CHUNKS, steps, groups), axis=1)
    step_size = jnp.broadcast_to(jnp.exp(log_step_ref[...]), (8, groups))
    spread = exact_dot(jnp.concatenate([sums, step_size], axis=0), spread_g)
    chunk_logs, step = spread[:CHUNKS], spread[CHUNKS : CHUNKS + 1]
    vec[pl.ds(16, CHUNKS), :] = chunk_logs
    for s in range(sequences):
        total = jnp.sum(chunk_logs[s * quarters : (s + 1) * quarters], axis=0, keepdims=True)
        for k in range(packs):
            for b in range(blocks):
                lo = k * part + b * LANES
                row = s * blocks + b
                log_pack[k, row : row + 1, :] = total[:, lo : lo + LANES]

    def norm(side):
        for s in range(sequences):
            for r in range(0, own, 32):
                wide = tokens[s, pl.ds(pl.multiple_of(side * own + r, 32), 32), :].astype(F32)
                at = slice(s * own + r, s * own + r + 32)
                normed[side, at, :] = (wide * norm_gain_ref[...]).astype(BF16)
                scale = lax.rsqrt(jnp.mean(wide * wide, axis=-1, keepdims=True) + EPS)
                scales[side, at, :] = jnp.broadcast_to(scale, (32, 256))

    def project(side, weight, out):
        @pl.loop(0, width // 256)
        def _(c):
            lanes = pl.ds(pl.multiple_of(c * 256, 256), 256)
            product = dot(normed[side], weight[:, lanes]) * scales[side]
            at = pl.ds(pl.multiple_of(side * own, own), own)
            out[:, at, lanes] = product.reshape(sequences, own, 256).astype(BF16)

    later = jnp.where(ends_block, nz - 1 - mz, 0)
    loads[0].wait()
    norm(tp)

    on_group = (iota((groups, modes), 1) >> 6) == iota((groups, modes), 0)
    rates = exact_dot(jnp.concatenate([rate_re_ref[...], rate_im_ref[...]], axis=0), spread_p)
    rate_re = jnp.sum(jnp.where(on_group, rates[:groups], 0.0), axis=0, keepdims=True)
    rate_im = jnp.sum(jnp.where(on_group, rates[groups:], 0.0), axis=0, keepdims=True)
    real_step, angle = rate_re * step, rate_im * step
    size = jnp.exp(real_step)
    cosine, sine = small_cosine(angle), small_sine(angle)
    lam = (size * cosine, size * sine)
    power = lam
    for _ in range(int(math.log2(steps))):
        power = cmul(power, power)
    lam_chunk = power
    for _ in range(int(math.log2(quarters))):
        power = cmul(power, power)
    for i, value in enumerate((*lam, *lam_chunk, *power, rate_re, rate_im, real_step, angle)):
        vec[i : i + 1, :] = value

    pl.semaphore_wait(barrier, nx + BLOCK - 1 - place_z + later)
    log_sends = to_x(log_pack, log_x, lx_send, lx_recv)
    for copy in log_sends:
        copy.start()
    x_copy = remote(tokens.at[:, mine, :], tokens.at[:, mine, :], x_send, x_recv, partner)
    x_copy.start()
    log_x[mx] = log_pack[...]

    order = scan_order(rows)
    pieces = [dot(order, piece) for piece in split(jnp.exp(offsets))]
    spread_3 = one_hot((iota((3 * groups, modes), 1) >> 6) == (iota((3 * groups, modes), 0) & (groups - 1)))
    mags[...] = dot(jnp.concatenate(pieces, axis=1).astype(BF16), spread_3)

    per_tile = LANES // states

    def doubled(value):
        return jnp.concatenate([value.astype(F32)] * per_tile, axis=1)

    on_lane = iota((channels, LANES), 1) // states

    def block_diagonal(target, value):
        for g in range(groups):
            at = slice(g * channels, (g + 1) * channels)
            lo = (g % (groups // 2)) // per_tile * LANES
            kept = jnp.where(on_lane == g % per_tile, value(g, at), 0.0)
            target[at, lo : lo + LANES] = kept.astype(BF16)

    for copy in loads[6:8]:
        copy.wait()
    two_re, two_im = doubled(table_re_ref[...]), doubled(table_im_ref[...])
    block_diagonal(wide_re, lambda g, at: two_re[at])
    block_diagonal(wide_im, lambda g, at: two_im[at])

    loads[8].wait()
    project(tp, in_w, raw_in)

    x_copy.wait()
    w_copies = [
        remote(out_w_hbm.at[at], far_w_ref.at[at], w_send.at[i], w_recv.at[i], partner)
        for i, at in enumerate((pl.ds(0, 3 * width // 4), pl.ds(3 * width // 4, width // 4)))
    ]
    w_copies[0].start()
    norm(1 - tp)
    project(1 - tp, in_w, raw_in)
    inputs[...] = dot(order, raw_in[...].reshape(rows, width)).astype(BF16)

    for h in range(2):
        use, lanes = slice(h * hw, (h + 1) * hw), slice(h * half, (h + 1) * half)
        drive_re[:, lanes] = dot(inputs[:, use], wide_re[use, :])
        drive_im[:, lanes] = dot(inputs[:, use], wide_im[use, :])

    span = 512

    def scan(first, keep):
        @pl.loop(0, modes // span)
        def _(c):
            lanes = pl.ds(pl.multiple_of(c * span, span), span)
            lr = jnp.broadcast_to(vec[0:1, lanes], (UNROLL * CHUNKS, span))
            li = jnp.broadcast_to(vec[1:2, lanes], (UNROLL * CHUNKS, span))
            if first is None:
                start = (jnp.zeros((CHUNKS, span), F32), jnp.zeros((CHUNKS, span), F32))
            else:
                start = (first[0, :, lanes], first[1, :, lanes])

            def body(t, now):
                re, im = now
                at = pl.ds(pl.multiple_of(t * UNROLL * CHUNKS, UNROLL * CHUNKS), UNROLL * CHUNKS)
                dr, di = drive_re[at, lanes], drive_im[at, lanes]
                if keep:
                    ar, ai = trans_re[at, lanes], trans_im[at, lanes]
                else:
                    m = mags[at, lanes]
                    ar, ai = m * lr, m * li
                    trans_re[at, lanes] = ar
                    trans_im[at, lanes] = ai
                kept = []
                for u in range(UNROLL):
                    use = slice(u * CHUNKS, (u + 1) * CHUNKS)
                    re, im = (
                        ar[use] * re - ai[use] * im + dr[use],
                        ar[use] * im + ai[use] * re + di[use],
                    )
                    kept.append((re, im))
                if keep:
                    states_re[at, lanes] = jnp.concatenate([k[0] for k in kept], axis=0).astype(BF16)
                    states_im[at, lanes] = jnp.concatenate([k[1] for k in kept], axis=0).astype(BF16)
                return re, im

            re, im = lax.fori_loop(0, steps // UNROLL, body, start)
            if not keep:
                ends[0, :, lanes] = re
                ends[1, :, lanes] = im

    scan(None, False)

    place = iota((CHUNKS, modes), 0) & (quarters - 1)
    grown = jnp.exp(vec[pl.ds(16, CHUNKS), :])
    a = (grown * vec[2:3, :], grown * vec[3:4, :])
    b = (ends[0], ends[1])
    d = 1
    while d < quarters:
        ok = place >= d
        a_old = tuple(pltpu.roll(v, d, axis=0) for v in a)
        b_old = tuple(pltpu.roll(v, d, axis=0) for v in b)
        add = cmul(a, b_old)
        new_a = cmul(a, a_old)
        b = tuple(jnp.where(ok, v + w, v) for v, w in zip(b, add))
        a = tuple(jnp.where(ok, w, v) for v, w in zip(a, new_a))
        d *= 2
    for c in range(2):
        for s in range(sequences):
            last = (s + 1) * quarters - 1
            for k in range(packs):
                for blk in range(blocks):
                    lo = k * part + blk * LANES
                    row = c * tile + s * blocks + blk
                    sum_stage[k, row : row + 1, :] = b[c][last : last + 1, lo : lo + LANES]
    sum_pack[...] = sum_stage[...].astype(BF16)
    for i, (value, empty) in enumerate(((a[0], 1.0), (a[1], 0.0), (b[0], 0.0), (b[1], 0.0))):
        before[i] = jnp.where(place == 0, empty, pltpu.roll(value, 1, axis=0))
    sum_sends = to_x(sum_pack, sum_x, sx_send, sx_recv)
    for copy in sum_sends:
        copy.start()
    sum_x[mx] = sum_pack[...]

    for copy in log_sends:
        copy.wait()
    log_row[...] = jnp.sum(log_x[...], axis=0)
    log_z_sends = to_block(log_row, log_z, lz_send, lz_recv)
    start_block(log_z_sends)
    for c in range(2):
        for k in range(packs):
            for blk in range(blocks):
                lo = k * part + blk * LANES
                for s in range(sequences):
                    row = s * blocks + blk
                    lam_pack[c, k, row : row + 1, :] = vec[4 + c : 5 + c, lo : lo + LANES]
    lam_dev = (lam_pack[0], lam_pack[1])
    zero = jnp.zeros((packs, tile, LANES), F32)
    one = (jnp.ones((packs, tile, LANES), F32), zero)
    lam_pow = [one]
    for _ in range(nx):
        lam_pow.append(cmul(lam_pow[-1], lam_dev))

    def grow(logs, base):
        size = jnp.exp(logs)
        return size * base[0], size * base[1]

    def halves(value):
        wide = value.astype(F32)
        return wide[:, :tile], wide[:, tile:]

    def plus(u, v):
        return u[0] + v[0], u[1] + v[1]

    logs = [log_x[k] for k in range(nx)]
    to_end = [None] * nx
    gone = zero
    for k in range(nx - 1, -1, -1):
        to_end[k] = grow(gone, lam_pow[nx - 1 - k])
        gone = gone + logs[k]
    row_logs = gone
    gone, power = zero, one
    for k in range(nx - 1):
        gone = jnp.where(k < mx, gone + logs[k], gone)
        power = tuple(jnp.where(k < mx, n, o) for n, o in zip(lam_pow[k + 1], power))
    to_own = grow(gone, power)

    loads[9].wait()
    project(tp, gate_w, raw_gate)
    project(1 - tp, gate_w, raw_gate)
    gates = dot(scan_order(rows), raw_gate[...].reshape(rows, width))
    opened[...] = 1.0 / (1.0 + jnp.exp(-gates))

    for copy in loads[10:14]:
        copy.wait()
    two_re, two_im = doubled(read_re_ref[...]), doubled(read_im_ref[...])

    rate_re, rate_im, real_step, angle = (vec[i : i + 1, :] for i in range(6, 10))
    half_sine = small_sine(0.5 * angle)
    top_re = small_expm1(real_step) * small_cosine(angle) - 2.0 * half_sine * half_sine
    top_im = jnp.exp(real_step) * small_sine(angle)
    inverse = 1.0 / (rate_re * rate_re + rate_im * rate_im)
    vec[10:11, :] = (top_re * rate_re + top_im * rate_im) * inverse
    vec[11:12, :] = (top_im * rate_re - top_re * rate_im) * inverse

    def coef(g):
        lo = g // per_tile * LANES
        return vec[10:11, lo : lo + LANES], vec[11:12, lo : lo + LANES]

    def lifted_re(g, at):
        kr, ki = coef(g)
        return two_re[at] * kr - two_im[at] * ki

    def lifted_im(g, at):
        kr, ki = coef(g)
        return -(two_re[at] * ki + two_im[at] * kr)

    block_diagonal(lift_re, lifted_re)
    block_diagonal(lift_im, lifted_im)

    recv_block(log_z_sends)
    gone, power, weights = zero, one, {}
    for d in range(1, BLOCK):
        weights[d] = grow(gone, power)
        gone = gone + log_z[d - 1]
        power = tuple(jnp.where(d <= place_z, n, o) for n, o in zip(cmul(power, lam_pow[nx]), power))
    through = grow(gone, power)
    log_block[...] = gone + row_logs
    log_far_sends = to_later(log_block, log_far, lf_send, lf_recv)
    start_later(log_far_sends)
    lam_block = one
    for _ in range(BLOCK):
        lam_block = cmul(lam_block, lam_pow[nx])

    for copy in sum_sends:
        copy.wait()
    came = [halves(sum_x[k]) for k in range(nx)]
    total = cmul(to_end[0], came[0])
    for k in range(1, nx):
        total = plus(total, cmul(to_end[k], came[k]))
    sum_row[...] = jnp.concatenate(total, axis=1).astype(BF16)
    sum_z_sends = to_block(sum_row, sum_z, sz_send, sz_recv)
    start_block(sum_z_sends)

    inside = (zero, zero)
    for k in range(nx - 1):
        new = plus(cmul(inside, grow(logs[k], lam_dev)), came[k])
        inside = tuple(jnp.where(k < mx, n, o) for n, o in zip(new, inside))
    recv_block(sum_z_sends)
    carry = (zero, zero)
    for d in range(1, BLOCK):
        carry = plus(carry, cmul(weights[d], halves(sum_z[d - 1])))
    filled = plus(cmul(carry, grow(row_logs, lam_pow[nx])), total)
    sum_block[...] = jnp.concatenate(filled, axis=1).astype(BF16)
    sum_far_sends = to_later(sum_block, sum_far, sf_send, sf_recv)
    start_later(sum_far_sends)

    recv_later(log_far_sends)
    gone, power = zero, one
    for e in range(1, count):
        weights[e] = cmul(through, grow(gone, power))
        gone = gone + log_far[e - 1]
        power = cmul(power, lam_block)
    recv_later(sum_far_sends)
    for e in range(1, count):
        carry = plus(carry, cmul(weights[e], halves(sum_far[e - 1])))
    carry = plus(cmul(carry, to_own), inside)
    upper = iota((CHUNKS, LANES), 0) < quarters
    for k in range(packs):
        for blk in range(blocks):
            lo = k * part + blk * LANES
            lanes = slice(lo, lo + LANES)
            into = tuple(
                jnp.where(upper, v[k, blk : blk + 1, :], v[k, blocks + blk : blocks + blk + 1, :]) for v in carry
            )
            moved = cmul((before[0, :, lanes], before[1, :, lanes]), into)
            init[0, :, lanes] = before[2, :, lanes] + moved[0]
            init[1, :, lanes] = before[3, :, lanes] + moved[1]

    w_copies[1].start()
    scan(init, True)

    parts = []
    for h in range(2):
        use = slice(h * hw, (h + 1) * hw)
        lanes = slice(h * half, (h + 1) * half)
        mixed = dot_t(states_re[:, lanes], lift_re[use, :]) + dot_t(states_im[:, lanes], lift_im[use, :])
        mixed = mixed + skip_ref[:, use] * inputs[:, use].astype(F32)
        gelu = 0.5 * mixed * (1.0 + lax.erf(mixed * math.sqrt(0.5)))
        parts.append((gelu * opened[:, use]).astype(BF16))
    back = natural_order(rows)
    for h in range(2):
        act[:, :, h * hw : (h + 1) * hw] = dot(back, parts[h]).astype(BF16).reshape(sequences, 2 * own, hw)
    a_copy = remote(act.at[:, theirs, :], far_ref, a_send, a_recv, partner)
    a_copy.start()
    near = act[:, mine, :].astype(F32).reshape(sequences * own, width)
    square_ref[...] = jnp.broadcast_to(jnp.sum(near * near, axis=-1, keepdims=True), square_ref.shape)
    near = (near * gain_ref[:, pl.ds(pl.multiple_of(tp * width, width), width)]).astype(BF16)
    loads[14].wait()
    for c in range(depth // 512):
        lanes = slice(c * 512, (c + 1) * 512)
        near_ref[:, lanes] = dot(near, out_w[:, lanes])
    for copy in w_copies:
        copy.wait()
    a_copy.wait()

    sent_block(log_z_sends)
    sent_block(sum_z_sends)
    sent_later(log_far_sends)
    sent_later(sum_far_sends)


def finish_kernel(near_ref, square_ref, far_ref, gain_ref, far_w_ref, out_hbm, staged, sem):
    tp = lax.axis_index("tp")
    sequences, own, width = far_ref.shape
    depth = far_w_ref.shape[1]

    far = far_ref[...].astype(F32).reshape(sequences * own, width)
    square = square_ref[:, :1] + jnp.sum(far * far, axis=-1, keepdims=True)
    scale = lax.rsqrt(square * (0.5 / width) + EPS)
    far = (far * gain_ref[:, pl.ds(pl.multiple_of((1 - tp) * width, width), width)]).astype(BF16)
    copies = []
    for c in range(depth // 512):
        lanes = slice(c * 512, (c + 1) * 512)
        result = (near_ref[:, lanes] + dot(far, far_w_ref[:, lanes])) * scale
        staged[:, :, lanes] = result.astype(BF16).reshape(sequences, own, 512)
        copies.append(pltpu.make_async_copy(staged.at[:, :, lanes], out_hbm.at[:, :, lanes], sem.at[c]))
        copies[-1].start()
    for copy in copies:
        copy.wait()


def vmem():
    return pl.BlockSpec(memory_space=pltpu.VMEM)


def hbm():
    return pl.BlockSpec(memory_space=pl.ANY)


def shards(
    layer_input,
    norm_gain,
    in_weight,
    gate_weight,
    rate_real,
    rate_imag,
    log_step,
    input_real,
    input_imag,
    output_real,
    output_imag,
    skip_weight,
    decay_offset,
    channel_gain,
    out_weight,
):
    nz, nx = lax.axis_size("sp_0"), lax.axis_size("sp_1")
    sequences, own, depth = layer_input.shape
    width = in_weight.shape[1]
    groups, states = rate_real.shape
    modes = groups * states
    rows = sequences * 2 * own
    dma = pltpu.SemaphoreType.DMA
    later = nz // BLOCK - 1
    tile = CHUNKS
    packs = modes // (tile // sequences * LANES)
    f32 = functools.partial(pltpu.VMEM, dtype=F32)
    b16 = functools.partial(pltpu.VMEM, dtype=BF16)
    near, square, far, far_w = pl.pallas_call(
        mixer_kernel,
        name="mixer",
        out_shape=[
            pltpu.VMEM((sequences * own, depth), F32),
            pltpu.VMEM((sequences * own, LANES), F32),
            pltpu.VMEM((sequences, own, width), BF16),
            pltpu.VMEM((width, depth), BF16),
        ],
        in_specs=[pl.BlockSpec(memory_space=pltpu.HBM)] * 15,
        out_specs=[vmem()] * 4,
        scratch_shapes=[
            b16((sequences, 2 * own, depth)),
            b16((depth, width)),
            b16((depth, width)),
            f32((1, depth)),
            f32((groups, states)),
            f32((groups, states)),
            f32((1, groups)),
            b16((width, states)),
            b16((width, states)),
            b16((width, states)),
            b16((width, states)),
            f32((1, width)),
            f32((sequences, groups, 2 * own)),
            f32((1, 2 * width)),
            b16((width, depth)),
            b16((2, sequences * own, depth)),
            f32((2, sequences * own, 256)),
            b16((sequences, 2 * own, width)),
            b16((sequences, 2 * own, width)),
            b16((rows, width)),
            f32((rows, width)),
            f32((rows, modes)),
            f32((rows, modes)),
            f32((rows, modes)),
            b16((width, modes // 2)),
            b16((width, modes // 2)),
            f32((rows, modes)),
            f32((rows, modes)),
            b16((rows, modes)),
            b16((rows, modes)),
            b16((width, modes // 2)),
            b16((width, modes // 2)),
            f32((24, modes)),
            f32((2, CHUNKS, modes)),
            f32((4, CHUNKS, modes)),
            f32((2, CHUNKS, modes)),
            f32((packs, tile, LANES)),
            f32((nx, packs, tile, LANES)),
            f32((packs, tile, LANES)),
            f32((BLOCK - 1, packs, tile, LANES)),
            f32((packs, tile, LANES)),
            f32((later, packs, tile, LANES)),
            f32((packs, 2 * tile, LANES)),
            b16((packs, 2 * tile, LANES)),
            b16((nx, packs, 2 * tile, LANES)),
            b16((packs, 2 * tile, LANES)),
            b16((BLOCK - 1, packs, 2 * tile, LANES)),
            b16((packs, 2 * tile, LANES)),
            b16((later, packs, 2 * tile, LANES)),
            f32((2, packs, tile, LANES)),
            b16((sequences, 2 * own, width)),
            dma((15,)),
            dma,
            dma,
            dma((2,)),
            dma((2,)),
            dma((nx - 1,)),
            dma((nx - 1,)),
            dma((BLOCK - 1,)),
            dma((BLOCK - 1,)),
            dma((nz - BLOCK,)),
            dma((later,)),
            dma((nx - 1,)),
            dma((nx - 1,)),
            dma((BLOCK - 1,)),
            dma((BLOCK - 1,)),
            dma((nz - BLOCK,)),
            dma((later,)),
            dma,
            dma,
        ],
        compiler_params=pltpu.CompilerParams(collective_id=0, has_side_effects=True, vmem_limit_bytes=67043328 - (5 << 20)),
    )(
        layer_input,
        in_weight,
        gate_weight,
        out_weight,
        norm_gain[None],
        rate_real,
        rate_imag,
        log_step[None],
        jnp.swapaxes(input_real, 1, 2).reshape(width, states),
        jnp.swapaxes(input_imag, 1, 2).reshape(width, states),
        output_real.reshape(width, states),
        output_imag.reshape(width, states),
        skip_weight[None],
        jnp.swapaxes(decay_offset, 1, 2),
        channel_gain[None],
    )
    return pl.pallas_call(
        finish_kernel,
        name="finish",
        out_shape=jax.ShapeDtypeStruct((sequences, own, depth), BF16),
        in_specs=[vmem()] * 5,
        out_specs=hbm(),
        scratch_shapes=[b16((sequences, own, depth)), dma((depth // 512,))],
        compiler_params=pltpu.CompilerParams(vmem_limit_bytes=16 << 20),
    )(near, square, far, channel_gain[None], far_w)


def solution(mesh):
    torus = Mesh(
        mesh.devices.reshape(mesh.shape["grp"], 16, 4, mesh.shape["tp"]),
        ("grp", "sp_0", "sp_1", "tp"),
    )
    return build(torus)


def build(torus):
    in_specs = (
        P("grp", SP_TP, None),
        P(),
        P(None, "tp"),
        P(None, "tp"),
        P("tp", None),
        P("tp", None),
        P("tp"),
        P("tp", None, None),
        P("tp", None, None),
        P("tp", None, None),
        P("tp", None, None),
        P("tp"),
        P("grp", SP, "tp"),
        P(),
        P("tp", None),
    )
    out_specs = P("grp", SP_TP, None)
    return jax.shard_map(shards, mesh=torus, in_specs=in_specs, out_specs=out_specs, check_vma=False)
```

```python
import functools
import math

import jax
import jax.numpy as jnp
from jax import lax
from jax.experimental import pallas as pl
from jax.experimental.pallas import tpu as pltpu
from jax.sharding import Mesh
from jax.sharding import PartitionSpec as P

SP = ("sp_0", "sp_1")
SP_TP = ("sp_0", "sp_1", "tp")
MESH = pl.DeviceIdType.MESH
F32 = jnp.float32
BF16 = jnp.bfloat16
EPS = 1e-06
LANES = 128
CHUNKS = 8
BLOCK = 4
UNROLL = 8


def dot(a, b):
    return jnp.dot(a, b, preferred_element_type=F32)


def dot_t(a, b):
    return lax.dot_general(a, b, (((1,), (1,)), ((), ())), preferred_element_type=F32)


def iota(shape, dim):
    return lax.broadcasted_iota(jnp.int32, shape, dim)


def one_hot(cond):
    return jnp.where(cond, 1.0, 0.0).astype(BF16)


def split(value):
    high = value.astype(BF16)
    rest = value - high.astype(F32)
    middle = rest.astype(BF16)
    low = (rest - middle.astype(F32)).astype(BF16)
    return high, middle, low


def exact_dot(value, table):
    high, middle, low = split(value)
    return dot(high, table) + dot(middle, table) + dot(low, table)


def cmul(a, b):
    return a[0] * b[0] - a[1] * b[1], a[0] * b[1] + a[1] * b[0]


def small_expm1(x):
    series = x * (1.0 + x * (1 / 2 + x * (1 / 6 + x * (1 / 24 + x * (1 / 120 + x * (1 / 720 + x / 5040))))))
    return jnp.where(x > -0.3, series, jnp.exp(x) - 1.0)


def scan_order(rows):
    steps = rows // CHUNKS
    at = iota((rows, rows), 0)
    return one_hot(iota((rows, rows), 1) == (at & (CHUNKS - 1)) * steps + (at >> 3))


def natural_order(rows):
    steps = rows // CHUNKS
    at = iota((rows, rows), 1)
    return one_hot(iota((rows, rows), 0) == (at & (CHUNKS - 1)) * steps + (at >> 3))


def small_sine(x):
    q = x * x
    return x * (1.0 + q * (-1 / 6 + q * (1 / 120 + q * (-1 / 5040 + q * (1 / 362880 - q / 39916800)))))


def small_cosine(x):
    q = x * x
    return 1.0 + q * (-1 / 2 + q * (1 / 24 + q * (-1 / 720 + q * (1 / 40320 + q * (-1 / 3628800 + q / 479001600)))))


def mixer_kernel(
    x_hbm,
    in_w_hbm,
    gate_w_hbm,
    out_w_hbm,
    norm_gain_hbm,
    rate_re_hbm,
    rate_im_hbm,
    log_step_hbm,
    table_re_hbm,
    table_im_hbm,
    read_re_hbm,
    read_im_hbm,
    skip_hbm,
    offset_hbm,
    gain_hbm,
    near_ref,
    square_ref,
    far_ref,
    far_w_ref,
    tokens,
    in_w,
    gate_w,
    norm_gain_ref,
    rate_re_ref,
    rate_im_ref,
    log_step_ref,
    table_re_ref,
    table_im_ref,
    read_re_ref,
    read_im_ref,
    skip_ref,
    offset_ref,
    gain_ref,
    out_w,
    normed,
    scales,
    raw_in,
    raw_gate,
    inputs,
    opened,
    mags,
    trans_re,
    trans_im,
    wide_re,
    wide_im,
    drive_re,
    drive_im,
    states_re,
    states_im,
    lift_re,
    lift_im,
    vec,
    ends,
    before,
    init,
    log_pack,
    log_x,
    log_row,
    log_z,
    log_block,
    log_far,
    sum_stage,
    sum_pack,
    sum_x,
    sum_row,
    sum_z,
    sum_block,
    sum_far,
    lam_pack,
    act,
    load_sem,
    x_send,
    x_recv,
    w_send,
    w_recv,
    lx_send,
    lx_recv,
    lz_send,
    lz_recv,
    lf_send,
    lf_recv,
    sx_send,
    sx_recv,
    sz_send,
    sz_recv,
    sf_send,
    sf_recv,
    a_send,
    a_recv,
):
    nz, nx = lax.axis_size("sp_0"), lax.axis_size("sp_1")
    mz, mx, tp = lax.axis_index("sp_0"), lax.axis_index("sp_1"), lax.axis_index("tp")
    sequences, own, depth = x_hbm.shape
    width = in_w_hbm.shape[1]
    rows = sequences * 2 * own
    groups, states = rate_re_hbm.shape
    channels = width // groups
    modes = groups * states
    steps = rows // CHUNKS
    quarters = CHUNKS // sequences
    tile = CHUNKS
    blocks = tile // sequences
    part = blocks * LANES
    packs = modes // part
    half = modes // 2
    hw = width // 2
    mine = pl.ds(pl.multiple_of(tp * own, own), own)
    theirs = pl.ds(pl.multiple_of((1 - tp) * own, own), own)
    partner = {"tp": 1 - tp}

    loads = [
        pltpu.make_async_copy(source, target, load_sem.at[i])
        for i, (source, target) in enumerate(
            (
                (x_hbm, tokens.at[:, mine, :]),
                (offset_hbm, offset_ref),
                (rate_re_hbm, rate_re_ref),
                (rate_im_hbm, rate_im_ref),
                (log_step_hbm, log_step_ref),
                (norm_gain_hbm, norm_gain_ref),
                (table_re_hbm, table_re_ref),
                (table_im_hbm, table_im_ref),
                (in_w_hbm, in_w),
                (gate_w_hbm, gate_w),
                (read_re_hbm, read_re_ref),
                (read_im_hbm, read_im_ref),
                (skip_hbm, skip_ref),
                (gain_hbm, gain_ref),
                (out_w_hbm, out_w),
            )
        )
    ]
    for copy in loads:
        copy.start()

    for ref in (log_z, sum_z, log_far, sum_far):
        ref[...] = jnp.zeros_like(ref)
    barrier = pltpu.get_barrier_semaphore()
    pl.semaphore_signal(barrier, inc=1, device_id=partner, device_id_type=MESH)
    for d in range(1, nx):
        pl.semaphore_signal(barrier, inc=1, device_id={"sp_1": lax.rem(mx + d, nx)}, device_id_type=MESH)
    count = nz // BLOCK
    block, place_z = mz // BLOCK, mz % BLOCK
    ends_block = place_z == BLOCK - 1

    def signal_z(z):
        pl.semaphore_signal(barrier, inc=1, device_id={"sp_0": z}, device_id_type=MESH)

    for d in range(1, BLOCK):
        pl.when(d <= place_z)(lambda d=d: signal_z(mz - d))
    for e in range(1, count):
        pl.when(e <= block)(lambda e=e: signal_z((block - e) * BLOCK + BLOCK - 1))

    def remote(source, target, send, recv, device):
        return pltpu.make_async_remote_copy(
            src_ref=source, dst_ref=target, send_sem=send, recv_sem=recv, device_id=device, device_id_type=MESH
        )

    def to_x(source, target, send, recv):
        made = []
        for d in sorted(range(1, nx), key=lambda d: -min(d, nx - d)):
            k = lax.rem(mx + d, nx)
            made.append(remote(source, target.at[mx], send.at[d - 1], recv.at[d - 1], {"sp_1": k}))
        return made

    def to_block(source, target, send, recv):
        return {
            d: remote(source, target.at[d - 1], send.at[d - 1], recv.at[d - 1], {"sp_0": lax.rem(mz + d, nz)})
            for d in range(1, BLOCK)
        }

    def to_later(source, target, send, recv):
        made = {}
        for d in sorted(range(1, nz - BLOCK + 1), key=lambda d: min(d, nz - d)):
            e = (d + BLOCK - 1) // BLOCK - 1
            made[d] = remote(source, target.at[e], send.at[d - 1], recv.at[e], {"sp_0": lax.rem(mz + d, nz)})
        return made

    def start_block(made):
        for d, copy in made.items():
            pl.when(place_z + d < BLOCK)(copy.start)

    def start_later(made):
        @pl.when(ends_block)
        def _():
            for d, copy in made.items():
                pl.when(mz + d < nz)(copy.start)

    def recv_block(made):
        for d, copy in made.items():
            pl.when(d <= place_z)(copy.wait_recv)

    def recv_later(made):
        for e in range(1, count):
            pl.when(e <= block)(made[(e - 1) * BLOCK + 1].wait_recv)

    def sent_block(made):
        for d, copy in made.items():
            pl.when(place_z + d < BLOCK)(copy.wait_send)

    def sent_later(made):
        @pl.when(ends_block)
        def _():
            for d, copy in made.items():
                pl.when(mz + d < nz)(copy.wait_send)

    for ref in (wide_re, wide_im, lift_re, lift_im):
        ref[...] = jnp.zeros_like(ref)

    for copy in loads[1:6]:
        copy.wait()
    spread_g = one_hot((iota((groups, modes), 1) >> 6) == iota((groups, modes), 0))
    spread_p = one_hot((iota((states, modes), 1) & (states - 1)) == iota((states, modes), 0))
    offsets = jnp.concatenate([offset_ref[s].T for s in range(sequences)], axis=0)
    sums = jnp.sum(offsets.reshape(CHUNKS, steps, groups), axis=1)
    step_size = jnp.broadcast_to(jnp.exp(log_step_ref[...]), (8, groups))
    spread = exact_dot(jnp.concatenate([sums, step_size], axis=0), spread_g)
    chunk_logs, step = spread[:CHUNKS], spread[CHUNKS : CHUNKS + 1]
    vec[pl.ds(16, CHUNKS), :] = chunk_logs
    for s in range(sequences):
        total = jnp.sum(chunk_logs[s * quarters : (s + 1) * quarters], axis=0, keepdims=True)
        for k in range(packs):
            for b in range(blocks):
                lo = k * part + b * LANES
                row = s * blocks + b
                log_pack[k, row : row + 1, :] = total[:, lo : lo + LANES]

    def norm(side):
        for s in range(sequences):
            for r in range(0, own, 32):
                wide = tokens[s, pl.ds(pl.multiple_of(side * own + r, 32), 32), :].astype(F32)
                at = slice(s * own + r, s * own + r + 32)
                normed[side, at, :] = (wide * norm_gain_ref[...]).astype(BF16)
                scale = lax.rsqrt(jnp.mean(wide * wide, axis=-1, keepdims=True) + EPS)
                scales[side, at, :] = jnp.broadcast_to(scale, (32, 256))

    def project(side, weight, out):
        @pl.loop(0, width // 256)
        def _(c):
            lanes = pl.ds(pl.multiple_of(c * 256, 256), 256)
            product = dot(normed[side], weight[:, lanes]) * scales[side]
            at = pl.ds(pl.multiple_of(side * own, own), own)
            out[:, at, lanes] = product.reshape(sequences, own, 256).astype(BF16)

    later = jnp.where(ends_block, nz - 1 - mz, 0)
    loads[0].wait()
    norm(tp)

    pl.semaphore_wait(barrier, nx + BLOCK - 1 - place_z + later)
    log_sends = to_x(log_pack, log_x, lx_send, lx_recv)
    for copy in log_sends:
        copy.start()
    x_copy = remote(tokens.at[:, mine, :], tokens.at[:, mine, :], x_send, x_recv, partner)
    x_copy.start()
    log_x[mx] = log_pack[...]

    on_group = (iota((groups, modes), 1) >> 6) == iota((groups, modes), 0)
    rates = exact_dot(jnp.concatenate([rate_re_ref[...], rate_im_ref[...]], axis=0), spread_p)
    rate_re = jnp.sum(jnp.where(on_group, rates[:groups], 0.0), axis=0, keepdims=True)
    rate_im = jnp.sum(jnp.where(on_group, rates[groups:], 0.0), axis=0, keepdims=True)
    real_step, angle = rate_re * step, rate_im * step
    size = jnp.exp(real_step)
    cosine, sine = small_cosine(angle), small_sine(angle)
    lam = (size * cosine, size * sine)
    power = lam
    for _ in range(int(math.log2(steps))):
        power = cmul(power, power)
    lam_chunk = power
    for _ in range(int(math.log2(quarters))):
        power = cmul(power, power)
    for i, value in enumerate((*lam, *lam_chunk, *power, rate_re, rate_im, real_step, angle)):
        vec[i : i + 1, :] = value

    order = scan_order(rows)
    pieces = [dot(order, piece) for piece in split(jnp.exp(offsets))]
    spread_3 = one_hot((iota((3 * groups, modes), 1) >> 6) == (iota((3 * groups, modes), 0) & (groups - 1)))
    mags[...] = dot(jnp.concatenate(pieces, axis=1).astype(BF16), spread_3)

    per_tile = LANES // states

    def doubled(value):
        return jnp.concatenate([value.astype(F32)] * per_tile, axis=1)

    on_lane = iota((channels, LANES), 1) // states

    def block_diagonal(target, value):
        for g in range(groups):
            at = slice(g * channels, (g + 1) * channels)
            lo = (g % (groups // 2)) // per_tile * LANES
            kept = jnp.where(on_lane == g % per_tile, value(g, at), 0.0)
            target[at, lo : lo + LANES] = kept.astype(BF16)

    for copy in loads[6:8]:
        copy.wait()
    two_re, two_im = doubled(table_re_ref[...]), doubled(table_im_ref[...])
    block_diagonal(wide_re, lambda g, at: two_re[at])
    block_diagonal(wide_im, lambda g, at: two_im[at])

    loads[8].wait()
    project(tp, in_w, raw_in)

    x_copy.wait()
    w_copies = [
        remote(out_w_hbm.at[at], far_w_ref.at[at], w_send.at[i], w_recv.at[i], partner)
        for i, at in enumerate((pl.ds(0, 3 * width // 4), pl.ds(3 * width // 4, width // 4)))
    ]
    w_copies[0].start()
    norm(1 - tp)
    project(1 - tp, in_w, raw_in)
    inputs[...] = dot(order, raw_in[...].reshape(rows, width)).astype(BF16)

    for h in range(2):
        use, lanes = slice(h * hw, (h + 1) * hw), slice(h * half, (h + 1) * half)
        drive_re[:, lanes] = dot(inputs[:, use], wide_re[use, :])
        drive_im[:, lanes] = dot(inputs[:, use], wide_im[use, :])

    span = 512

    def scan(first, keep):
        @pl.loop(0, modes // span)
        def _(c):
            lanes = pl.ds(pl.multiple_of(c * span, span), span)
            lr = jnp.broadcast_to(vec[0:1, lanes], (UNROLL * CHUNKS, span))
            li = jnp.broadcast_to(vec[1:2, lanes], (UNROLL * CHUNKS, span))
            if first is None:
                start = (jnp.zeros((CHUNKS, span), F32), jnp.zeros((CHUNKS, span), F32))
            else:
                start = (first[0, :, lanes], first[1, :, lanes])

            def body(t, now):
                re, im = now
                at = pl.ds(pl.multiple_of(t * UNROLL * CHUNKS, UNROLL * CHUNKS), UNROLL * CHUNKS)
                dr, di = drive_re[at, lanes], drive_im[at, lanes]
                if keep:
                    ar, ai = trans_re[at, lanes], trans_im[at, lanes]
                else:
                    m = mags[at, lanes]
                    ar, ai = m * lr, m * li
                    trans_re[at, lanes] = ar
                    trans_im[at, lanes] = ai
                kept = []
                for u in range(UNROLL):
                    use = slice(u * CHUNKS, (u + 1) * CHUNKS)
                    re, im = (
                        ar[use] * re - ai[use] * im + dr[use],
                        ar[use] * im + ai[use] * re + di[use],
                    )
                    kept.append((re, im))
                if keep:
                    states_re[at, lanes] = jnp.concatenate([k[0] for k in kept], axis=0).astype(BF16)
                    states_im[at, lanes] = jnp.concatenate([k[1] for k in kept], axis=0).astype(BF16)
                return re, im

            re, im = lax.fori_loop(0, steps // UNROLL, body, start)
            if not keep:
                ends[0, :, lanes] = re
                ends[1, :, lanes] = im

    scan(None, False)

    place = iota((CHUNKS, modes), 0) & (quarters - 1)
    grown = jnp.exp(vec[pl.ds(16, CHUNKS), :])
    a = (grown * vec[2:3, :], grown * vec[3:4, :])
    b = (ends[0], ends[1])
    d = 1
    while d < quarters:
        ok = place >= d
        a_old = tuple(pltpu.roll(v, d, axis=0) for v in a)
        b_old = tuple(pltpu.roll(v, d, axis=0) for v in b)
        add = cmul(a, b_old)
        new_a = cmul(a, a_old)
        b = tuple(jnp.where(ok, v + w, v) for v, w in zip(b, add))
        a = tuple(jnp.where(ok, w, v) for v, w in zip(a, new_a))
        d *= 2
    for c in range(2):
        for s in range(sequences):
            last = (s + 1) * quarters - 1
            for k in range(packs):
                for blk in range(blocks):
                    lo = k * part + blk * LANES
                    row = c * tile + s * blocks + blk
                    sum_stage[k, row : row + 1, :] = b[c][last : last + 1, lo : lo + LANES]
    sum_pack[...] = sum_stage[...].astype(BF16)
    for i, (value, empty) in enumerate(((a[0], 1.0), (a[1], 0.0), (b[0], 0.0), (b[1], 0.0))):
        before[i] = jnp.where(place == 0, empty, pltpu.roll(value, 1, axis=0))
    sum_sends = to_x(sum_pack, sum_x, sx_send, sx_recv)
    for copy in sum_sends:
        copy.start()
    sum_x[mx] = sum_pack[...]

    for copy in log_sends:
        copy.wait()
    log_row[...] = jnp.sum(log_x[...], axis=0)
    log_z_sends = to_block(log_row, log_z, lz_send, lz_recv)
    start_block(log_z_sends)
    for c in range(2):
        for k in range(packs):
            for blk in range(blocks):
                lo = k * part + blk * LANES
                for s in range(sequences):
                    row = s * blocks + blk
                    lam_pack[c, k, row : row + 1, :] = vec[4 + c : 5 + c, lo : lo + LANES]
    lam_dev = (lam_pack[0], lam_pack[1])
    zero = jnp.zeros((packs, tile, LANES), F32)
    one = (jnp.ones((packs, tile, LANES), F32), zero)
    lam_pow = [one]
    for _ in range(nx):
        lam_pow.append(cmul(lam_pow[-1], lam_dev))

    def grow(logs, base):
        size = jnp.exp(logs)
        return size * base[0], size * base[1]

    def halves(value):
        wide = value.astype(F32)
        return wide[:, :tile], wide[:, tile:]

    def plus(u, v):
        return u[0] + v[0], u[1] + v[1]

    logs = [log_x[k] for k in range(nx)]
    to_end = [None] * nx
    gone = zero
    for k in range(nx - 1, -1, -1):
        to_end[k] = grow(gone, lam_pow[nx - 1 - k])
        gone = gone + logs[k]
    row_logs = gone
    gone, power = zero, one
    for k in range(nx - 1):
        gone = jnp.where(k < mx, gone + logs[k], gone)
        power = tuple(jnp.where(k < mx, n, o) for n, o in zip(lam_pow[k + 1], power))
    to_own = grow(gone, power)

    loads[9].wait()
    project(tp, gate_w, raw_gate)
    project(1 - tp, gate_w, raw_gate)
    gates = dot(scan_order(rows), raw_gate[...].reshape(rows, width))
    opened[...] = 1.0 / (1.0 + jnp.exp(-gates))

    for copy in loads[10:14]:
        copy.wait()
    two_re, two_im = doubled(read_re_ref[...]), doubled(read_im_ref[...])

    rate_re, rate_im, real_step, angle = (vec[i : i + 1, :] for i in range(6, 10))
    half_sine = small_sine(0.5 * angle)
    top_re = small_expm1(real_step) * small_cosine(angle) - 2.0 * half_sine * half_sine
    top_im = jnp.exp(real_step) * small_sine(angle)
    inverse = 1.0 / (rate_re * rate_re + rate_im * rate_im)
    vec[10:11, :] = (top_re * rate_re + top_im * rate_im) * inverse
    vec[11:12, :] = (top_im * rate_re - top_re * rate_im) * inverse

    def coef(g):
        lo = g // per_tile * LANES
        return vec[10:11, lo : lo + LANES], vec[11:12, lo : lo + LANES]

    def lifted_re(g, at):
        kr, ki = coef(g)
        return two_re[at] * kr - two_im[at] * ki

    def lifted_im(g, at):
        kr, ki = coef(g)
        return -(two_re[at] * ki + two_im[at] * kr)

    block_diagonal(lift_re, lifted_re)
    block_diagonal(lift_im, lifted_im)

    recv_block(log_z_sends)
    gone, power, weights = zero, one, {}
    for d in range(1, BLOCK):
        weights[d] = grow(gone, power)
        gone = gone + log_z[d - 1]
        power = tuple(jnp.where(d <= place_z, n, o) for n, o in zip(cmul(power, lam_pow[nx]), power))
    through = grow(gone, power)
    log_block[...] = gone + row_logs
    log_far_sends = to_later(log_block, log_far, lf_send, lf_recv)
    start_later(log_far_sends)
    lam_block = one
    for _ in range(BLOCK):
        lam_block = cmul(lam_block, lam_pow[nx])

    for copy in sum_sends:
        copy.wait()
    came = [halves(sum_x[k]) for k in range(nx)]
    total = cmul(to_end[0], came[0])
    for k in range(1, nx):
        total = plus(total, cmul(to_end[k], came[k]))
    sum_row[...] = jnp.concatenate(total, axis=1).astype(BF16)
    sum_z_sends = to_block(sum_row, sum_z, sz_send, sz_recv)
    start_block(sum_z_sends)

    inside = (zero, zero)
    for k in range(nx - 1):
        new = plus(cmul(inside, grow(logs[k], lam_dev)), came[k])
        inside = tuple(jnp.where(k < mx, n, o) for n, o in zip(new, inside))
    recv_block(sum_z_sends)
    carry = (zero, zero)
    for d in range(1, BLOCK):
        carry = plus(carry, cmul(weights[d], halves(sum_z[d - 1])))
    filled = plus(cmul(carry, grow(row_logs, lam_pow[nx])), total)
    sum_block[...] = jnp.concatenate(filled, axis=1).astype(BF16)
    sum_far_sends = to_later(sum_block, sum_far, sf_send, sf_recv)
    start_later(sum_far_sends)

    recv_later(log_far_sends)
    gone, power = zero, one
    for e in range(1, count):
        weights[e] = cmul(through, grow(gone, power))
        gone = gone + log_far[e - 1]
        power = cmul(power, lam_block)
    recv_later(sum_far_sends)
    for e in range(1, count):
        carry = plus(carry, cmul(weights[e], halves(sum_far[e - 1])))
    carry = plus(cmul(carry, to_own), inside)
    upper = iota((CHUNKS, LANES), 0) < quarters
    for k in range(packs):
        for blk in range(blocks):
            lo = k * part + blk * LANES
            lanes = slice(lo, lo + LANES)
            into = tuple(
                jnp.where(upper, v[k, blk : blk + 1, :], v[k, blocks + blk : blocks + blk + 1, :]) for v in carry
            )
            moved = cmul((before[0, :, lanes], before[1, :, lanes]), into)
            init[0, :, lanes] = before[2, :, lanes] + moved[0]
            init[1, :, lanes] = before[3, :, lanes] + moved[1]

    w_copies[1].start()
    scan(init, True)

    parts = []
    for h in range(2):
        use = slice(h * hw, (h + 1) * hw)
        lanes = slice(h * half, (h + 1) * half)
        mixed = dot_t(states_re[:, lanes], lift_re[use, :]) + dot_t(states_im[:, lanes], lift_im[use, :])
        mixed = mixed + skip_ref[:, use] * inputs[:, use].astype(F32)
        gelu = 0.5 * mixed * (1.0 + lax.erf(mixed * math.sqrt(0.5)))
        parts.append((gelu * opened[:, use]).astype(BF16))
    back = natural_order(rows)
    for h in range(2):
        act[:, :, h * hw : (h + 1) * hw] = dot(back, parts[h]).astype(BF16).reshape(sequences, 2 * own, hw)
    a_copy = remote(act.at[:, theirs, :], far_ref, a_send, a_recv, partner)
    a_copy.start()
    near = act[:, mine, :].astype(F32).reshape(sequences * own, width)
    square_ref[...] = jnp.broadcast_to(jnp.sum(near * near, axis=-1, keepdims=True), square_ref.shape)
    near = (near * gain_ref[:, pl.ds(pl.multiple_of(tp * width, width), width)]).astype(BF16)
    loads[14].wait()
    for c in range(depth // 512):
        lanes = slice(c * 512, (c + 1) * 512)
        near_ref[:, lanes] = dot(near, out_w[:, lanes])
    for copy in w_copies:
        copy.wait()
    a_copy.wait()

    sent_block(log_z_sends)
    sent_block(sum_z_sends)
    sent_later(log_far_sends)
    sent_later(sum_far_sends)


def finish_kernel(near_ref, square_ref, far_ref, gain_ref, far_w_ref, out_hbm, staged, sem):
    tp = lax.axis_index("tp")
    sequences, own, width = far_ref.shape
    depth = far_w_ref.shape[1]

    far = far_ref[...].astype(F32).reshape(sequences * own, width)
    square = square_ref[:, :1] + jnp.sum(far * far, axis=-1, keepdims=True)
    scale = lax.rsqrt(square * (0.5 / width) + EPS)
    far = (far * gain_ref[:, pl.ds(pl.multiple_of((1 - tp) * width, width), width)]).astype(BF16)
    copies = []
    for c in range(depth // 512):
        lanes = slice(c * 512, (c + 1) * 512)
        result = (near_ref[:, lanes] + dot(far, far_w_ref[:, lanes])) * scale
        staged[:, :, lanes] = result.astype(BF16).reshape(sequences, own, 512)
        copies.append(pltpu.make_async_copy(staged.at[:, :, lanes], out_hbm.at[:, :, lanes], sem.at[c]))
        copies[-1].start()
    for copy in copies:
        copy.wait()


def vmem():
    return pl.BlockSpec(memory_space=pltpu.VMEM)


def hbm():
    return pl.BlockSpec(memory_space=pl.ANY)


def shards(
    layer_input,
    norm_gain,
    in_weight,
    gate_weight,
    rate_real,
    rate_imag,
    log_step,
    input_real,
    input_imag,
    output_real,
    output_imag,
    skip_weight,
    decay_offset,
    channel_gain,
    out_weight,
):
    nz, nx = lax.axis_size("sp_0"), lax.axis_size("sp_1")
    sequences, own, depth = layer_input.shape
    width = in_weight.shape[1]
    groups, states = rate_real.shape
    modes = groups * states
    rows = sequences * 2 * own
    dma = pltpu.SemaphoreType.DMA
    later = nz // BLOCK - 1
    tile = CHUNKS
    packs = modes // (tile // sequences * LANES)
    f32 = functools.partial(pltpu.VMEM, dtype=F32)
    b16 = functools.partial(pltpu.VMEM, dtype=BF16)
    near, square, far, far_w = pl.pallas_call(
        mixer_kernel,
        name="mixer",
        out_shape=[
            pltpu.VMEM((sequences * own, depth), F32),
            pltpu.VMEM((sequences * own, LANES), F32),
            pltpu.VMEM((sequences, own, width), BF16),
            pltpu.VMEM((width, depth), BF16),
        ],
        in_specs=[pl.BlockSpec(memory_space=pltpu.HBM)] * 15,
        out_specs=[vmem()] * 4,
        scratch_shapes=[
            b16((sequences, 2 * own, depth)),
            b16((depth, width)),
            b16((depth, width)),
            f32((1, depth)),
            f32((groups, states)),
            f32((groups, states)),
            f32((1, groups)),
            b16((width, states)),
            b16((width, states)),
            b16((width, states)),
            b16((width, states)),
            f32((1, width)),
            f32((sequences, groups, 2 * own)),
            f32((1, 2 * width)),
            b16((width, depth)),
            b16((2, sequences * own, depth)),
            f32((2, sequences * own, 256)),
            b16((sequences, 2 * own, width)),
            b16((sequences, 2 * own, width)),
            b16((rows, width)),
            f32((rows, width)),
            f32((rows, modes)),
            f32((rows, modes)),
            f32((rows, modes)),
            b16((width, modes // 2)),
            b16((width, modes // 2)),
            f32((rows, modes)),
            f32((rows, modes)),
            b16((rows, modes)),
            b16((rows, modes)),
            b16((width, modes // 2)),
            b16((width, modes // 2)),
            f32((24, modes)),
            f32((2, CHUNKS, modes)),
            f32((4, CHUNKS, modes)),
            f32((2, CHUNKS, modes)),
            f32((packs, tile, LANES)),
            f32((nx, packs, tile, LANES)),
            f32((packs, tile, LANES)),
            f32((BLOCK - 1, packs, tile, LANES)),
            f32((packs, tile, LANES)),
            f32((later, packs, tile, LANES)),
            f32((packs, 2 * tile, LANES)),
            b16((packs, 2 * tile, LANES)),
            b16((nx, packs, 2 * tile, LANES)),
            b16((packs, 2 * tile, LANES)),
            b16((BLOCK - 1, packs, 2 * tile, LANES)),
            b16((packs, 2 * tile, LANES)),
            b16((later, packs, 2 * tile, LANES)),
            f32((2, packs, tile, LANES)),
            b16((sequences, 2 * own, width)),
            dma((15,)),
            dma,
            dma,
            dma((2,)),
            dma((2,)),
            dma((nx - 1,)),
            dma((nx - 1,)),
            dma((BLOCK - 1,)),
            dma((BLOCK - 1,)),
            dma((nz - BLOCK,)),
            dma((later,)),
            dma((nx - 1,)),
            dma((nx - 1,)),
            dma((BLOCK - 1,)),
            dma((BLOCK - 1,)),
            dma((nz - BLOCK,)),
            dma((later,)),
            dma,
            dma,
        ],
        compiler_params=pltpu.CompilerParams(collective_id=0, has_side_effects=True, vmem_limit_bytes=67043328 - (5 << 20)),
    )(
        layer_input,
        in_weight,
        gate_weight,
        out_weight,
        norm_gain[None],
        rate_real,
        rate_imag,
        log_step[None],
        jnp.swapaxes(input_real, 1, 2).reshape(width, states),
        jnp.swapaxes(input_imag, 1, 2).reshape(width, states),
        output_real.reshape(width, states),
        output_imag.reshape(width, states),
        skip_weight[None],
        jnp.swapaxes(decay_offset, 1, 2),
        channel_gain[None],
    )
    return pl.pallas_call(
        finish_kernel,
        name="finish",
        out_shape=jax.ShapeDtypeStruct((sequences, own, depth), BF16),
        in_specs=[vmem()] * 5,
        out_specs=hbm(),
        scratch_shapes=[b16((sequences, own, depth)), dma((depth // 512,))],
        compiler_params=pltpu.CompilerParams(vmem_limit_bytes=16 << 20),
    )(near, square, far, channel_gain[None], far_w)


def solution(mesh):
    torus = Mesh(
        mesh.devices.reshape(mesh.shape["grp"], 16, 4, mesh.shape["tp"]),
        ("grp", "sp_0", "sp_1", "tp"),
    )
    return build(torus)


def build(torus):
    in_specs = (
        P("grp", SP_TP, None),
        P(),
        P(None, "tp"),
        P(None, "tp"),
        P("tp", None),
        P("tp", None),
        P("tp"),
        P("tp", None, None),
        P("tp", None, None),
        P("tp", None, None),
        P("tp", None, None),
        P("tp"),
        P("grp", SP, "tp"),
        P(),
        P("tp", None),
    )
    out_specs = P("grp", SP_TP, None)
    return jax.shard_map(shards, mesh=torus, in_specs=in_specs, out_specs=out_specs, check_vma=False)
```
